32 devices in a mesh: dp: 4 (over y, x), kv: 4 (over z), tp: 2 (over core).
Axes of the slice: x: 2, y: 2, z: 4, core: 2. Of those that a mesh axis runs over, the one named last changes fastest.
Arguments:
- tokens: bfloat16 [256, 2048], P('dp', ('kv', 'tp')), parts along dimension 0, may hold values from -64 to 64, as said below
- lengths: int32 [32], P(('dp', 'kv', 'tp')), parts along dimension 0, may hold values from 1 to 8, 28 in all
- state: float32 [32, 16, 128, 128], P(('dp', 'kv', 'tp')), parts along dimension 0, may hold values from -1.8 to 1.8
- gain_first: float32 [2048], replicated, may hold values from 0.1 to 1.9
- first_gate: bfloat16 [2048, 5632], P(None, 'kv'), may hold values from -0.125 to 0.125
- first_up: bfloat16 [2048, 5632], P(None, 'kv'), may hold values from -0.125 to 0.125
- first_down: bfloat16 [5632, 2048], P('kv'), may hold values from -0.109375 to 0.109375
- gain_mix: float32 [2048], replicated, may hold values from 0.1 to 1.9
- query_weight: bfloat16 [2048, 2048], P(None, ('kv', 'tp')), may hold values from -0.125 to 0.125
- key_weight: bfloat16 [2048, 2048], P(None, ('kv', 'tp')), may hold values from -0.125 to 0.125
- value_weight: bfloat16 [2048, 2048], P(None, ('kv', 'tp')), may hold values from -0.125 to 0.125
- gating_weight: bfloat16 [2048, 2048], P(None, ('kv', 'tp')), may hold values from -0.125 to 0.125
- write_weight: bfloat16 [2048, 16], replicated, may hold values from -0.125 to 0.125
- forget_weight: bfloat16 [2048, 16], replicated, may hold values from -0.125 to 0.125
- forget_rate: float32 [16], replicated, may hold values from -4 to 1.5
- out_weight: bfloat16 [2048, 2048], P(None, ('kv', 'tp')), may hold values from -0.125 to 0.125
- gain_second: float32 [2048], replicated, may hold values from 0.1 to 1.9
- second_gate: bfloat16 [2048, 5632], P(None, 'kv'), may hold values from -0.125 to 0.125
- second_up: bfloat16 [2048, 5632], P(None, 'kv'), may hold values from -0.125 to 0.125
- second_down: bfloat16 [5632, 2048], P('kv'), may hold values from -0.109375 to 0.109375
Outputs:
- mixed_out: bfloat16 [256, 2048], P('dp', ('kv', 'tp')), parts along dimension 0
- new_state: float32 [32, 16, 128, 128], P(('dp', 'kv', 'tp')), parts along dimension 0
The draws below stay inside these ranges and needn't reach their ends.
There are 4 independent parts, one for each index of `dp`. The reference program is written for one: setup_inputs(seed, part) draws one part's arguments, and reference() takes and returns one part's arrays. A program takes and returns all parts, laid end to end along the dimension named above; an argument that names none is the same for every part. Nothing has to cross between parts.
Inputs may be any that keep to these rules, and one draw needn't show every extreme that they name: Activations of the new tokens. `lengths`: the live new tokens of each sequence; within each independent group of 8 sequences (one part along dp) they sum to seven halves of 8, rounded down, and some sequence of each group has all 8 live.
All inputs are finite; a program needn't handle non-finite values.
Results may differ from the reference program's by a relative error of at most 0.0058.
Values may be sent and summed in bfloat16 or wider, within the bound.
No kernel may reach another device: no remote copies, remote signals or barrier semaphores. Data moves between devices by JAX's collectives and lax.ppermute only.
A program may use at most 128 MiB of HBM per device.

```python
import math
import jax
import jax.numpy as jnp
import numpy as np
from jax import lax

D = 2048
HEADS = 16
HEAD = 128
FF = 5632
BLK = 8
SEQS = 8
ROWS = 64


def draw_tokens(key, part):
    key_base = jax.random.fold_in(key, 17)
    key_one, key_two, key_three = jax.random.split(key_base, 3)
    columns = jnp.arange(D, dtype=jnp.float32)
    rough_cols = jnp.exp(jax.random.uniform(key_two, (1, D), jnp.float32, -0.35, 0.35))
    col_scale = jnp.exp(math.log(5.0) * (columns[None, :] / D - 0.5)) * rough_cols
    base = jnp.clip(jax.random.normal(key_one, (ROWS, D), jnp.float32), -5.0, 5.0)
    row_scale = jnp.exp(jax.random.uniform(key_three, (ROWS, 1), jnp.float32, math.log(0.4), math.log(4.0)))
    return (base * row_scale * col_scale).astype(jnp.bfloat16)


def spiked(array, key, source, target, blocks, factor):
    owner, partner = [(jnp.arange(array.shape[position]) // (array.shape[position] // blocks)).reshape([-1 if axis == position else 1 for axis in range(array.ndim)]) for position in (source, target)]
    chosen = jax.random.permutation(key, blocks)[partner]
    strong = (owner == chosen) | (owner == (partner + blocks // 2) % blocks)
    return jnp.where(strong, factor * array, array)


def steps_of(own_key, dims, pieces, smallest, high):
    level = 1.0
    for axis_at, parts in pieces:
        heights = jax.random.uniform(jax.random.fold_in(jax.random.fold_in(own_key, 6), axis_at), (parts,), jnp.float32, smallest / len(pieces), high / len(pieces))
        level = level * jnp.repeat(jnp.exp(heights), dims[axis_at] // parts).reshape((-1,) + (1,) * (len(dims) - 1 - axis_at))
    return level


def profile(count, total, most, skew):
    loads = [(1 << 20) // math.isqrt(standing ** skew) + 1 for standing in range(2, count + 1)]
    spare, given = total - most - (count - 1), [1] * (count - 1)
    while spare > 0:
        free = [i for i in range(count - 1) if given[i] < most]
        whole, left = sum([loads[i] for i in free]), spare
        for i in free:
            addition = min(most - given[i], max(1, left * loads[i] // whole), spare)
            given[i] = given[i] + addition
            spare = spare - addition
    return np.array([most] + given)


def uneven_parts(stream_key, number_of, total, most, slope):
    if number_of == 2:
        one = jax.random.randint(stream_key, (), max(1, total - most), min(most, total - 1) + 1)
        return jnp.stack([one, total - one])
    tallies = jnp.asarray(profile(number_of, total, most, slope), jnp.int32)
    pairs = (number_of - 1) // 2
    source_of, taker = tallies[1:1 + 2 * pairs:2], tallies[2:2 + 2 * pairs:2]
    slack = jnp.minimum(source_of - 1, most - taker)
    passed = jax.random.randint(jax.random.fold_in(stream_key, 1), (pairs,), 0, 1 << 20) % (slack + 1)
    tallies = tallies.at[1:1 + 2 * pairs:2].set(source_of - passed).at[2:2 + 2 * pairs:2].set(taker + passed)
    return tallies[jax.random.permutation(jax.random.fold_in(stream_key, 2), number_of)]


def gaussian(own_key, extent, spread, most, shards=(), kind=jnp.bfloat16):
    loudness = steps_of(own_key, extent, shards, -0.22, 0.18) if shards else 1.0
    values = jax.random.normal(own_key, extent, jnp.float32) * spread * loudness
    return jnp.minimum(jnp.maximum(values, -most), most).astype(kind)


def gaussian_with(stream_key, shape, scale, most, cuts, heavy, held_as=jnp.bfloat16):
    values = scale * jax.random.normal(stream_key, shape, jnp.float32)
    if cuts:
        values = values * steps_of(stream_key, shape, cuts, -0.22, 0.18)
    return jnp.clip(spiked(values, jax.random.fold_in(stream_key, 3), *heavy), -most, most).astype(held_as)


def setup_inputs(seed: int = 0, part: int = 0) -> dict:
    keys = jax.random.split(jax.random.key(seed), 21)
    part_splits = jax.random.split(jax.random.fold_in(keys[20], part), 21)
    tokens = draw_tokens(jax.random.fold_in(jax.random.fold_in(keys[20], part), 71), part)
    lengths = uneven_parts(part_splits[1], SEQS, SEQS * 7 // 2, BLK, 2).astype(jnp.int32)
    state = gaussian(part_splits[2], (SEQS, HEADS, HEAD, HEAD), 0.3, 1.8, ((0, 8),), jnp.float32)
    gain_first = jnp.clip(1.0 + 0.18 * jax.random.normal(keys[3], (D,), jnp.float32), 0.1, 1.9)
    first_gate = gaussian(keys[4], (D, FF), D ** -0.5, 0.125, ((1, 4),))
    first_up = gaussian(keys[5], (D, FF), D ** -0.5, 0.125, ((1, 4),))
    first_down = gaussian_with(keys[6], (FF, D), FF ** -0.5, 0.109375, ((0, 4),), (0, 1, 4, 2.0))
    gain_mix = jnp.clip(1.0 + 0.18 * jax.random.normal(keys[7], (D,), jnp.float32), 0.1, 1.9)
    query_weight = gaussian(keys[8], (D, HEADS * HEAD), D ** -0.5, 0.125, ((1, 8),))
    key_weight = gaussian(keys[9], (D, HEADS * HEAD), D ** -0.5, 0.125, ((1, 8),))
    value_weight = gaussian(keys[10], (D, HEADS * HEAD), D ** -0.5, 0.125, ((1, 8),))
    gating_weight = gaussian(keys[11], (D, HEADS * HEAD), D ** -0.5, 0.125, ((1, 8),))
    write_weight = gaussian(keys[12], (D, HEADS), D ** -0.5, 0.125)
    forget_weight = gaussian(keys[13], (D, HEADS), D ** -0.5, 0.125)
    forget_rate = jnp.clip(jax.random.uniform(keys[14], (HEADS,), jnp.float32, -4.0, 1.5), -4.0, 1.5)
    out_weight = gaussian(keys[15], (HEADS * HEAD, D), (HEADS * HEAD) ** -0.5, 0.125, ((1, 8),))
    gain_second = jnp.clip(1.0 + 0.18 * jax.random.normal(keys[16], (D,), jnp.float32), 0.1, 1.9)
    second_gate = gaussian(keys[17], (D, FF), D ** -0.5, 0.125, ((1, 4),))
    second_up = gaussian(keys[18], (D, FF), D ** -0.5, 0.125, ((1, 4),))
    second_down = gaussian_with(keys[19], (FF, D), FF ** -0.5, 0.109375, ((0, 4),), (0, 1, 4, 2.0))
    return {"tokens": tokens, "lengths": lengths, "state": state, "gain_first": gain_first, "first_gate": first_gate, "first_up": first_up, "first_down": first_down, "gain_mix": gain_mix, "query_weight": query_weight, "key_weight": key_weight, "value_weight": value_weight, "gating_weight": gating_weight, "write_weight": write_weight, "forget_weight": forget_weight, "forget_rate": forget_rate, "out_weight": out_weight, "gain_second": gain_second, "second_gate": second_gate, "second_up": second_up, "second_down": second_down}


EPSILON = 1e-06

def feed_forward(hidden_in, gain, w_gate, w_up, w_down):
    values = hidden_in.astype(jnp.float32)
    row_scale = lax.rsqrt(lax.optimization_barrier(jnp.mean(values * values, axis=1, keepdims=True)) + EPSILON)
    scaled = (values * gain).astype(jnp.bfloat16)
    gate_act = jnp.dot(scaled, w_gate, preferred_element_type=jnp.float32) * row_scale
    up_act = jnp.dot(scaled, w_up, preferred_element_type=jnp.float32) * row_scale
    hidden = (jax.nn.silu(gate_act) * up_act).astype(jnp.bfloat16)
    result = jnp.dot(hidden, w_down, preferred_element_type=jnp.float32)
    return (values + 0.5 * result).astype(jnp.bfloat16)

def delta_block(query, key_in, value, gating, write_pre, forget_pre, rates, live, state):
    seq_count, block_len, head_count, head_size = query.shape
    precise = lax.Precision.HIGHEST
    query_unit = query * lax.rsqrt(lax.optimization_barrier(jnp.sum(query * query, axis=-1, keepdims=True)) + EPSILON) / math.sqrt(head_size)
    key_unit = key_in * lax.rsqrt(lax.optimization_barrier(jnp.sum(key_in * key_in, axis=-1, keepdims=True)) + EPSILON)
    live_rows = live[:, :, None]
    write_gate = jax.nn.sigmoid(write_pre) * live_rows
    forget = -jnp.exp(rates)[None, None, :] * jax.nn.softplus(forget_pre) * live_rows
    cumulative = jnp.cumsum(forget, axis=1)
    cum_heads = jnp.transpose(cumulative, (0, 2, 1))
    positions = jnp.arange(block_len)
    causal = positions[:, None] >= positions[None, :]
    strict = positions[:, None] > positions[None, :]
    differ = jnp.minimum(cum_heads[:, :, :, None] - cum_heads[:, :, None, :], 0.0)
    decay_mat = jnp.where(causal, jnp.exp(differ), 0.0)
    key_dots = jnp.einsum('sthd,suhd->shtu', key_unit, key_unit, precision=precise)
    write_heads = jnp.transpose(write_gate, (0, 2, 1))
    strict_part = jnp.where(strict, write_heads[:, :, :, None] * decay_mat * key_dots, 0.0)
    identity = jnp.eye(block_len, dtype=jnp.float32)
    squared = jnp.einsum('shtu,shuv->shtv', strict_part, strict_part, precision=precise)
    fourth = jnp.einsum('shtu,shuv->shtv', squared, squared, precision=precise)
    inverse = jnp.einsum('shtu,shuv->shtv', identity - strict_part, identity + squared, precision=precise)
    inverse = jnp.einsum('shtu,shuv->shtv', inverse, identity + fourth, precision=precise)
    growth = jnp.exp(cumulative)
    target = jnp.einsum('shtu,suhv->sthv', inverse, write_gate[..., None] * value, precision=precise)
    key_mix = jnp.einsum('shtu,suhk->sthk', inverse, (write_gate * growth)[..., None] * key_unit, precision=precise)
    update = target - jnp.einsum('sthk,shkv->sthv', key_mix, state, precision=precise)
    scores = jnp.einsum('sthd,suhd->shtu', query_unit, key_unit, precision=precise) * decay_mat
    attend = jnp.einsum('sthk,shkv->sthv', query_unit * growth[..., None], state, precision=precise)
    attend = attend + jnp.einsum('shtu,suhv->sthv', scores, update, precision=precise)
    final_cum = cumulative[:, -1:, :]
    fading = jnp.exp(final_cum - cumulative)
    new_state = jnp.exp(final_cum[:, 0, :])[:, :, None, None] * state
    new_state = new_state + jnp.einsum('sthk,sthv->shkv', key_unit * fading[..., None], update, precision=precise)
    normed = attend * lax.rsqrt(lax.optimization_barrier(jnp.mean(attend * attend, axis=-1, keepdims=True)) + EPSILON)
    normed = normed * jax.nn.silu(gating) * live[:, :, None, None]
    mixed_heads = normed.reshape(seq_count * block_len, head_count * head_size).astype(jnp.bfloat16)
    return (mixed_heads, new_state)

def reference(tokens, lengths, state, gain_first, first_gate, first_up, first_down, gain_mix, query_weight, key_weight, value_weight, gating_weight, write_weight, forget_weight, forget_rate, out_weight, gain_second, second_gate, second_up, second_down):
    after_first = feed_forward(tokens, gain_first, first_gate, first_up, first_down)
    values = after_first.astype(jnp.float32)
    mix_scale = lax.rsqrt(lax.optimization_barrier(jnp.mean(values * values, axis=1, keepdims=True)) + EPSILON)
    mix_in = (values * gain_mix).astype(jnp.bfloat16)

    def project(matrix):
        return jnp.dot(mix_in, matrix, preferred_element_type=jnp.float32) * mix_scale
    query = project(query_weight).reshape(SEQS, BLK, HEADS, HEAD)
    key_in = project(key_weight).reshape(SEQS, BLK, HEADS, HEAD)
    value = project(value_weight).reshape(SEQS, BLK, HEADS, HEAD)
    gating = project(gating_weight).reshape(SEQS, BLK, HEADS, HEAD)
    write_pre = project(write_weight).reshape(SEQS, BLK, HEADS)
    forget_pre = project(forget_weight).reshape(SEQS, BLK, HEADS)
    positions = jnp.arange(BLK, dtype=jnp.int32)
    live = (positions[None, :] < lengths[:, None]).astype(jnp.float32)
    mixed_heads, new_state = delta_block(query, key_in, value, gating, write_pre, forget_pre, forget_rate, live, state)
    half_cols = HEADS * HEAD // 2
    running = values
    for half_index in range(2):
        portion = jnp.dot(mixed_heads[:, half_index * half_cols:(half_index + 1) * half_cols], out_weight[half_index * half_cols:(half_index + 1) * half_cols], preferred_element_type=jnp.float32)
        rounded = lax.optimization_barrier(portion.astype(jnp.bfloat16)).astype(jnp.float32)
        running = running + rounded
    after_mix = running.astype(jnp.bfloat16)
    mixed_out = feed_forward(after_mix, gain_second, second_gate, second_up, second_down)
    return (mixed_out, new_state)
```

```python
import functools
import math

import jax
import jax.numpy as jnp
from jax import lax
from jax.experimental import pallas as pl
from jax.experimental.pallas import tpu as pltpu
from jax.sharding import PartitionSpec as P

HEADS = 16
HEAD = 128
BLK = 8


EPSILON = 1e-06


def fold_step(gain, gate_cols, up_cols, portion):
    values = portion.astype(jnp.float32)
    scaled = (values * gain).astype(jnp.bfloat16)
    gate_acc = jnp.dot(scaled, gate_cols, preferred_element_type=jnp.float32)
    up_acc = jnp.dot(scaled, up_cols, preferred_element_type=jnp.float32)
    squares = jnp.sum(values * values, axis=1)
    return (gate_acc, up_acc, squares)


def finish_units(gate_acc, up_acc, squares, channels, down_rows):
    row_scale = lax.rsqrt(squares / channels + EPSILON)[:, None]
    hidden = (jax.nn.silu(gate_acc * row_scale) * (up_acc * row_scale)).astype(jnp.bfloat16)
    return jnp.dot(hidden, down_rows, preferred_element_type=jnp.float32)


def feed_forward(hidden_in, gain, w_gate, w_up, w_down):
    channels = gain.shape[0]
    paired = lax.all_to_all(hidden_in, "tp", split_axis=0, concat_axis=1, tiled=True)
    gate_acc, up_acc, squares = fold_step(
        gain, w_gate, w_up, lax.all_gather(paired, "kv", axis=1, tiled=True)
    )
    ffn_term = finish_units(gate_acc, up_acc, squares, channels, w_down)
    partial_value = lax.psum_scatter(ffn_term, "kv", scatter_dimension=1, tiled=True)
    summed = lax.all_to_all(partial_value, "tp", split_axis=1, concat_axis=0, tiled=True)
    return (hidden_in.astype(jnp.float32) + 0.5 * summed).astype(jnp.bfloat16)


def delta_block(query, key_in, value, gating, write_pre, forget_pre, rates, live, state):
    seq_count, block_len, head_count, head_size = query.shape
    precise = lax.Precision.HIGHEST
    query_unit = (
        query
        * lax.rsqrt(jnp.sum(query * query, axis=-1, keepdims=True) + EPSILON)
        / math.sqrt(head_size)
    )
    key_unit = key_in * lax.rsqrt(jnp.sum(key_in * key_in, axis=-1, keepdims=True) + EPSILON)
    live_rows = live[:, :, None]
    write_gate = jax.nn.sigmoid(write_pre) * live_rows
    forget = -jnp.exp(rates)[None, None, :] * jax.nn.softplus(forget_pre) * live_rows
    cumulative = jnp.cumsum(forget, axis=1)
    cum_heads = jnp.transpose(cumulative, (0, 2, 1))
    positions = jnp.arange(block_len)
    causal = positions[:, None] >= positions[None, :]
    strict = positions[:, None] > positions[None, :]
    differ = jnp.minimum(cum_heads[:, :, :, None] - cum_heads[:, :, None, :], 0.0)
    decay_mat = jnp.where(causal, jnp.exp(differ), 0.0)
    key_dots = jnp.einsum("sthd,suhd->shtu", key_unit, key_unit, precision=precise)
    write_heads = jnp.transpose(write_gate, (0, 2, 1))
    strict_part = jnp.where(strict, write_heads[:, :, :, None] * decay_mat * key_dots, 0.0)
    identity = jnp.eye(block_len, dtype=jnp.float32)
    squared = jnp.einsum("shtu,shuv->shtv", strict_part, strict_part, precision=precise)
    fourth = jnp.einsum("shtu,shuv->shtv", squared, squared, precision=precise)
    inverse = jnp.einsum(
        "shtu,shuv->shtv", identity - strict_part, identity + squared, precision=precise
    )
    inverse = jnp.einsum("shtu,shuv->shtv", inverse, identity + fourth, precision=precise)
    growth = jnp.exp(cumulative)
    target = jnp.einsum(
        "shtu,suhv->sthv", inverse, write_gate[..., None] * value, precision=precise
    )
    key_mix = jnp.einsum(
        "shtu,suhk->sthk", inverse, (write_gate * growth)[..., None] * key_unit, precision=precise
    )
    update = target - jnp.einsum("sthk,shkv->sthv", key_mix, state, precision=precise)
    scores = jnp.einsum("sthd,suhd->shtu", query_unit, key_unit, precision=precise) * decay_mat
    attend = jnp.einsum("sthk,shkv->sthv", query_unit * growth[..., None], state, precision=precise)
    attend = attend + jnp.einsum("shtu,suhv->sthv", scores, update, precision=precise)
    final_cum = cumulative[:, -1:, :]
    fading = jnp.exp(final_cum - cumulative)
    new_state = jnp.exp(final_cum[:, 0, :])[:, :, None, None] * state
    new_state = new_state + jnp.einsum(
        "sthk,sthv->shkv", key_unit * fading[..., None], update, precision=precise
    )
    normed = attend * lax.rsqrt(jnp.mean(attend * attend, axis=-1, keepdims=True) + EPSILON)
    normed = normed * jax.nn.silu(gating) * live[:, :, None, None]
    mixed_heads = normed.reshape(seq_count * block_len, head_count * head_size).astype(jnp.bfloat16)
    return (mixed_heads, new_state)


def general_device(
    tokens,
    lengths,
    state,
    gain_first,
    first_gate,
    first_up,
    first_down,
    gain_mix,
    query_weight,
    key_weight,
    value_weight,
    gating_weight,
    write_weight,
    forget_weight,
    forget_rate,
    out_weight,
    gain_second,
    second_gate,
    second_up,
    second_down,
):
    after_first = feed_forward(tokens, gain_first, first_gate, first_up, first_down)
    seq_count = lengths.shape[0]
    own_count = seq_count * BLK
    whole_rows = lax.all_gather(after_first, ("kv", "tp"), axis=1, tiled=True)
    scaled_all = (whole_rows.astype(jnp.float32) * gain_mix).astype(jnp.bfloat16)
    stacked = jnp.stack(
        [
            jnp.dot(scaled_all, matrix, preferred_element_type=jnp.float32)
            for matrix in (query_weight, key_weight, value_weight, gating_weight)
        ]
    )
    owned = lax.all_to_all(
        stacked.astype(jnp.bfloat16), ("kv", "tp"), split_axis=1, concat_axis=2, tiled=True
    ).astype(stacked.dtype)
    row_start = lax.axis_index(("kv", "tp")) * own_count
    own_values = lax.dynamic_slice_in_dim(whole_rows, row_start, own_count, 0).astype(jnp.float32)
    own_scaled = lax.dynamic_slice_in_dim(scaled_all, row_start, own_count, 0)
    mix_scale = lax.rsqrt(jnp.mean(own_values * own_values, axis=1, keepdims=True) + EPSILON)
    query = (owned[0] * mix_scale).reshape(seq_count, BLK, HEADS, HEAD)
    key_in = (owned[1] * mix_scale).reshape(seq_count, BLK, HEADS, HEAD)
    value = (owned[2] * mix_scale).reshape(seq_count, BLK, HEADS, HEAD)
    gating = (owned[3] * mix_scale).reshape(seq_count, BLK, HEADS, HEAD)
    write_pre = (
        jnp.dot(own_scaled, write_weight, preferred_element_type=jnp.float32) * mix_scale
    ).reshape(seq_count, BLK, HEADS)
    forget_pre = (
        jnp.dot(own_scaled, forget_weight, preferred_element_type=jnp.float32) * mix_scale
    ).reshape(seq_count, BLK, HEADS)
    positions = jnp.arange(BLK, dtype=jnp.int32)
    live = (positions[None, :] < lengths[:, None]).astype(jnp.float32)
    mixed_heads, new_state = delta_block(
        query, key_in, value, gating, write_pre, forget_pre, forget_rate, live, state
    )
    half_cols = mixed_heads.shape[1] // 2
    portion = lax.all_gather(mixed_heads, ("kv", "tp"), axis=0, tiled=True)
    first_half = jnp.dot(
        portion[:, :half_cols], out_weight[:half_cols], preferred_element_type=jnp.float32
    ).astype(jnp.bfloat16)
    second_half = jnp.dot(
        portion[:, half_cols:], out_weight[half_cols:], preferred_element_type=jnp.float32
    ).astype(jnp.bfloat16)
    first_half, second_half = lax.optimization_barrier((first_half, second_half))
    mixed_sum = first_half.astype(jnp.float32) + second_half.astype(jnp.float32)
    after_mix = (after_first.astype(jnp.float32) + mixed_sum).astype(jnp.bfloat16)
    mixed_out = feed_forward(after_mix, gain_second, second_gate, second_up, second_down)
    return (mixed_out, new_state)


VMEM_SPEC = pl.BlockSpec(memory_space=pltpu.VMEM)
HBM_SPEC = pl.BlockSpec(memory_space=pl.ANY)
GROUP = ("kv", "tp")
F32, BF16 = jnp.float32, jnp.bfloat16


def call(body, out_shapes, args, in_specs=None, scratch=(), limit=16 << 20, out_specs=None, name=None):
    single = not isinstance(out_shapes, (list, tuple))
    shapes = [out_shapes] if single else list(out_shapes)
    outs = pl.pallas_call(
        body,
        out_shape=shapes,
        in_specs=in_specs or [VMEM_SPEC] * len(args),
        out_specs=out_specs or [VMEM_SPEC] * len(shapes),
        scratch_shapes=list(scratch),
        compiler_params=pltpu.CompilerParams(vmem_limit_bytes=limit),
        name=name,
    )(*args)
    return outs[0] if single else outs


def my_index():
    return lax.axis_index("kv") * lax.axis_size("tp") + lax.axis_index("tp")


def swap(value, mask, count):
    return lax.ppermute(value, GROUP, [(i, i ^ mask) for i in range(count)])


def gather_blocks(own, count):
    near = [own] + [swap(own, mask, count) for mask in range(2, count, 2)]
    blocks = []
    for block in near:
        blocks += [block, swap(block, 1, count)]
    return blocks


def assemble(blocks, index, gain_ref, scaled_ref):
    width = blocks[0].shape[1]
    squares = None
    for mask, block in enumerate(blocks):
        values = block[...].astype(F32)
        owner = index ^ mask
        gain = gain_ref[pl.ds(owner, 1), :]
        column = pl.multiple_of(owner * width, width)
        scaled_ref[:, pl.ds(column, width)] = (values * gain).astype(BF16)
        part = values * values
        squares = part if squares is None else squares + part
    total = jnp.sum(squares, axis=1, keepdims=True)
    channels = width * len(blocks)
    return lax.rsqrt(total / channels + EPSILON)


def ffn_kernel(count, span, skip, *refs):
    blocks = refs[:count]
    gain_ref, gate_hbm, up_hbm, down_hbm = refs[count : count + 4]
    own_ref, cross_ref = refs[count + 4 : count + 6]
    scaled, gate_buf, up_buf, down_buf, gate_sem, up_sem, down_sem = refs[count + 6 :]
    index = my_index()
    core = lax.axis_index("tp")
    start = pl.multiple_of(core * skip, 128)
    width = blocks[0].shape[1]
    channels = width * count
    pieces = gate_buf.shape[0]
    depth = channels // pieces
    copies = []
    for piece in range(pieces):
        rows = pl.ds(piece * depth, depth)
        for hbm, buf, sem in ((gate_hbm, gate_buf, gate_sem), (up_hbm, up_buf, up_sem)):
            copy = pltpu.make_async_copy(
                hbm.at[rows, pl.ds(start, span)], buf.at[piece], sem.at[piece]
            )
            copy.start()
            copies.append(copy)
    order = list(range(1, count, 2)) + list(range(0, count, 2))
    down_copies = {}
    for mask in order:
        column = pl.multiple_of((index ^ mask) * width, width)
        copy = pltpu.make_async_copy(
            down_hbm.at[pl.ds(start, span), pl.ds(column, width)], down_buf.at[mask], down_sem.at[mask]
        )
        copy.start()
        down_copies[mask] = copy
    row_scale = assemble(blocks, index, gain_ref, scaled)
    gate_acc = up_acc = None
    for piece in range(pieces):
        lhs = scaled[:, piece * depth : (piece + 1) * depth]
        copies[2 * piece].wait()
        part = jnp.dot(lhs, gate_buf[piece], preferred_element_type=F32)
        gate_acc = part if gate_acc is None else gate_acc + part
        copies[2 * piece + 1].wait()
        part = jnp.dot(lhs, up_buf[piece], preferred_element_type=F32)
        up_acc = part if up_acc is None else up_acc + part
    gate_act = gate_acc * row_scale
    hidden = gate_act * jax.nn.sigmoid(gate_act) * (up_acc * row_scale)
    unit = lax.broadcasted_iota(jnp.int32, hidden.shape, 1)
    repeated = core * (lax.axis_size("tp") * span - down_hbm.shape[0])
    hidden = jnp.where(unit >= repeated, hidden, 0.0).astype(BF16)
    for mask in order:
        down_copies[mask].wait()
        part = jnp.dot(hidden, down_buf[mask], preferred_element_type=F32)
        if mask % 2:
            cross_ref[mask // 2] = part.astype(BF16)
        else:
            own_ref[mask // 2] = part


def pair_sum_kernel(own_ref, cross_ref, mine_ref, *sends):
    mine_ref[...] = own_ref[0] + cross_ref[0].astype(F32)
    for step, send in enumerate(sends):
        send[...] = (own_ref[step + 1] + cross_ref[step + 1].astype(F32)).astype(BF16)


def residual_kernel(base_ref, mine_ref, *refs):
    total = mine_ref[...]
    for received in refs[:-1]:
        total = total + received[...].astype(F32)
    refs[-1][...] = (base_ref[...].astype(F32) + 0.5 * total).astype(BF16)


def half_step(own, count, gain, gate, up, down):
    rows, width = own.shape
    near = count // 2
    units = gate.shape[1]
    tiles = units // 128
    span = -(-tiles // 2) * 128
    skip = units - span
    blocks = gather_blocks(own, count)
    pieces = 4
    depth = width * count // pieces
    own_part, cross_part = call(
        functools.partial(ffn_kernel, count, span, skip),
        [pltpu.VMEM((near, rows, width), F32), pltpu.VMEM((near, rows, width), BF16)],
        [*blocks, gain.reshape(count, width), gate, up, down],
        in_specs=[VMEM_SPEC] * (count + 1) + [HBM_SPEC] * 3,
        scratch=[
            pltpu.VMEM((rows, width * count), BF16),
            pltpu.VMEM((pieces, depth, span), BF16),
            pltpu.VMEM((pieces, depth, span), BF16),
            pltpu.VMEM((count, span, width), BF16),
            pltpu.SemaphoreType.DMA((pieces,)),
            pltpu.SemaphoreType.DMA((pieces,)),
            pltpu.SemaphoreType.DMA((count,)),
        ],
        limit=24 << 20,
        name="ffn",
    )
    cross_sum = swap(cross_part, 1, count)
    mine, *sends = call(
        pair_sum_kernel,
        [pltpu.VMEM((rows, width), F32)] + [pltpu.VMEM((rows, width), BF16)] * (near - 1),
        [own_part, cross_sum],
        name="pair_sum",
    )
    received = [swap(send, 2 * (step + 1), count) for step, send in enumerate(sends)]
    return call(
        residual_kernel,
        pltpu.VMEM((rows, width), BF16),
        [own, mine, *received],
        name="residual",
    )


def project_kernel(count, *refs):
    blocks = refs[:count]
    gain_ref, query_w, key_w, value_w, gating_w, write_t, forget_t = refs[count : count + 7]
    sends = refs[count + 7 : count + 7 + count]
    pre_ref, scaled, result, pre_scratch = refs[count + 7 + count :]
    index = my_index()
    row_scale = assemble(blocks, index, gain_ref, scaled)
    lhs = scaled[...]
    width = query_w.shape[1]
    for place, weight in enumerate((query_w, key_w, value_w, gating_w)):
        part = jnp.dot(lhs, weight[...], preferred_element_type=F32)
        result[:, place * width : (place + 1) * width] = part * row_scale
    heads = write_t.shape[0]
    contract = (((1,), (1,)), ((), ()))
    for place, weight in enumerate((write_t, forget_t)):
        part = lax.dot_general(lhs, weight[...], contract, preferred_element_type=F32)
        pre_scratch[:, place * heads : (place + 1) * heads] = part * row_scale
    for mask, send in enumerate(sends):
        row = pl.multiple_of((index ^ mask) * BLK, BLK)
        send[...] = result[pl.ds(row, BLK), :].astype(BF16)
    row = pl.multiple_of(index * BLK, BLK)
    pre_ref[...] = pre_scratch[pl.ds(row, BLK), :]


def parts(value):
    high = value.astype(BF16)
    return high, (value - high.astype(F32)).astype(BF16)


def dot_parts(left, right, dims=(((1,), (0,)), ((), ()))):
    left_high, left_low = left
    right_high, right_low = right
    total = lax.dot_general(left_high, right_low, dims, preferred_element_type=F32)
    total = total + lax.dot_general(left_low, right_high, dims, preferred_element_type=F32)
    return total + lax.dot_general(left_high, right_high, dims, preferred_element_type=F32)


def delta_kernel(count, *refs):
    blocks = refs[:count]
    pre_ref, rate_ref, length_ref, state_ref = refs[count : count + 4]
    mixed_ref, update_ref, faded_ref, final_ref, ordered = refs[count + 4 :]
    index = my_index()
    for mask, block in enumerate(blocks):
        ordered[pl.ds(index ^ mask, 1)] = block[...].astype(F32)[None]
    heads = rate_ref.shape[1]
    size = state_ref.shape[-1]
    per_block = heads // count
    rows = heads * BLK
    width = per_block * size

    def stack(place):
        found = []
        for head in range(heads):
            column = place * width + (head % per_block) * size
            found.append(ordered[head // per_block, :, column : column + size])
        return jnp.concatenate(found, axis=0)

    query, key_in, value, gating = (stack(place) for place in range(4))
    query_unit = query * lax.rsqrt(jnp.sum(query * query, axis=1, keepdims=True) + EPSILON) * (1.0 / math.sqrt(size))
    key_unit = key_in * lax.rsqrt(jnp.sum(key_in * key_in, axis=1, keepdims=True) + EPSILON)
    step_of = lax.broadcasted_iota(jnp.int32, (BLK, heads), 0)
    live = (step_of < length_ref[0]).astype(F32)
    pre = pre_ref[...]
    write_gate = jax.nn.sigmoid(pre[:, :heads]) * live
    forget_in = pre[:, heads:]
    softplus = jnp.maximum(forget_in, 0.0) + jnp.log1p(jnp.exp(-jnp.abs(forget_in)))
    forget = -jnp.exp(rate_ref[...]) * softplus * live
    cumulative = forget
    lower = 1
    while lower < BLK:
        moved = pltpu.roll(cumulative, lower, 0)
        cumulative = cumulative + jnp.where(step_of >= lower, moved, 0.0)
        lower *= 2
    final = jnp.broadcast_to(cumulative[BLK - 1 :, :], (BLK, heads))
    row_head = lax.broadcasted_iota(jnp.int32, (rows, heads), 0) // BLK
    picked = row_head == lax.broadcasted_iota(jnp.int32, (rows, heads), 1)

    def column_of(array):
        tall = jnp.concatenate([array] * heads, axis=0)
        return jnp.sum(jnp.where(picked, tall, 0.0), axis=1, keepdims=True)

    write_col, live_col = column_of(write_gate), column_of(live)
    cum_col, final_col = column_of(cumulative), column_of(final)
    down_at = lax.broadcasted_iota(jnp.int32, (rows, rows), 0)
    over_at = lax.broadcasted_iota(jnp.int32, (rows, rows), 1)
    same = (down_at // BLK) == (over_at // BLK)
    diagonal = down_at == over_at
    cum_row = jnp.sum(jnp.where(diagonal, cum_col, 0.0), axis=0, keepdims=True)
    causal = same & (down_at >= over_at)
    decay = jnp.where(causal, jnp.exp(jnp.minimum(cum_col - cum_row, 0.0)), 0.0)
    across = (((1,), (1,)), ((), ()))
    key_parts = parts(key_unit)
    strict_part = jnp.where(diagonal, 0.0, write_col * decay * dot_parts(key_parts, key_parts, across))
    scores = decay * dot_parts(parts(query_unit), key_parts, across)
    identity = diagonal.astype(F32)
    strict_split = parts(strict_part)
    squared = dot_parts(strict_split, strict_split)
    squared_split = parts(squared)
    fourth = dot_parts(squared_split, squared_split)
    inverse = identity - strict_part + squared - dot_parts(strict_split, squared_split)
    inverse = inverse + dot_parts(parts(inverse), parts(fourth))
    growth = jnp.exp(cum_col)
    key_grown, query_grown = key_unit * growth, query_unit * growth
    from_key, from_query = [], []
    for head in range(heads):
        at = slice(head * BLK, (head + 1) * BLK)
        both = jnp.concatenate([key_grown[at], query_grown[at]], axis=0)
        found = dot_parts(parts(both), parts(state_ref[head]))
        from_key.append(found[:BLK])
        from_query.append(found[BLK:])
    target = write_col * (value - jnp.concatenate(from_key, axis=0))
    update = dot_parts(parts(inverse), parts(target))
    attend = jnp.concatenate(from_query, axis=0) + dot_parts(parts(scores), parts(update))
    normed = attend * lax.rsqrt(jnp.mean(attend * attend, axis=1, keepdims=True) + EPSILON)
    normed = (normed * (gating * jax.nn.sigmoid(gating)) * live_col).astype(BF16)
    for head in range(heads):
        mixed_ref[:, head * size : (head + 1) * size] = normed[head * BLK : (head + 1) * BLK]
    update_ref[...] = update
    faded_ref[...] = key_unit * jnp.exp(final_col - cum_col)
    final_ref[...] = jnp.broadcast_to(jnp.exp(final_col), final_ref.shape)


def state_kernel(update_ref, faded_ref, final_ref, state_ref, new_ref):
    heads = state_ref.shape[0]
    along = (((0,), (0,)), ((), ()))
    for head in range(heads):
        at = slice(head * BLK, (head + 1) * BLK)
        left_high, left_low = parts(faded_ref[at])
        right_high, right_low = parts(update_ref[at])
        left = jnp.concatenate([left_high, left_high, left_low, left_low], axis=0)
        right = jnp.concatenate([right_high, right_low, right_high, right_low], axis=0)
        grown = lax.dot_general(left, right, along, preferred_element_type=F32)
        scale = final_ref[head * BLK : head * BLK + 1, :]
        new_ref[head] = scale * state_ref[head] + grown


def out_kernel(count, *refs):
    blocks = refs[:count]
    weight_ref, base_ref, out_ref, scratch = refs[count:]
    index = my_index()
    lhs = jnp.concatenate([block[...].astype(F32) for block in blocks], axis=0).astype(BF16)
    half = lhs.shape[1] // 2
    first = jnp.dot(lhs[:, :half], weight_ref[:half, :], preferred_element_type=F32).astype(BF16)
    second = jnp.dot(lhs[:, half:], weight_ref[half:, :], preferred_element_type=F32).astype(BF16)
    total = first.astype(F32) + second.astype(F32)
    for mask in range(count):
        row = pl.multiple_of((index ^ mask) * BLK, BLK)
        scratch[pl.ds(row, BLK), :] = total[mask * BLK : (mask + 1) * BLK]
    out_ref[...] = (base_ref[...].astype(F32) + scratch[...]).astype(BF16)


def group_device(
    tokens,
    lengths,
    state,
    gain_first,
    first_gate,
    first_up,
    first_down,
    gain_mix,
    query_weight,
    key_weight,
    value_weight,
    gating_weight,
    write_weight,
    forget_weight,
    forget_rate,
    out_weight,
    gain_second,
    second_gate,
    second_up,
    second_down,
):
    count = lax.axis_size("kv") * lax.axis_size("tp")
    rows, width = tokens.shape
    channels = gain_first.shape[0]
    heads, size = state.shape[1], state.shape[2]
    after_first = half_step(tokens, count, gain_first, first_gate, first_up, first_down)
    blocks = gather_blocks(after_first, count)
    columns = 4 * width
    *sends, pre = call(
        functools.partial(project_kernel, count),
        [pltpu.VMEM((BLK, columns), BF16)] * count + [pltpu.VMEM((BLK, 2 * heads), F32)],
        [
            *blocks,
            gain_mix.reshape(count, width),
            query_weight,
            key_weight,
            value_weight,
            gating_weight,
            write_weight.T,
            forget_weight.T,
        ],
        scratch=[
            pltpu.VMEM((rows, channels), BF16),
            pltpu.VMEM((rows, columns), F32),
            pltpu.VMEM((rows, 2 * heads), F32),
        ],
        name="project",
    )
    owned = [sends[0]] + [swap(sends[mask], mask, count) for mask in range(1, count)]
    matrices = state.reshape(heads, size, size)
    mixed, update, faded, final = call(
        functools.partial(delta_kernel, count),
        [
            pltpu.VMEM((BLK, channels), BF16),
            pltpu.VMEM((heads * BLK, size), F32),
            pltpu.VMEM((heads * BLK, size), F32),
            pltpu.VMEM((heads * BLK, size), F32),
        ],
        [*owned, pre, forget_rate.reshape(1, heads), lengths, matrices],
        in_specs=[VMEM_SPEC] * (count + 2) + [pl.BlockSpec(memory_space=pltpu.SMEM), VMEM_SPEC],
        scratch=[pltpu.VMEM((count, BLK, columns), F32)],
        name="delta",
    )
    head_blocks = gather_blocks(mixed, count)
    new_state = call(
        state_kernel,
        jax.ShapeDtypeStruct((heads, size, size), F32),
        [update, faded, final, matrices],
        name="state",
    )
    after_mix = call(
        functools.partial(out_kernel, count),
        pltpu.VMEM((rows, width), BF16),
        [*head_blocks, out_weight, after_first],
        scratch=[pltpu.VMEM((rows, width), F32)],
        name="out",
    )
    mixed_out = half_step(after_mix, count, gain_second, second_gate, second_up, second_down)
    return (mixed_out, new_state.reshape(state.shape))


def fits_group(mesh):
    near, cores = mesh.shape["kv"], mesh.shape["tp"]
    count = near * cores
    return cores == 2 and near & (near - 1) == 0 and near <= 8 and (HEADS * HEAD) % (count * 128) == 0


def per_device(mesh, *arrays):
    tokens, lengths, gate = arrays[0], arrays[1], arrays[4]
    suits = fits_group(mesh) and lengths.shape[0] == 1 and gate.shape[1] % 128 == 0
    return (group_device if suits else general_device)(*arrays)


def solution(mesh):
    in_specs = (
        P("dp", ("kv", "tp")),
        P(("dp", "kv", "tp")),
        P(("dp", "kv", "tp"), None, None, None),
        P(),
        P(None, "kv"),
        P(None, "kv"),
        P("kv", None),
        P(),
        P(None, ("kv", "tp")),
        P(None, ("kv", "tp")),
        P(None, ("kv", "tp")),
        P(None, ("kv", "tp")),
        P(),
        P(),
        P(),
        P(None, ("kv", "tp")),
        P(),
        P(None, "kv"),
        P(None, "kv"),
        P("kv", None),
    )
    out_specs = (P("dp", ("kv", "tp")), P(("dp", "kv", "tp"), None, None, None))
    return jax.shard_map(
        functools.partial(per_device, mesh), mesh=mesh, in_specs=in_specs, out_specs=out_specs, check_vma=False
    )
```

```python
import functools
import math

import jax
import jax.numpy as jnp
from jax import lax
from jax.experimental import pallas as pl
from jax.experimental.pallas import tpu as pltpu
from jax.sharding import PartitionSpec as P


HEADS = 16
HEAD = 128
BLK = 8


EPSILON = 1e-06


def fold_step(gain, gate_cols, up_cols, portion):
    values = portion.astype(jnp.float32)
    scaled = (values * gain).astype(jnp.bfloat16)
    gate_acc = jnp.dot(scaled, gate_cols, preferred_element_type=jnp.float32)
    up_acc = jnp.dot(scaled, up_cols, preferred_element_type=jnp.float32)
    squares = jnp.sum(values * values, axis=1)
    return (gate_acc, up_acc, squares)


def finish_units(gate_acc, up_acc, squares, channels, down_rows):
    row_scale = lax.rsqrt(squares / channels + EPSILON)[:, None]
    hidden = (jax.nn.silu(gate_acc * row_scale) * (up_acc * row_scale)).astype(jnp.bfloat16)
    return jnp.dot(hidden, down_rows, preferred_element_type=jnp.float32)


def feed_forward(hidden_in, gain, w_gate, w_up, w_down):
    channels = gain.shape[0]
    paired = lax.all_to_all(hidden_in, "tp", split_axis=0, concat_axis=1, tiled=True)
    gate_acc, up_acc, squares = fold_step(
        gain, w_gate, w_up, lax.all_gather(paired, "kv", axis=1, tiled=True)
    )
    ffn_term = finish_units(gate_acc, up_acc, squares, channels, w_down)
    partial_value = lax.psum_scatter(ffn_term, "kv", scatter_dimension=1, tiled=True)
    summed = lax.all_to_all(partial_value, "tp", split_axis=1, concat_axis=0, tiled=True)
    return (hidden_in.astype(jnp.float32) + 0.5 * summed).astype(jnp.bfloat16)


def delta_block(query, key_in, value, gating, write_pre, forget_pre, rates, live, state):
    seq_count, block_len, head_count, head_size = query.shape
    precise = lax.Precision.HIGHEST
    query_unit = (
        query
        * lax.rsqrt(jnp.sum(query * query, axis=-1, keepdims=True) + EPSILON)
        / math.sqrt(head_size)
    )
    key_unit = key_in * lax.rsqrt(jnp.sum(key_in * key_in, axis=-1, keepdims=True) + EPSILON)
    live_rows = live[:, :, None]
    write_gate = jax.nn.sigmoid(write_pre) * live_rows
    forget = -jnp.exp(rates)[None, None, :] * jax.nn.softplus(forget_pre) * live_rows
    cumulative = jnp.cumsum(forget, axis=1)
    cum_heads = jnp.transpose(cumulative, (0, 2, 1))
    positions = jnp.arange(block_len)
    causal = positions[:, None] >= positions[None, :]
    strict = positions[:, None] > positions[None, :]
    differ = jnp.minimum(cum_heads[:, :, :, None] - cum_heads[:, :, None, :], 0.0)
    decay_mat = jnp.where(causal, jnp.exp(differ), 0.0)
    key_dots = jnp.einsum("sthd,suhd->shtu", key_unit, key_unit, precision=precise)
    write_heads = jnp.transpose(write_gate, (0, 2, 1))
    strict_part = jnp.where(strict, write_heads[:, :, :, None] * decay_mat * key_dots, 0.0)
    identity = jnp.eye(block_len, dtype=jnp.float32)
    squared = jnp.einsum("shtu,shuv->shtv", strict_part, strict_part, precision=precise)
    fourth = jnp.einsum("shtu,shuv->shtv", squared, squared, precision=precise)
    inverse = jnp.einsum(
        "shtu,shuv->shtv", identity - strict_part, identity + squared, precision=precise
    )
    inverse = jnp.einsum("shtu,shuv->shtv", inverse, identity + fourth, precision=precise)
    growth = jnp.exp(cumulative)
    target = jnp.einsum(
        "shtu,suhv->sthv", inverse, write_gate[..., None] * value, precision=precise
    )
    key_mix = jnp.einsum(
        "shtu,suhk->sthk", inverse, (write_gate * growth)[..., None] * key_unit, precision=precise
    )
    update = target - jnp.einsum("sthk,shkv->sthv", key_mix, state, precision=precise)
    scores = jnp.einsum("sthd,suhd->shtu", query_unit, key_unit, precision=precise) * decay_mat
    attend = jnp.einsum("sthk,shkv->sthv", query_unit * growth[..., None], state, precision=precise)
    attend = attend + jnp.einsum("shtu,suhv->sthv", scores, update, precision=precise)
    final_cum = cumulative[:, -1:, :]
    fading = jnp.exp(final_cum - cumulative)
    new_state = jnp.exp(final_cum[:, 0, :])[:, :, None, None] * state
    new_state = new_state + jnp.einsum(
        "sthk,sthv->shkv", key_unit * fading[..., None], update, precision=precise
    )
    normed = attend * lax.rsqrt(jnp.mean(attend * attend, axis=-1, keepdims=True) + EPSILON)
    normed = normed * jax.nn.silu(gating) * live[:, :, None, None]
    mixed_heads = normed.reshape(seq_count * block_len, head_count * head_size).astype(jnp.bfloat16)
    return (mixed_heads, new_state)


def general_device(
    tokens,
    lengths,
    state,
    gain_first,
    first_gate,
    first_up,
    first_down,
    gain_mix,
    query_weight,
    key_weight,
    value_weight,
    gating_weight,
    write_weight,
    forget_weight,
    forget_rate,
    out_weight,
    gain_second,
    second_gate,
    second_up,
    second_down,
):
    after_first = feed_forward(tokens, gain_first, first_gate, first_up, first_down)
    seq_count = lengths.shape[0]
    own_count = seq_count * BLK
    whole_rows = lax.all_gather(after_first, ("kv", "tp"), axis=1, tiled=True)
    scaled_all = (whole_rows.astype(jnp.float32) * gain_mix).astype(jnp.bfloat16)
    stacked = jnp.stack(
        [
            jnp.dot(scaled_all, matrix, preferred_element_type=jnp.float32)
            for matrix in (query_weight, key_weight, value_weight, gating_weight)
        ]
    )
    owned = lax.all_to_all(
        stacked.astype(jnp.bfloat16), ("kv", "tp"), split_axis=1, concat_axis=2, tiled=True
    ).astype(stacked.dtype)
    row_start = lax.axis_index(("kv", "tp")) * own_count
    own_values = lax.dynamic_slice_in_dim(whole_rows, row_start, own_count, 0).astype(jnp.float32)
    own_scaled = lax.dynamic_slice_in_dim(scaled_all, row_start, own_count, 0)
    mix_scale = lax.rsqrt(jnp.mean(own_values * own_values, axis=1, keepdims=True) + EPSILON)
    query = (owned[0] * mix_scale).reshape(seq_count, BLK, HEADS, HEAD)
    key_in = (owned[1] * mix_scale).reshape(seq_count, BLK, HEADS, HEAD)
    value = (owned[2] * mix_scale).reshape(seq_count, BLK, HEADS, HEAD)
    gating = (owned[3] * mix_scale).reshape(seq_count, BLK, HEADS, HEAD)
    write_pre = (
        jnp.dot(own_scaled, write_weight, preferred_element_type=jnp.float32) * mix_scale
    ).reshape(seq_count, BLK, HEADS)
    forget_pre = (
        jnp.dot(own_scaled, forget_weight, preferred_element_type=jnp.float32) * mix_scale
    ).reshape(seq_count, BLK, HEADS)
    positions = jnp.arange(BLK, dtype=jnp.int32)
    live = (positions[None, :] < lengths[:, None]).astype(jnp.float32)
    mixed_heads, new_state = delta_block(
        query, key_in, value, gating, write_pre, forget_pre, forget_rate, live, state
    )
    half_cols = mixed_heads.shape[1] // 2
    portion = lax.all_gather(mixed_heads, ("kv", "tp"), axis=0, tiled=True)
    first_half = jnp.dot(
        portion[:, :half_cols], out_weight[:half_cols], preferred_element_type=jnp.float32
    ).astype(jnp.bfloat16)
    second_half = jnp.dot(
        portion[:, half_cols:], out_weight[half_cols:], preferred_element_type=jnp.float32
    ).astype(jnp.bfloat16)
    first_half, second_half = lax.optimization_barrier((first_half, second_half))
    mixed_sum = first_half.astype(jnp.float32) + second_half.astype(jnp.float32)
    after_mix = (after_first.astype(jnp.float32) + mixed_sum).astype(jnp.bfloat16)
    mixed_out = feed_forward(after_mix, gain_second, second_gate, second_up, second_down)
    return (mixed_out, new_state)


VMEM_SPEC = pl.BlockSpec(memory_space=pltpu.VMEM)
HBM_SPEC = pl.BlockSpec(memory_space=pltpu.HBM)
GROUP = ("kv", "tp")
F32, BF16 = jnp.float32, jnp.bfloat16


def call(body, out_shapes, args, in_specs=None, scratch=(), limit=5 << 20, out_specs=None):
    single = not isinstance(out_shapes, (list, tuple))
    shapes = [out_shapes] if single else list(out_shapes)
    outs = pl.pallas_call(
        body,
        out_shape=shapes,
        in_specs=in_specs or [VMEM_SPEC] * len(args),
        out_specs=out_specs or [VMEM_SPEC] * len(shapes),
        scratch_shapes=list(scratch),
        compiler_params=pltpu.CompilerParams(vmem_limit_bytes=limit),
    )(*args)
    return outs[0] if single else outs


def my_index():
    return lax.axis_index("kv") * lax.axis_size("tp") + lax.axis_index("tp")


def swap(value, mask, count):
    return lax.ppermute(value, GROUP, [(i, i ^ mask) for i in range(count)])


def far_swaps(sends, count):
    received = []
    for step, send in enumerate(sends):
        received.append(swap(send, 2 * (step + 1), count))
    return received


def pair_up(near, count):
    blocks = []
    for block in near:
        blocks += [block, swap(block, 1, count)]
    return blocks


def gather_blocks(own, count):
    near = [own] + far_swaps([own] * (count // 2 - 1), count)
    return pair_up(near, count)


def entry_kernel(tokens_hbm, gate_hbm, up_hbm, down_hbm, tokens_ref, sem):
    copy = pltpu.make_async_copy(tokens_hbm, tokens_ref, sem)
    copy.start()
    copy.wait()


def enter(tokens, *weights):
    arrays = [pltpu.with_memory_space_constraint(a, pltpu.HBM) for a in (tokens, *weights)]
    return call(
        entry_kernel,
        pltpu.VMEM(tokens.shape, tokens.dtype),
        arrays,
        in_specs=[HBM_SPEC] * len(arrays),
        scratch=[pltpu.SemaphoreType.DMA],
        limit=1 << 20,
    )


def core_span(units):
    tiles = units // 128
    span = -(-tiles // 2) * 128
    return span, units - span


def assemble(blocks, index, gain_ref, scaled_ref):
    width = blocks[0].shape[1]
    squares = None
    for mask, block in enumerate(blocks):
        values = block[...].astype(F32)
        owner = index ^ mask
        column = pl.multiple_of(owner * width, width)
        gain = gain_ref[:, pl.ds(column, width)]
        scaled_ref[:, pl.ds(column, width)] = (values * gain).astype(BF16)
        part = values * values
        squares = part if squares is None else squares + part
    total = jnp.sum(squares, axis=1, keepdims=True)
    channels = width * len(blocks)
    return lax.rsqrt(total / channels + EPSILON)


def ffn_kernel(count, span, skip, *refs):
    blocks = refs[:count]
    gain_ref, gate_ref, up_ref, down_ref = refs[count : count + 4]
    own_ref, cross_ref, scaled, hidden_ref = refs[count + 4 :]
    index = my_index()
    core = lax.axis_index("tp")
    start = pl.multiple_of(core * skip, 128)
    width = blocks[0].shape[1]
    row_scale = assemble(blocks, index, gain_ref, scaled)
    lhs = scaled[...]
    repeated = core * (lax.axis_size("tp") * span - down_ref.shape[0])
    for first in range(0, span, 256):
        size = min(256, span - first)
        columns = pl.ds(pl.multiple_of(start + first, 128), size)
        gate_act = jnp.dot(lhs, gate_ref[:, columns], preferred_element_type=F32) * row_scale
        up_act = jnp.dot(lhs, up_ref[:, columns], preferred_element_type=F32) * row_scale
        hidden = gate_act * jax.nn.sigmoid(gate_act) * up_act
        unit = lax.broadcasted_iota(jnp.int32, hidden.shape, 1) + first
        hidden_ref[:, first : first + size] = jnp.where(unit >= repeated, hidden, 0.0).astype(BF16)
    hidden = hidden_ref[...]
    for mask in list(range(1, count, 2)) + list(range(0, count, 2)):
        column = pl.multiple_of((index ^ mask) * width, width)
        weight = down_ref[pl.ds(start, span), pl.ds(column, width)]
        part = jnp.dot(hidden, weight, preferred_element_type=F32)
        if mask % 2:
            cross_ref[mask // 2] = part.astype(BF16)
        else:
            own_ref[mask // 2] = part


def pair_sum_kernel(own_ref, cross_ref, mine_ref, *sends):
    mine_ref[...] = own_ref[0] + cross_ref[0].astype(F32)
    for step, send in enumerate(sends):
        send[...] = (own_ref[step + 1] + cross_ref[step + 1].astype(F32)).astype(BF16)


def residual_kernel(base_ref, mine_ref, *refs):
    total = mine_ref[...]
    for received in refs[:-1]:
        total = total + received[...].astype(F32)
    refs[-1][...] = (base_ref[...].astype(F32) + 0.5 * total).astype(BF16)


def half_step(own, count, gain, gate, up, down, last=False):
    rows, width = own.shape
    near = count // 2
    span, skip = core_span(down.shape[0])
    blocks = gather_blocks(own, count)
    own_part, cross_part = call(
        functools.partial(ffn_kernel, count, span, skip),
        [pltpu.VMEM((near, rows, width), F32), pltpu.VMEM((near, rows, width), BF16)],
        [*blocks, gain.reshape(1, count * width), gate, up, down],
        scratch=[pltpu.VMEM((rows, width * count), BF16), pltpu.VMEM((rows, span), BF16)],
    )
    cross_sum = swap(cross_part, 1, count)
    mine, *sends = call(
        pair_sum_kernel,
        [pltpu.VMEM((rows, width), F32)] + [pltpu.VMEM((rows, width), BF16)] * (near - 1),
        [own_part, cross_sum],
    )
    received = far_swaps(sends, count)
    shape = jax.ShapeDtypeStruct if last else pltpu.VMEM
    return call(residual_kernel, shape((rows, width), BF16), [own, mine, *received])


def project_kernel(count, *refs):
    blocks = refs[:count]
    gain_ref, query_w, key_w, value_w, gating_w, write_t, forget_t = refs[count : count + 7]
    *sends, pre_ref, scaled, result, pre_scratch = refs[count + 7 :]
    index = my_index()
    row_scale = assemble(blocks, index, gain_ref, scaled)
    lhs = scaled[...]
    width = query_w.shape[1]
    for place, weight in enumerate((query_w, key_w, value_w, gating_w)):
        part = jnp.dot(lhs, weight[...], preferred_element_type=F32)
        result[:, place * width : (place + 1) * width] = part * row_scale
    heads = write_t.shape[0]
    contract = (((1,), (1,)), ((), ()))
    for place, weight in enumerate((write_t, forget_t)):
        part = lax.dot_general(lhs, weight[...], contract, preferred_element_type=F32)
        pre_scratch[:, place * heads : (place + 1) * heads] = part * row_scale
    for step, send in enumerate(sends):
        rows = send.shape[0]
        row = pl.multiple_of((lax.axis_index("kv") ^ step) * rows, rows)
        send[...] = result[pl.ds(row, rows), :].astype(BF16)
    row = pl.multiple_of(index * BLK, BLK)
    pre_ref[...] = pre_scratch[pl.ds(row, BLK), :]


def parts(value):
    high = value.astype(BF16)
    return high, (value - high.astype(F32)).astype(BF16)


def dot_parts(left, right, dims=(((1,), (0,)), ((), ()))):
    left_high, left_low = left
    right_high, right_low = right
    total = lax.dot_general(left_high, right_low, dims, preferred_element_type=F32)
    total = total + lax.dot_general(left_low, right_high, dims, preferred_element_type=F32)
    return total + lax.dot_general(left_high, right_high, dims, preferred_element_type=F32)


def delta_kernel(count, *refs):
    blocks = refs[:count]
    pre_ref, rate_ref, length_ref, state_ref = refs[count : count + 4]
    mixed_ref, update_ref, faded_ref, final_ref, ordered = refs[count + 4 :]
    index = my_index()
    first_core = lax.axis_index("tp") == 0
    for mask, block in enumerate(blocks):
        both = block[...].astype(F32)
        ordered[pl.ds(index ^ mask, 1)] = jnp.where(first_core, both[:BLK], both[BLK:])[None]
    heads = rate_ref.shape[1]
    size = state_ref.shape[-1]
    per_block = heads // count
    rows = heads * BLK
    width = per_block * size

    def stack(place):
        found = []
        for head in range(heads):
            column = place * width + (head % per_block) * size
            found.append(ordered[head // per_block, :, column : column + size])
        return jnp.concatenate(found, axis=0)

    query, key_in, value, gating = (stack(place) for place in range(4))
    query_unit = query * lax.rsqrt(jnp.sum(query * query, axis=1, keepdims=True) + EPSILON) * (1.0 / math.sqrt(size))
    key_unit = key_in * lax.rsqrt(jnp.sum(key_in * key_in, axis=1, keepdims=True) + EPSILON)
    step_of = lax.broadcasted_iota(jnp.int32, (BLK, heads), 0)
    live = (step_of < length_ref[0]).astype(F32)
    pre = pre_ref[...]
    write_gate = jax.nn.sigmoid(pre[:, :heads]) * live
    forget_in = pre[:, heads:]
    softplus = jnp.maximum(forget_in, 0.0) + jnp.log1p(jnp.exp(-jnp.abs(forget_in)))
    forget = -jnp.exp(rate_ref[...]) * softplus * live
    cumulative = forget
    lower = 1
    while lower < BLK:
        moved = pltpu.roll(cumulative, lower, 0)
        cumulative = cumulative + jnp.where(step_of >= lower, moved, 0.0)
        lower *= 2
    final = jnp.broadcast_to(cumulative[BLK - 1 :, :], (BLK, heads))
    row_head = lax.broadcasted_iota(jnp.int32, (rows, heads), 0) // BLK
    picked = row_head == lax.broadcasted_iota(jnp.int32, (rows, heads), 1)

    def column_of(array):
        tall = jnp.concatenate([array] * heads, axis=0)
        return jnp.sum(jnp.where(picked, tall, 0.0), axis=1, keepdims=True)

    write_col, live_col = column_of(write_gate), column_of(live)
    cum_col, final_col = column_of(cumulative), column_of(final)
    down_at = lax.broadcasted_iota(jnp.int32, (rows, rows), 0)
    over_at = lax.broadcasted_iota(jnp.int32, (rows, rows), 1)
    same = (down_at // BLK) == (over_at // BLK)
    diagonal = down_at == over_at
    cum_row = jnp.sum(jnp.where(diagonal, cum_col, 0.0), axis=0, keepdims=True)
    causal = same & (down_at >= over_at)
    decay = jnp.where(causal, jnp.exp(jnp.minimum(cum_col - cum_row, 0.0)), 0.0)
    across = (((1,), (1,)), ((), ()))
    key_parts = parts(key_unit)
    strict_part = jnp.where(diagonal, 0.0, write_col * decay * dot_parts(key_parts, key_parts, across))
    scores = decay * dot_parts(parts(query_unit), key_parts, across)
    identity = diagonal.astype(F32)
    strict_split = parts(strict_part)
    squared = dot_parts(strict_split, strict_split)
    squared_split = parts(squared)
    fourth = dot_parts(squared_split, squared_split)
    inverse = identity - strict_part + squared - dot_parts(strict_split, squared_split)
    inverse = inverse + dot_parts(parts(inverse), parts(fourth))
    growth = jnp.exp(cum_col)
    key_grown, query_grown = key_unit * growth, query_unit * growth
    from_key, from_query = [], []
    for head in range(heads):
        at = slice(head * BLK, (head + 1) * BLK)
        both = jnp.concatenate([key_grown[at], query_grown[at]], axis=0)
        found = dot_parts(parts(both), parts(state_ref[head]))
        from_key.append(found[:BLK])
        from_query.append(found[BLK:])
    target = write_col * (value - jnp.concatenate(from_key, axis=0))
    update = dot_parts(parts(inverse), parts(target))
    attend = jnp.concatenate(from_query, axis=0) + dot_parts(parts(scores), parts(update))
    normed = attend * lax.rsqrt(jnp.mean(attend * attend, axis=1, keepdims=True) + EPSILON)
    normed = (normed * (gating * jax.nn.sigmoid(gating)) * live_col).astype(BF16)
    for head in range(heads):
        mixed_ref[:, head * size : (head + 1) * size] = normed[head * BLK : (head + 1) * BLK]
    update_ref[...] = update
    faded_ref[...] = key_unit * jnp.exp(final_col - cum_col)
    final_ref[...] = jnp.broadcast_to(jnp.exp(final_col), final_ref.shape)


def state_kernel(update_ref, faded_ref, final_ref, state_ref, new_ref):
    heads = state_ref.shape[0]
    along = (((0,), (0,)), ((), ()))
    for head in range(heads):
        at = slice(head * BLK, (head + 1) * BLK)
        left_high, left_low = parts(faded_ref[at])
        right_high, right_low = parts(update_ref[at])
        left = jnp.concatenate([left_high, left_high, left_low, left_low], axis=0)
        right = jnp.concatenate([right_high, right_low, right_high, right_low], axis=0)
        grown = lax.dot_general(left, right, along, preferred_element_type=F32)
        scale = final_ref[head * BLK : head * BLK + 1, :]
        new_ref[head] = scale * state_ref[head] + grown


def out_kernel(count, *refs):
    blocks = refs[:count]
    weight_ref, base_ref, out_ref, scratch = refs[count:]
    index = my_index()
    lhs = jnp.concatenate([block[...].astype(F32) for block in blocks], axis=0).astype(BF16)
    half = lhs.shape[1] // 2
    first = jnp.dot(lhs[:, :half], weight_ref[:half, :], preferred_element_type=F32).astype(BF16)
    second = jnp.dot(lhs[:, half:], weight_ref[half:, :], preferred_element_type=F32).astype(BF16)
    total = first.astype(F32) + second.astype(F32)
    for mask in range(count):
        row = pl.multiple_of((index ^ mask) * BLK, BLK)
        scratch[pl.ds(row, BLK), :] = total[mask * BLK : (mask + 1) * BLK]
    out_ref[...] = (base_ref[...].astype(F32) + scratch[...]).astype(BF16)


def group_device(
    tokens,
    lengths,
    state,
    gain_first,
    first_gate,
    first_up,
    first_down,
    gain_mix,
    query_weight,
    key_weight,
    value_weight,
    gating_weight,
    write_weight,
    forget_weight,
    forget_rate,
    out_weight,
    gain_second,
    second_gate,
    second_up,
    second_down,
):
    count = lax.axis_size("kv") * lax.axis_size("tp")
    rows, width = tokens.shape
    channels = gain_first.shape[0]
    heads, size = state.shape[1], state.shape[2]
    tokens = enter(tokens, first_gate, first_up, first_down)
    after_first = half_step(tokens, count, gain_first, first_gate, first_up, first_down)
    blocks = gather_blocks(after_first, count)
    weights = (query_weight, key_weight, value_weight, gating_weight)
    columns = 4 * width
    near = count // 2
    *sends, pre = call(
        functools.partial(project_kernel, count),
        [pltpu.VMEM((rows // near, columns), BF16)] * near + [pltpu.VMEM((BLK, 2 * heads), F32)],
        [*blocks, gain_mix.reshape(1, channels), *weights, write_weight.T, forget_weight.T],
        scratch=[
            pltpu.VMEM((rows, channels), BF16),
            pltpu.VMEM((rows, columns), F32),
            pltpu.VMEM((rows, 2 * heads), F32),
        ],
    )
    owned = pair_up([sends[0]] + far_swaps(sends[1:], count), count)
    matrices = state.reshape(heads, size, size)
    mixed, update, faded, final = call(
        functools.partial(delta_kernel, count),
        [
            pltpu.VMEM((BLK, channels), BF16),
            pltpu.VMEM((heads * BLK, size), F32),
            pltpu.VMEM((heads * BLK, size), F32),
            pltpu.VMEM((heads * BLK, size), F32),
        ],
        [*owned, pre, forget_rate.reshape(1, heads), lengths, matrices],
        in_specs=[VMEM_SPEC] * (count + 2) + [pl.BlockSpec(memory_space=pltpu.SMEM), VMEM_SPEC],
        scratch=[pltpu.VMEM((count, BLK, columns), F32)],
    )
    head_blocks = gather_blocks(mixed, count)
    new_state = call(
        state_kernel,
        jax.ShapeDtypeStruct((heads, size, size), F32),
        [update, faded, final, matrices],
    )
    after_mix = call(
        functools.partial(out_kernel, count),
        pltpu.VMEM((rows, width), BF16),
        [*head_blocks, out_weight, after_first],
        scratch=[pltpu.VMEM((rows, width), F32)],
    )
    mixed_out = half_step(
        after_mix, count, gain_second, second_gate, second_up, second_down, last=True
    )
    return (mixed_out, new_state.reshape(state.shape))


def fits_group(mesh):
    near, cores = mesh.shape["kv"], mesh.shape["tp"]
    count = near * cores
    return cores == 2 and near & (near - 1) == 0 and near <= 8 and (HEADS * HEAD) % (count * 128) == 0


def per_device(mesh, *arrays):
    lengths, gate = arrays[1], arrays[4]
    suits = fits_group(mesh) and lengths.shape[0] == 1 and gate.shape[1] % 128 == 0
    if not suits:
        return general_device(*arrays)
    return group_device(*arrays)


def solution(mesh):
    in_specs = (
        P("dp", ("kv", "tp")),
        P(("dp", "kv", "tp")),
        P(("dp", "kv", "tp"), None, None, None),
        P(),
        P(None, "kv"),
        P(None, "kv"),
        P("kv", None),
        P(),
        P(None, ("kv", "tp")),
        P(None, ("kv", "tp")),
        P(None, ("kv", "tp")),
        P(None, ("kv", "tp")),
        P(),
        P(),
        P(),
        P(None, ("kv", "tp")),
        P(),
        P(None, "kv"),
        P(None, "kv"),
        P("kv", None),
    )
    out_specs = (P("dp", ("kv", "tp")), P(("dp", "kv", "tp"), None, None, None))
    return jax.shard_map(
        functools.partial(per_device, mesh),
        mesh=mesh,
        in_specs=in_specs,
        out_specs=out_specs,
        check_vma=False,
    )
```

```python
import functools
import math

import jax
import jax.numpy as jnp
from jax import lax
from jax.experimental import pallas as pl
from jax.experimental.pallas import tpu as pltpu
from jax.sharding import PartitionSpec as P


HEADS = 16
HEAD = 128
BLK = 8


EPSILON = 1e-06


def fold_step(gain, gate_cols, up_cols, portion):
    values = portion.astype(jnp.float32)
    scaled = (values * gain).astype(jnp.bfloat16)
    gate_acc = jnp.dot(scaled, gate_cols, preferred_element_type=jnp.float32)
    up_acc = jnp.dot(scaled, up_cols, preferred_element_type=jnp.float32)
    squares = jnp.sum(values * values, axis=1)
    return (gate_acc, up_acc, squares)


def finish_units(gate_acc, up_acc, squares, channels, down_rows):
    row_scale = lax.rsqrt(squares / channels + EPSILON)[:, None]
    hidden = (jax.nn.silu(gate_acc * row_scale) * (up_acc * row_scale)).astype(jnp.bfloat16)
    return jnp.dot(hidden, down_rows, preferred_element_type=jnp.float32)


def feed_forward(hidden_in, gain, w_gate, w_up, w_down):
    channels = gain.shape[0]
    paired = lax.all_to_all(hidden_in, "tp", split_axis=0, concat_axis=1, tiled=True)
    gate_acc, up_acc, squares = fold_step(
        gain, w_gate, w_up, lax.all_gather(paired, "kv", axis=1, tiled=True)
    )
    ffn_term = finish_units(gate_acc, up_acc, squares, channels, w_down)
    partial_value = lax.psum_scatter(ffn_term, "kv", scatter_dimension=1, tiled=True)
    summed = lax.all_to_all(partial_value, "tp", split_axis=1, concat_axis=0, tiled=True)
    return (hidden_in.astype(jnp.float32) + 0.5 * summed).astype(jnp.bfloat16)


def delta_block(query, key_in, value, gating, write_pre, forget_pre, rates, live, state):
    seq_count, block_len, head_count, head_size = query.shape
    precise = lax.Precision.HIGHEST
    query_unit = (
        query
        * lax.rsqrt(jnp.sum(query * query, axis=-1, keepdims=True) + EPSILON)
        / math.sqrt(head_size)
    )
    key_unit = key_in * lax.rsqrt(jnp.sum(key_in * key_in, axis=-1, keepdims=True) + EPSILON)
    live_rows = live[:, :, None]
    write_gate = jax.nn.sigmoid(write_pre) * live_rows
    forget = -jnp.exp(rates)[None, None, :] * jax.nn.softplus(forget_pre) * live_rows
    cumulative = jnp.cumsum(forget, axis=1)
    cum_heads = jnp.transpose(cumulative, (0, 2, 1))
    positions = jnp.arange(block_len)
    causal = positions[:, None] >= positions[None, :]
    strict = positions[:, None] > positions[None, :]
    differ = jnp.minimum(cum_heads[:, :, :, None] - cum_heads[:, :, None, :], 0.0)
    decay_mat = jnp.where(causal, jnp.exp(differ), 0.0)
    key_dots = jnp.einsum("sthd,suhd->shtu", key_unit, key_unit, precision=precise)
    write_heads = jnp.transpose(write_gate, (0, 2, 1))
    strict_part = jnp.where(strict, write_heads[:, :, :, None] * decay_mat * key_dots, 0.0)
    identity = jnp.eye(block_len, dtype=jnp.float32)
    squared = jnp.einsum("shtu,shuv->shtv", strict_part, strict_part, precision=precise)
    fourth = jnp.einsum("shtu,shuv->shtv", squared, squared, precision=precise)
    inverse = jnp.einsum(
        "shtu,shuv->shtv", identity - strict_part, identity + squared, precision=precise
    )
    inverse = jnp.einsum("shtu,shuv->shtv", inverse, identity + fourth, precision=precise)
    growth = jnp.exp(cumulative)
    target = jnp.einsum(
        "shtu,suhv->sthv", inverse, write_gate[..., None] * value, precision=precise
    )
    key_mix = jnp.einsum(
        "shtu,suhk->sthk", inverse, (write_gate * growth)[..., None] * key_unit, precision=precise
    )
    update = target - jnp.einsum("sthk,shkv->sthv", key_mix, state, precision=precise)
    scores = jnp.einsum("sthd,suhd->shtu", query_unit, key_unit, precision=precise) * decay_mat
    attend = jnp.einsum("sthk,shkv->sthv", query_unit * growth[..., None], state, precision=precise)
    attend = attend + jnp.einsum("shtu,suhv->sthv", scores, update, precision=precise)
    final_cum = cumulative[:, -1:, :]
    fading = jnp.exp(final_cum - cumulative)
    new_state = jnp.exp(final_cum[:, 0, :])[:, :, None, None] * state
    new_state = new_state + jnp.einsum(
        "sthk,sthv->shkv", key_unit * fading[..., None], update, precision=precise
    )
    normed = attend * lax.rsqrt(jnp.mean(attend * attend, axis=-1, keepdims=True) + EPSILON)
    normed = normed * jax.nn.silu(gating) * live[:, :, None, None]
    mixed_heads = normed.reshape(seq_count * block_len, head_count * head_size).astype(jnp.bfloat16)
    return (mixed_heads, new_state)


def general_device(
    tokens,
    lengths,
    state,
    gain_first,
    first_gate,
    first_up,
    first_down,
    gain_mix,
    query_weight,
    key_weight,
    value_weight,
    gating_weight,
    write_weight,
    forget_weight,
    forget_rate,
    out_weight,
    gain_second,
    second_gate,
    second_up,
    second_down,
):
    after_first = feed_forward(tokens, gain_first, first_gate, first_up, first_down)
    seq_count = lengths.shape[0]
    own_count = seq_count * BLK
    whole_rows = lax.all_gather(after_first, ("kv", "tp"), axis=1, tiled=True)
    scaled_all = (whole_rows.astype(jnp.float32) * gain_mix).astype(jnp.bfloat16)
    stacked = jnp.stack(
        [
            jnp.dot(scaled_all, matrix, preferred_element_type=jnp.float32)
            for matrix in (query_weight, key_weight, value_weight, gating_weight)
        ]
    )
    owned = lax.all_to_all(
        stacked.astype(jnp.bfloat16), ("kv", "tp"), split_axis=1, concat_axis=2, tiled=True
    ).astype(stacked.dtype)
    row_start = lax.axis_index(("kv", "tp")) * own_count
    own_values = lax.dynamic_slice_in_dim(whole_rows, row_start, own_count, 0).astype(jnp.float32)
    own_scaled = lax.dynamic_slice_in_dim(scaled_all, row_start, own_count, 0)
    mix_scale = lax.rsqrt(jnp.mean(own_values * own_values, axis=1, keepdims=True) + EPSILON)
    query = (owned[0] * mix_scale).reshape(seq_count, BLK, HEADS, HEAD)
    key_in = (owned[1] * mix_scale).reshape(seq_count, BLK, HEADS, HEAD)
    value = (owned[2] * mix_scale).reshape(seq_count, BLK, HEADS, HEAD)
    gating = (owned[3] * mix_scale).reshape(seq_count, BLK, HEADS, HEAD)
    write_pre = (
        jnp.dot(own_scaled, write_weight, preferred_element_type=jnp.float32) * mix_scale
    ).reshape(seq_count, BLK, HEADS)
    forget_pre = (
        jnp.dot(own_scaled, forget_weight, preferred_element_type=jnp.float32) * mix_scale
    ).reshape(seq_count, BLK, HEADS)
    positions = jnp.arange(BLK, dtype=jnp.int32)
    live = (positions[None, :] < lengths[:, None]).astype(jnp.float32)
    mixed_heads, new_state = delta_block(
        query, key_in, value, gating, write_pre, forget_pre, forget_rate, live, state
    )
    half_cols = mixed_heads.shape[1] // 2
    portion = lax.all_gather(mixed_heads, ("kv", "tp"), axis=0, tiled=True)
    first_half = jnp.dot(
        portion[:, :half_cols], out_weight[:half_cols], preferred_element_type=jnp.float32
    ).astype(jnp.bfloat16)
    second_half = jnp.dot(
        portion[:, half_cols:], out_weight[half_cols:], preferred_element_type=jnp.float32
    ).astype(jnp.bfloat16)
    first_half, second_half = lax.optimization_barrier((first_half, second_half))
    mixed_sum = first_half.astype(jnp.float32) + second_half.astype(jnp.float32)
    after_mix = (after_first.astype(jnp.float32) + mixed_sum).astype(jnp.bfloat16)
    mixed_out = feed_forward(after_mix, gain_second, second_gate, second_up, second_down)
    return (mixed_out, new_state)


VMEM_SPEC = pl.BlockSpec(memory_space=pltpu.VMEM)
HBM_SPEC = pl.BlockSpec(memory_space=pltpu.HBM)
GROUP = ("kv", "tp")
F32, BF16 = jnp.float32, jnp.bfloat16


def call(body, out_shapes, args, in_specs=None, scratch=(), limit=5 << 20, out_specs=None):
    single = not isinstance(out_shapes, (list, tuple))
    shapes = [out_shapes] if single else list(out_shapes)
    outs = pl.pallas_call(
        body,
        out_shape=shapes,
        in_specs=in_specs or [VMEM_SPEC] * len(args),
        out_specs=out_specs or [VMEM_SPEC] * len(shapes),
        scratch_shapes=list(scratch),
        compiler_params=pltpu.CompilerParams(vmem_limit_bytes=limit),
    )(*args)
    return outs[0] if single else outs


def my_index():
    return lax.axis_index("kv") * lax.axis_size("tp") + lax.axis_index("tp")


def swap(value, mask, count):
    return lax.ppermute(value, GROUP, [(i, i ^ mask) for i in range(count)])


def far_swaps(sends, count):
    received = []
    for step, send in enumerate(sends):
        received.append(swap(send, 2 * (step + 1), count))
    return received


def pair_up(near, count):
    blocks = []
    for block in near:
        blocks += [block, swap(block, 1, count)]
    return blocks


def gather_blocks(own, count):
    near = [own] + far_swaps([own] * (count // 2 - 1), count)
    return pair_up(near, count)


def entry_kernel(gate_hbm, up_hbm, down_hbm, mark_ref):
    mark_ref[...] = jnp.zeros_like(mark_ref)


def enter(*weights):
    arrays = [pltpu.with_memory_space_constraint(a, pltpu.HBM) for a in weights]
    return call(
        entry_kernel,
        pltpu.VMEM((8, 128), F32),
        arrays,
        in_specs=[HBM_SPEC] * len(arrays),
        limit=1 << 20,
    )


def core_span(units):
    tiles = units // 128
    span = -(-tiles // 2) * 128
    return span, units - span


def gained(block, owner, gain_ref):
    width = block.shape[1]
    column = pl.multiple_of(owner * width, width)
    values = block[...].astype(F32)
    squares = values * values
    folded = squares[:, :128]
    for first in range(128, width, 128):
        folded = folded + squares[:, first : first + 128]
    return (values * gain_ref[:, pl.ds(column, width)]).astype(BF16), folded


def scale_of_rows(folded, channels):
    return lax.rsqrt(jnp.sum(folded, axis=1, keepdims=True) / channels + EPSILON)


def plus(total, part):
    return part if total is None else total + part


def early_masks(count):
    late = (3, 5) if count > 4 else (3,)
    return [m for m in range(count) if m not in late], list(late)


def entry_kernel(gate_hbm, up_hbm, down_hbm, mark_ref):
    mark_ref[...] = jnp.zeros_like(mark_ref)


def enter(*weights):
    arrays = [pltpu.with_memory_space_constraint(a, pltpu.HBM) for a in weights]
    return call(
        entry_kernel,
        pltpu.VMEM((8, 128), F32),
        arrays,
        in_specs=[HBM_SPEC] * len(arrays),
        limit=1 << 20,
    )


def core_span(units):
    tiles = units // 128
    span = -(-tiles // 2) * 128
    return span, units - span


def units_of(blocks, masks, gain_ref, gate_ref, up_ref, span, skip):
    index = my_index()
    start = pl.multiple_of(lax.axis_index("tp") * skip, 128)
    gate_acc = up_acc = squares = None
    for mask, block in zip(masks, blocks):
        owner = index ^ mask
        width = block.shape[1]
        rows = pl.ds(pl.multiple_of(owner * width, width), width)
        lhs, folded = gained(block, owner, gain_ref)
        squares = plus(squares, folded)
        columns = pl.ds(start, span)
        gate_acc = plus(gate_acc, jnp.dot(lhs, gate_ref[rows, columns], preferred_element_type=F32))
        up_acc = plus(up_acc, jnp.dot(lhs, up_ref[rows, columns], preferred_element_type=F32))
    return gate_acc, up_acc, squares


def ffn_early_kernel(masks, span, skip, *refs):
    blocks = refs[: len(masks)]
    gain_ref, gate_ref, up_ref, _, _, gate_out, up_out, squares_out = refs[len(masks) :]
    gate_out[...], up_out[...], squares_out[...] = units_of(
        blocks, masks, gain_ref, gate_ref, up_ref, span, skip
    )


def ffn_late_kernel(masks, count, span, skip, *refs):
    blocks = refs[: len(masks)]
    gain_ref, gate_ref, up_ref, down_ref, gate_in, up_in, squares_in = refs[len(masks) : len(masks) + 7]
    hidden_ref, cross_ref = refs[len(masks) + 7 :]
    gate_acc, up_acc, squares = units_of(blocks, masks, gain_ref, gate_ref, up_ref, span, skip)
    channels = gate_ref.shape[0]
    row_scale = scale_of_rows(squares + squares_in[...], channels)
    gate_act = (gate_acc + gate_in[...]) * row_scale
    hidden = gate_act * jax.nn.sigmoid(gate_act) * ((up_acc + up_in[...]) * row_scale)
    repeated = lax.axis_index("tp") * (lax.axis_size("tp") * span - down_ref.shape[0])
    unit = lax.broadcasted_iota(jnp.int32, hidden.shape, 1)
    hidden_ref[...] = jnp.where(unit >= repeated, hidden, 0.0).astype(BF16)
    hidden = hidden_ref[...]
    down_products(hidden, down_ref, range(1, count, 2), cross_ref, skip)


def down_products(hidden, down_ref, masks, out_ref, skip):
    index = my_index()
    start = pl.multiple_of(lax.axis_index("tp") * skip, 128)
    span, width = hidden.shape[1], out_ref.shape[2]
    for place, mask in enumerate(masks):
        column = pl.multiple_of((index ^ mask) * width, width)
        weight = down_ref[pl.ds(start, span), pl.ds(column, width)]
        out_ref[place] = jnp.dot(hidden, weight, preferred_element_type=F32).astype(out_ref.dtype)


def ffn_own_kernel(count, skip, hidden_ref, down_ref, own_ref):
    down_products(hidden_ref[...], down_ref, range(0, count, 2), own_ref, skip)


def pair_sum_kernel(own_ref, cross_ref, mine_ref, *sends):
    mine_ref[...] = own_ref[0] + cross_ref[0].astype(F32)
    for step, send in enumerate(sends):
        send[...] = (own_ref[step + 1] + cross_ref[step + 1].astype(F32)).astype(BF16)


def residual_kernel(base_ref, mine_ref, *refs):
    total = mine_ref[...]
    for received in refs[:-1]:
        total = total + received[...].astype(F32)
    refs[-1][...] = (base_ref[...].astype(F32) + 0.5 * total).astype(BF16)


def half_step(own, mark, count, gain, gate, up, down, last=False):
    rows, width = own.shape
    near = count // 2
    span, skip = core_span(down.shape[0])
    blocks = gather_blocks(own, count)
    gain = gain.reshape(1, count * width)
    early, late = early_masks(count)
    parts_early = call(
        functools.partial(ffn_early_kernel, early, span, skip),
        [pltpu.VMEM((rows, span), F32)] * 2 + [pltpu.VMEM((rows, 128), F32)],
        [*(blocks[m] for m in early), gain, gate, up, down, mark],
    )
    hidden, cross_part = call(
        functools.partial(ffn_late_kernel, late, count, span, skip),
        [pltpu.VMEM((rows, span), BF16), pltpu.VMEM((near, rows, width), BF16)],
        [*(blocks[m] for m in late), gain, gate, up, down, *parts_early],
    )
    cross_sum = swap(cross_part, 1, count)
    own_part = call(
        functools.partial(ffn_own_kernel, count, skip),
        pltpu.VMEM((near, rows, width), F32),
        [hidden, down],
    )
    mine, *sends = call(
        pair_sum_kernel,
        [pltpu.VMEM((rows, width), F32)] + [pltpu.VMEM((rows, width), BF16)] * (near - 1),
        [own_part, cross_sum],
    )
    received = far_swaps(sends, count)
    shape = jax.ShapeDtypeStruct if last else pltpu.VMEM
    return call(residual_kernel, shape((rows, width), BF16), [own, mine, *received])


def mixes_of(blocks, masks, gain_ref, weights, thin):
    index = my_index()
    wide = [None] * len(weights)
    narrow = [None] * len(thin)
    squares = None
    across = (((1,), (1,)), ((), ()))
    for mask, block in zip(masks, blocks):
        owner = index ^ mask
        width = block.shape[1]
        rows = pl.ds(pl.multiple_of(owner * width, width), width)
        lhs, folded = gained(block, owner, gain_ref)
        squares = plus(squares, folded)
        for place, weight in enumerate(weights):
            wide[place] = plus(wide[place], jnp.dot(lhs, weight[rows, :], preferred_element_type=F32))
        for place, weight in enumerate(thin):
            part = lax.dot_general(lhs, weight[:, rows], across, preferred_element_type=F32)
            narrow[place] = plus(narrow[place], part)
    return wide, narrow, squares


def project_early_kernel(masks, *refs):
    blocks = refs[: len(masks)]
    gain_ref, *weights = refs[len(masks) : len(masks) + 7]
    result, pre, squares_out = refs[len(masks) + 7 :]
    wide, narrow, squares_out[...] = mixes_of(blocks, masks, gain_ref, weights[:4], weights[4:])
    for place, part in enumerate(wide):
        width = part.shape[1]
        result[:, place * width : (place + 1) * width] = part
    for place, part in enumerate(narrow):
        width = part.shape[1]
        pre[:, place * width : (place + 1) * width] = part


def project_late_kernel(masks, *refs):
    blocks = refs[: len(masks)]
    gain_ref, *weights = refs[len(masks) : len(masks) + 7]
    result_in, pre_in, squares_in = refs[len(masks) + 7 : len(masks) + 10]
    *sends, pre_ref, result, pre_scratch = refs[len(masks) + 10 :]
    wide, narrow, squares = mixes_of(blocks, masks, gain_ref, weights[:4], weights[4:])
    row_scale = scale_of_rows(squares + squares_in[...], weights[0].shape[0])
    for place, part in enumerate(wide):
        width = part.shape[1]
        columns = slice(place * width, (place + 1) * width)
        result[:, columns] = (part + result_in[:, columns]) * row_scale
    for place, part in enumerate(narrow):
        width = part.shape[1]
        columns = slice(place * width, (place + 1) * width)
        pre_scratch[:, columns] = (part + pre_in[:, columns]) * row_scale
    for step, send in enumerate(sends):
        rows = send.shape[0]
        row = pl.multiple_of((lax.axis_index("kv") ^ step) * rows, rows)
        send[...] = result[pl.ds(row, rows), :].astype(BF16)
    row = pl.multiple_of(my_index() * BLK, BLK)
    pre_ref[...] = pre_scratch[pl.ds(row, BLK), :]


def parts(value):
    high = value.astype(BF16)
    return high, (value - high.astype(F32)).astype(BF16)


def dot_parts(left, right, dims=(((1,), (0,)), ((), ()))):
    left_high, left_low = left
    right_high, right_low = right
    total = lax.dot_general(left_high, right_low, dims, preferred_element_type=F32)
    total = total + lax.dot_general(left_low, right_high, dims, preferred_element_type=F32)
    return total + lax.dot_general(left_high, right_high, dims, preferred_element_type=F32)


def delta_kernel(count, *refs):
    blocks = refs[:count]
    pre_ref, rate_ref, length_ref, state_ref = refs[count : count + 4]
    mixed_ref, update_ref, faded_ref, final_ref, ordered = refs[count + 4 :]
    index = my_index()
    first_core = lax.axis_index("tp") == 0
    for mask, block in enumerate(blocks):
        both = block[...].astype(F32)
        ordered[pl.ds(index ^ mask, 1)] = jnp.where(first_core, both[:BLK], both[BLK:])[None]
    heads = rate_ref.shape[1]
    size = state_ref.shape[-1]
    per_block = heads // count
    rows = heads * BLK
    width = per_block * size

    def stack(place):
        found = []
        for head in range(heads):
            column = place * width + (head % per_block) * size
            found.append(ordered[head // per_block, :, column : column + size])
        return jnp.concatenate(found, axis=0)

    query, key_in, value, gating = (stack(place) for place in range(4))
    query_unit = query * lax.rsqrt(jnp.sum(query * query, axis=1, keepdims=True) + EPSILON) * (1.0 / math.sqrt(size))
    key_unit = key_in * lax.rsqrt(jnp.sum(key_in * key_in, axis=1, keepdims=True) + EPSILON)
    step_of = lax.broadcasted_iota(jnp.int32, (BLK, heads), 0)
    live = (step_of < length_ref[...]).astype(F32)
    pre = pre_ref[...]
    write_gate = jax.nn.sigmoid(pre[:, :heads]) * live
    forget_in = pre[:, heads:]
    softplus = jnp.maximum(forget_in, 0.0) + jnp.log1p(jnp.exp(-jnp.abs(forget_in)))
    forget = -jnp.exp(rate_ref[...]) * softplus * live
    cumulative = forget
    lower = 1
    while lower < BLK:
        moved = pltpu.roll(cumulative, lower, 0)
        cumulative = cumulative + jnp.where(step_of >= lower, moved, 0.0)
        lower *= 2
    final = jnp.broadcast_to(cumulative[BLK - 1 :, :], (BLK, heads))
    row_head = lax.broadcasted_iota(jnp.int32, (rows, heads), 0) // BLK
    picked = row_head == lax.broadcasted_iota(jnp.int32, (rows, heads), 1)

    def column_of(array):
        tall = jnp.concatenate([array] * heads, axis=0)
        return jnp.sum(jnp.where(picked, tall, 0.0), axis=1, keepdims=True)

    write_col, live_col = column_of(write_gate), column_of(live)
    cum_col, final_col = column_of(cumulative), column_of(final)
    down_at = lax.broadcasted_iota(jnp.int32, (rows, rows), 0)
    over_at = lax.broadcasted_iota(jnp.int32, (rows, rows), 1)
    same = (down_at // BLK) == (over_at // BLK)
    diagonal = down_at == over_at
    cum_row = jnp.sum(jnp.where(diagonal, cum_col, 0.0), axis=0, keepdims=True)
    causal = same & (down_at >= over_at)
    decay = jnp.where(causal, jnp.exp(jnp.minimum(cum_col - cum_row, 0.0)), 0.0)
    across = (((1,), (1,)), ((), ()))
    key_parts = parts(key_unit)
    strict_part = jnp.where(diagonal, 0.0, write_col * decay * dot_parts(key_parts, key_parts, across))
    scores = decay * dot_parts(parts(query_unit), key_parts, across)
    identity = diagonal.astype(F32)
    strict_split = parts(strict_part)
    squared = dot_parts(strict_split, strict_split)
    squared_split = parts(squared)
    fourth = dot_parts(squared_split, squared_split)
    inverse = identity - strict_part + squared - dot_parts(strict_split, squared_split)
    inverse = inverse + dot_parts(parts(inverse), parts(fourth))
    growth = jnp.exp(cum_col)
    key_grown, query_grown = key_unit * growth, query_unit * growth
    from_key, from_query = [], []
    for head in range(heads):
        at = slice(head * BLK, (head + 1) * BLK)
        both = jnp.concatenate([key_grown[at], query_grown[at]], axis=0)
        found = dot_parts(parts(both), parts(state_ref[head]))
        from_key.append(found[:BLK])
        from_query.append(found[BLK:])
    target = write_col * (value - jnp.concatenate(from_key, axis=0))
    update = dot_parts(parts(inverse), parts(target))
    attend = jnp.concatenate(from_query, axis=0) + dot_parts(parts(scores), parts(update))
    normed = attend * lax.rsqrt(jnp.mean(attend * attend, axis=1, keepdims=True) + EPSILON)
    normed = (normed * (gating * jax.nn.sigmoid(gating)) * live_col).astype(BF16)
    for head in range(heads):
        mixed_ref[:, head * size : (head + 1) * size] = normed[head * BLK : (head + 1) * BLK]
    update_ref[...] = update
    faded_ref[...] = key_unit * jnp.exp(final_col - cum_col)
    final_ref[...] = jnp.broadcast_to(jnp.exp(final_col), final_ref.shape)


def state_kernel(update_ref, faded_ref, final_ref, state_ref, new_ref):
    heads = state_ref.shape[0]
    along = (((0,), (0,)), ((), ()))
    for head in range(heads):
        at = slice(head * BLK, (head + 1) * BLK)
        left_high, left_low = parts(faded_ref[at])
        right_high, right_low = parts(update_ref[at])
        left = jnp.concatenate([left_high, left_high, left_low, left_low], axis=0)
        right = jnp.concatenate([right_high, right_low, right_high, right_low], axis=0)
        grown = lax.dot_general(left, right, along, preferred_element_type=F32)
        scale = final_ref[head * BLK : head * BLK + 1, :]
        new_ref[head] = scale * state_ref[head] + grown


def out_kernel(count, *refs):
    blocks = refs[:count]
    weight_ref, base_ref, out_ref, scratch = refs[count:]
    index = my_index()
    lhs = jnp.concatenate([block[...].astype(F32) for block in blocks], axis=0).astype(BF16)
    half = lhs.shape[1] // 2
    first = jnp.dot(lhs[:, :half], weight_ref[:half, :], preferred_element_type=F32).astype(BF16)
    second = jnp.dot(lhs[:, half:], weight_ref[half:, :], preferred_element_type=F32).astype(BF16)
    total = first.astype(F32) + second.astype(F32)
    for mask in range(count):
        row = pl.multiple_of((index ^ mask) * BLK, BLK)
        scratch[pl.ds(row, BLK), :] = total[mask * BLK : (mask + 1) * BLK]
    out_ref[...] = (base_ref[...].astype(F32) + scratch[...]).astype(BF16)


def group_device(
    tokens,
    lengths,
    state,
    gain_first,
    first_gate,
    first_up,
    first_down,
    gain_mix,
    query_weight,
    key_weight,
    value_weight,
    gating_weight,
    write_weight,
    forget_weight,
    forget_rate,
    out_weight,
    gain_second,
    second_gate,
    second_up,
    second_down,
):
    count = lax.axis_size("kv") * lax.axis_size("tp")
    rows, width = tokens.shape
    channels = gain_first.shape[0]
    heads, size = state.shape[1], state.shape[2]
    mark = enter(first_gate, first_up, first_down)
    after_first = half_step(tokens, mark, count, gain_first, first_gate, first_up, first_down)
    blocks = gather_blocks(after_first, count)
    columns = 4 * width
    near = count // 2
    early, late = early_masks(count)
    mixers = [
        gain_mix.reshape(1, channels),
        query_weight,
        key_weight,
        value_weight,
        gating_weight,
        write_weight.T,
        forget_weight.T,
    ]
    parts_early = call(
        functools.partial(project_early_kernel, early),
        [
            pltpu.VMEM((rows, columns), F32),
            pltpu.VMEM((rows, 2 * heads), F32),
            pltpu.VMEM((rows, 128), F32),
        ],
        [*(blocks[m] for m in early), *mixers],
    )
    *sends, pre = call(
        functools.partial(project_late_kernel, late),
        [pltpu.VMEM((rows // near, columns), BF16)] * near + [pltpu.VMEM((BLK, 2 * heads), F32)],
        [*(blocks[m] for m in late), *mixers, *parts_early],
        scratch=[pltpu.VMEM((rows, columns), F32), pltpu.VMEM((rows, 2 * heads), F32)],
    )
    owned = pair_up([sends[0]] + far_swaps(sends[1:], count), count)
    matrices = state.reshape(heads, size, size)
    mixed, update, faded, final = call(
        functools.partial(delta_kernel, count),
        [
            pltpu.VMEM((BLK, channels), BF16),
            pltpu.VMEM((heads * BLK, size), F32),
            pltpu.VMEM((heads * BLK, size), F32),
            pltpu.VMEM((heads * BLK, size), F32),
        ],
        [*owned, pre, forget_rate.reshape(1, heads), lengths.reshape(1, 1), matrices],
        scratch=[pltpu.VMEM((count, BLK, columns), F32)],
    )
    head_blocks = gather_blocks(mixed, count)
    new_state = call(
        state_kernel,
        jax.ShapeDtypeStruct((heads, size, size), F32),
        [update, faded, final, matrices],
    )
    after_mix = call(
        functools.partial(out_kernel, count),
        pltpu.VMEM((rows, width), BF16),
        [*head_blocks, out_weight, after_first],
        scratch=[pltpu.VMEM((rows, width), F32)],
    )
    mixed_out = half_step(
        after_mix, mark, count, gain_second, second_gate, second_up, second_down, last=True
    )
    return (mixed_out, new_state.reshape(state.shape))


def fits_group(mesh):
    near, cores = mesh.shape["kv"], mesh.shape["tp"]
    count = near * cores
    return cores == 2 and near & (near - 1) == 0 and near <= 8 and (HEADS * HEAD) % (count * 128) == 0


def per_device(mesh, *arrays):
    lengths, gate = arrays[1], arrays[4]
    suits = fits_group(mesh) and lengths.shape[0] == 1 and gate.shape[1] % 128 == 0
    if not suits:
        return general_device(*arrays)
    return group_device(*arrays)


def solution(mesh):
    in_specs = (
        P("dp", ("kv", "tp")),
        P(("dp", "kv", "tp")),
        P(("dp", "kv", "tp"), None, None, None),
        P(),
        P(None, "kv"),
        P(None, "kv"),
        P("kv", None),
        P(),
        P(None, ("kv", "tp")),
        P(None, ("kv", "tp")),
        P(None, ("kv", "tp")),
        P(None, ("kv", "tp")),
        P(),
        P(),
        P(),
        P(None, ("kv", "tp")),
        P(),
        P(None, "kv"),
        P(None, "kv"),
        P("kv", None),
    )
    out_specs = (P("dp", ("kv", "tp")), P(("dp", "kv", "tp"), None, None, None))
    return jax.shard_map(
        functools.partial(per_device, mesh),
        mesh=mesh,
        in_specs=in_specs,
        out_specs=out_specs,
        check_vma=False,
    )
```

```python
import functools
import math

import jax
import jax.numpy as jnp
from jax import lax
from jax.experimental import pallas as pl
from jax.experimental.pallas import tpu as pltpu
from jax.sharding import PartitionSpec as P


HEADS = 16
HEAD = 128
BLK = 8


EPSILON = 1e-06


def fold_step(gain, gate_cols, up_cols, portion):
    values = portion.astype(jnp.float32)
    scaled = (values * gain).astype(jnp.bfloat16)
    gate_acc = jnp.dot(scaled, gate_cols, preferred_element_type=jnp.float32)
    up_acc = jnp.dot(scaled, up_cols, preferred_element_type=jnp.float32)
    squares = jnp.sum(values * values, axis=1)
    return (gate_acc, up_acc, squares)


def finish_units(gate_acc, up_acc, squares, channels, down_rows):
    row_scale = lax.rsqrt(squares / channels + EPSILON)[:, None]
    hidden = (jax.nn.silu(gate_acc * row_scale) * (up_acc * row_scale)).astype(jnp.bfloat16)
    return jnp.dot(hidden, down_rows, preferred_element_type=jnp.float32)


def feed_forward(hidden_in, gain, w_gate, w_up, w_down):
    channels = gain.shape[0]
    paired = lax.all_to_all(hidden_in, "tp", split_axis=0, concat_axis=1, tiled=True)
    gate_acc, up_acc, squares = fold_step(
        gain, w_gate, w_up, lax.all_gather(paired, "kv", axis=1, tiled=True)
    )
    ffn_term = finish_units(gate_acc, up_acc, squares, channels, w_down)
    partial_value = lax.psum_scatter(ffn_term, "kv", scatter_dimension=1, tiled=True)
    summed = lax.all_to_all(partial_value, "tp", split_axis=1, concat_axis=0, tiled=True)
    return (hidden_in.astype(jnp.float32) + 0.5 * summed).astype(jnp.bfloat16)


def delta_block(query, key_in, value, gating, write_pre, forget_pre, rates, live, state):
    seq_count, block_len, head_count, head_size = query.shape
    precise = lax.Precision.HIGHEST
    query_unit = (
        query
        * lax.rsqrt(jnp.sum(query * query, axis=-1, keepdims=True) + EPSILON)
        / math.sqrt(head_size)
    )
    key_unit = key_in * lax.rsqrt(jnp.sum(key_in * key_in, axis=-1, keepdims=True) + EPSILON)
    live_rows = live[:, :, None]
    write_gate = jax.nn.sigmoid(write_pre) * live_rows
    forget = -jnp.exp(rates)[None, None, :] * jax.nn.softplus(forget_pre) * live_rows
    cumulative = jnp.cumsum(forget, axis=1)
    cum_heads = jnp.transpose(cumulative, (0, 2, 1))
    positions = jnp.arange(block_len)
    causal = positions[:, None] >= positions[None, :]
    strict = positions[:, None] > positions[None, :]
    differ = jnp.minimum(cum_heads[:, :, :, None] - cum_heads[:, :, None, :], 0.0)
    decay_mat = jnp.where(causal, jnp.exp(differ), 0.0)
    key_dots = jnp.einsum("sthd,suhd->shtu", key_unit, key_unit, precision=precise)
    write_heads = jnp.transpose(write_gate, (0, 2, 1))
    strict_part = jnp.where(strict, write_heads[:, :, :, None] * decay_mat * key_dots, 0.0)
    identity = jnp.eye(block_len, dtype=jnp.float32)
    squared = jnp.einsum("shtu,shuv->shtv", strict_part, strict_part, precision=precise)
    fourth = jnp.einsum("shtu,shuv->shtv", squared, squared, precision=precise)
    inverse = jnp.einsum(
        "shtu,shuv->shtv", identity - strict_part, identity + squared, precision=precise
    )
    inverse = jnp.einsum("shtu,shuv->shtv", inverse, identity + fourth, precision=precise)
    growth = jnp.exp(cumulative)
    target = jnp.einsum(
        "shtu,suhv->sthv", inverse, write_gate[..., None] * value, precision=precise
    )
    key_mix = jnp.einsum(
        "shtu,suhk->sthk", inverse, (write_gate * growth)[..., None] * key_unit, precision=precise
    )
    update = target - jnp.einsum("sthk,shkv->sthv", key_mix, state, precision=precise)
    scores = jnp.einsum("sthd,suhd->shtu", query_unit, key_unit, precision=precise) * decay_mat
    attend = jnp.einsum("sthk,shkv->sthv", query_unit * growth[..., None], state, precision=precise)
    attend = attend + jnp.einsum("shtu,suhv->sthv", scores, update, precision=precise)
    final_cum = cumulative[:, -1:, :]
    fading = jnp.exp(final_cum - cumulative)
    new_state = jnp.exp(final_cum[:, 0, :])[:, :, None, None] * state
    new_state = new_state + jnp.einsum(
        "sthk,sthv->shkv", key_unit * fading[..., None], update, precision=precise
    )
    normed = attend * lax.rsqrt(jnp.mean(attend * attend, axis=-1, keepdims=True) + EPSILON)
    normed = normed * jax.nn.silu(gating) * live[:, :, None, None]
    mixed_heads = normed.reshape(seq_count * block_len, head_count * head_size).astype(jnp.bfloat16)
    return (mixed_heads, new_state)


def general_device(
    tokens,
    lengths,
    state,
    gain_first,
    first_gate,
    first_up,
    first_down,
    gain_mix,
    query_weight,
    key_weight,
    value_weight,
    gating_weight,
    write_weight,
    forget_weight,
    forget_rate,
    out_weight,
    gain_second,
    second_gate,
    second_up,
    second_down,
):
    after_first = feed_forward(tokens, gain_first, first_gate, first_up, first_down)
    seq_count = lengths.shape[0]
    own_count = seq_count * BLK
    whole_rows = lax.all_gather(after_first, ("kv", "tp"), axis=1, tiled=True)
    scaled_all = (whole_rows.astype(jnp.float32) * gain_mix).astype(jnp.bfloat16)
    stacked = jnp.stack(
        [
            jnp.dot(scaled_all, matrix, preferred_element_type=jnp.float32)
            for matrix in (query_weight, key_weight, value_weight, gating_weight)
        ]
    )
    owned = lax.all_to_all(
        stacked.astype(jnp.bfloat16), ("kv", "tp"), split_axis=1, concat_axis=2, tiled=True
    ).astype(stacked.dtype)
    row_start = lax.axis_index(("kv", "tp")) * own_count
    own_values = lax.dynamic_slice_in_dim(whole_rows, row_start, own_count, 0).astype(jnp.float32)
    own_scaled = lax.dynamic_slice_in_dim(scaled_all, row_start, own_count, 0)
    mix_scale = lax.rsqrt(jnp.mean(own_values * own_values, axis=1, keepdims=True) + EPSILON)
    query = (owned[0] * mix_scale).reshape(seq_count, BLK, HEADS, HEAD)
    key_in = (owned[1] * mix_scale).reshape(seq_count, BLK, HEADS, HEAD)
    value = (owned[2] * mix_scale).reshape(seq_count, BLK, HEADS, HEAD)
    gating = (owned[3] * mix_scale).reshape(seq_count, BLK, HEADS, HEAD)
    write_pre = (
        jnp.dot(own_scaled, write_weight, preferred_element_type=jnp.float32) * mix_scale
    ).reshape(seq_count, BLK, HEADS)
    forget_pre = (
        jnp.dot(own_scaled, forget_weight, preferred_element_type=jnp.float32) * mix_scale
    ).reshape(seq_count, BLK, HEADS)
    positions = jnp.arange(BLK, dtype=jnp.int32)
    live = (positions[None, :] < lengths[:, None]).astype(jnp.float32)
    mixed_heads, new_state = delta_block(
        query, key_in, value, gating, write_pre, forget_pre, forget_rate, live, state
    )
    half_cols = mixed_heads.shape[1] // 2
    portion = lax.all_gather(mixed_heads, ("kv", "tp"), axis=0, tiled=True)
    first_half = jnp.dot(
        portion[:, :half_cols], out_weight[:half_cols], preferred_element_type=jnp.float32
    ).astype(jnp.bfloat16)
    second_half = jnp.dot(
        portion[:, half_cols:], out_weight[half_cols:], preferred_element_type=jnp.float32
    ).astype(jnp.bfloat16)
    first_half, second_half = lax.optimization_barrier((first_half, second_half))
    mixed_sum = first_half.astype(jnp.float32) + second_half.astype(jnp.float32)
    after_mix = (after_first.astype(jnp.float32) + mixed_sum).astype(jnp.bfloat16)
    mixed_out = feed_forward(after_mix, gain_second, second_gate, second_up, second_down)
    return (mixed_out, new_state)


VMEM_SPEC = pl.BlockSpec(memory_space=pltpu.VMEM)
HBM_SPEC = pl.BlockSpec(memory_space=pltpu.HBM)
GROUP = ("kv", "tp")
F32, BF16 = jnp.float32, jnp.bfloat16


def call(body, out_shapes, args, in_specs=None, scratch=(), limit=5 << 20, out_specs=None):
    single = not isinstance(out_shapes, (list, tuple))
    shapes = [out_shapes] if single else list(out_shapes)
    outs = pl.pallas_call(
        body,
        out_shape=shapes,
        in_specs=in_specs or [VMEM_SPEC] * len(args),
        out_specs=out_specs or [VMEM_SPEC] * len(shapes),
        scratch_shapes=list(scratch),
        compiler_params=pltpu.CompilerParams(vmem_limit_bytes=limit),
    )(*args)
    return outs[0] if single else outs


def my_index():
    return lax.axis_index("kv") * lax.axis_size("tp") + lax.axis_index("tp")


def swap(value, mask, count):
    return lax.ppermute(value, GROUP, [(i, i ^ mask) for i in range(count)])


def far_swaps(sends, count):
    received = []
    for step, send in enumerate(sends):
        received.append(swap(send, 2 * (step + 1), count))
    return received


def pair_up(near, count):
    blocks = []
    for block in near:
        blocks += [block, swap(block, 1, count)]
    return blocks


def gather_blocks(own, count):
    near = [own] + far_swaps([own] * (count // 2 - 1), count)
    return pair_up(near, count)


def entry_kernel(gate_hbm, up_hbm, down_hbm, mark_ref):
    mark_ref[...] = jnp.zeros_like(mark_ref)


def enter(*weights):
    arrays = [pltpu.with_memory_space_constraint(a, pltpu.HBM) for a in weights]
    return call(
        entry_kernel,
        pltpu.VMEM((8, 128), F32),
        arrays,
        in_specs=[HBM_SPEC] * len(arrays),
        limit=1 << 20,
    )


def stage_kernel(count, *refs):
    sources, targets, sem = refs[:count], refs[count : 2 * count], refs[2 * count]
    copies = [pltpu.make_async_copy(*pair, sem.at[i]) for i, pair in enumerate(zip(sources, targets))]
    for copy in copies:
        copy.start()
    for copy in copies:
        copy.wait()


def stage(*arrays):
    return call(
        functools.partial(stage_kernel, len(arrays)),
        [pltpu.VMEM(a.shape, a.dtype) for a in arrays],
        [pltpu.with_memory_space_constraint(a, pltpu.HBM) for a in arrays],
        in_specs=[HBM_SPEC] * len(arrays),
        scratch=[pltpu.SemaphoreType.DMA((len(arrays),))],
        limit=1 << 20,
    )


def core_span(units):
    tiles = units // 128
    span = -(-tiles // 2) * 128
    return span, units - span


def gained(block, owner, gain_ref):
    width = block.shape[1]
    column = pl.multiple_of(owner * width, width)
    values = block[...].astype(F32)
    squares = values * values
    folded = squares[:, :128]
    for first in range(128, width, 128):
        folded = folded + squares[:, first : first + 128]
    return (values * gain_ref[:, pl.ds(column, width)]).astype(BF16), folded


def scale_of_rows(folded, channels):
    return lax.rsqrt(jnp.sum(folded, axis=1, keepdims=True) / channels + EPSILON)


def plus(total, part):
    return part if total is None else total + part


def early_masks(count):
    late = (3, 5) if count > 4 else (3,)
    return [m for m in range(count) if m not in late], list(late)


def entry_kernel(gate_hbm, up_hbm, down_hbm, mark_ref):
    mark_ref[...] = jnp.zeros_like(mark_ref)


def enter(*weights):
    arrays = [pltpu.with_memory_space_constraint(a, pltpu.HBM) for a in weights]
    return call(
        entry_kernel,
        pltpu.VMEM((8, 128), F32),
        arrays,
        in_specs=[HBM_SPEC] * len(arrays),
        limit=1 << 20,
    )


def core_span(units):
    tiles = units // 128
    span = -(-tiles // 2) * 128
    return span, units - span


def units_of(blocks, masks, gain_ref, gate_ref, up_ref, span, skip):
    index = my_index()
    start = pl.multiple_of(lax.axis_index("tp") * skip, 128)
    gate_acc = up_acc = squares = None
    for mask, block in zip(masks, blocks):
        owner = index ^ mask
        width = block.shape[1]
        rows = pl.ds(pl.multiple_of(owner * width, width), width)
        lhs, folded = gained(block, owner, gain_ref)
        squares = plus(squares, folded)
        columns = pl.ds(start, span)
        gate_acc = plus(gate_acc, jnp.dot(lhs, gate_ref[rows, columns], preferred_element_type=F32))
        up_acc = plus(up_acc, jnp.dot(lhs, up_ref[rows, columns], preferred_element_type=F32))
    return gate_acc, up_acc, squares


def ffn_early_kernel(masks, span, skip, *refs):
    blocks = refs[: len(masks)]
    gain_ref, gate_ref, up_ref, _, _, gate_out, up_out, squares_out = refs[len(masks) :]
    gate_out[...], up_out[...], squares_out[...] = units_of(
        blocks, masks, gain_ref, gate_ref, up_ref, span, skip
    )


def ffn_late_kernel(masks, count, span, skip, *refs):
    blocks = refs[: len(masks)]
    gain_ref, gate_ref, up_ref, down_ref, gate_in, up_in, squares_in = refs[len(masks) : len(masks) + 7]
    hidden_ref, cross_ref = refs[len(masks) + 7 :]
    gate_acc, up_acc, squares = units_of(blocks, masks, gain_ref, gate_ref, up_ref, span, skip)
    channels = gate_ref.shape[0]
    row_scale = scale_of_rows(squares + squares_in[...], channels)
    gate_act = (gate_acc + gate_in[...]) * row_scale
    hidden = gate_act * jax.nn.sigmoid(gate_act) * ((up_acc + up_in[...]) * row_scale)
    repeated = lax.axis_index("tp") * (lax.axis_size("tp") * span - down_ref.shape[0])
    unit = lax.broadcasted_iota(jnp.int32, hidden.shape, 1)
    hidden_ref[...] = jnp.where(unit >= repeated, hidden, 0.0).astype(BF16)
    hidden = hidden_ref[...]
    down_products(hidden, down_ref, range(1, count, 2), cross_ref, skip)


def down_products(hidden, down_ref, masks, out_ref, skip):
    index = my_index()
    start = pl.multiple_of(lax.axis_index("tp") * skip, 128)
    span, width = hidden.shape[1], out_ref.shape[2]
    for place, mask in enumerate(masks):
        column = pl.multiple_of((index ^ mask) * width, width)
        weight = down_ref[pl.ds(start, span), pl.ds(column, width)]
        out_ref[place] = jnp.dot(hidden, weight, preferred_element_type=F32).astype(out_ref.dtype)


def ffn_own_kernel(count, skip, hidden_ref, down_ref, own_ref):
    down_products(hidden_ref[...], down_ref, range(0, count, 2), own_ref, skip)


def pair_sum_kernel(own_ref, cross_ref, mine_ref, *sends):
    mine_ref[...] = own_ref[0] + cross_ref[0].astype(F32)
    for step, send in enumerate(sends):
        send[...] = (own_ref[step + 1] + cross_ref[step + 1].astype(F32)).astype(BF16)


def residual_kernel(base_ref, mine_ref, *refs):
    total = mine_ref[...]
    for received in refs[:-1]:
        total = total + received[...].astype(F32)
    refs[-1][...] = (base_ref[...].astype(F32) + 0.5 * total).astype(BF16)


def half_step(own, mark, count, gain, gate, up, down, first=False, last=False):
    rows, width = own.shape
    near = count // 2
    span, skip = core_span(down.shape[0])
    gain = gain.reshape(1, count * width)
    near_own = own
    if first:
        own, gain = stage(own, gain)
    received = far_swaps([near_own] * (near - 1), count)
    blocks = pair_up([own, *received], count)
    early, late = early_masks(count)
    parts_early = call(
        functools.partial(ffn_early_kernel, early, span, skip),
        [pltpu.VMEM((rows, span), F32)] * 2 + [pltpu.VMEM((rows, 128), F32)],
        [*(blocks[m] for m in early), gain, gate, up, down, mark],
    )
    hidden, cross_part = call(
        functools.partial(ffn_late_kernel, late, count, span, skip),
        [pltpu.VMEM((rows, span), BF16), pltpu.VMEM((near, rows, width), BF16)],
        [*(blocks[m] for m in late), gain, gate, up, down, *parts_early],
    )
    cross_sum = swap(cross_part, 1, count)
    own_part = call(
        functools.partial(ffn_own_kernel, count, skip),
        pltpu.VMEM((near, rows, width), F32),
        [hidden, down],
    )
    mine, *sends = call(
        pair_sum_kernel,
        [pltpu.VMEM((rows, width), F32)] + [pltpu.VMEM((rows, width), BF16)] * (near - 1),
        [own_part, cross_sum],
    )
    received = far_swaps(sends, count)
    shape = jax.ShapeDtypeStruct if last else pltpu.VMEM
    return call(residual_kernel, shape((rows, width), BF16), [own, mine, *received])


def mixes_of(blocks, masks, gain_ref, weights, thin):
    index = my_index()
    wide = [None] * len(weights)
    narrow = [None] * len(thin)
    squares = None
    across = (((1,), (1,)), ((), ()))
    for mask, block in zip(masks, blocks):
        owner = index ^ mask
        width = block.shape[1]
        rows = pl.ds(pl.multiple_of(owner * width, width), width)
        lhs, folded = gained(block, owner, gain_ref)
        squares = plus(squares, folded)
        for place, weight in enumerate(weights):
            wide[place] = plus(wide[place], jnp.dot(lhs, weight[rows, :], preferred_element_type=F32))
        for place, weight in enumerate(thin):
            part = lax.dot_general(lhs, weight[:, rows], across, preferred_element_type=F32)
            narrow[place] = plus(narrow[place], part)
    return wide, narrow, squares


def project_early_kernel(masks, *refs):
    blocks = refs[: len(masks)]
    gain_ref, *weights = refs[len(masks) : len(masks) + 7]
    result, pre, squares_out = refs[len(masks) + 7 :]
    wide, narrow, squares_out[...] = mixes_of(blocks, masks, gain_ref, weights[:4], weights[4:])
    for place, part in enumerate(wide):
        width = part.shape[1]
        result[:, place * width : (place + 1) * width] = part
    for place, part in enumerate(narrow):
        width = part.shape[1]
        pre[:, place * width : (place + 1) * width] = part


def project_late_kernel(masks, *refs):
    blocks = refs[: len(masks)]
    gain_ref, *weights = refs[len(masks) : len(masks) + 7]
    result_in, pre_in, squares_in = refs[len(masks) + 7 : len(masks) + 10]
    *sends, pre_ref, result, pre_scratch = refs[len(masks) + 10 :]
    wide, narrow, squares = mixes_of(blocks, masks, gain_ref, weights[:4], weights[4:])
    row_scale = scale_of_rows(squares + squares_in[...], weights[0].shape[0])
    for place, part in enumerate(wide):
        width = part.shape[1]
        columns = slice(place * width, (place + 1) * width)
        result[:, columns] = (part + result_in[:, columns]) * row_scale
    for place, part in enumerate(narrow):
        width = part.shape[1]
        columns = slice(place * width, (place + 1) * width)
        pre_scratch[:, columns] = (part + pre_in[:, columns]) * row_scale
    for step, send in enumerate(sends):
        rows = send.shape[0]
        row = pl.multiple_of((lax.axis_index("kv") ^ step) * rows, rows)
        send[...] = result[pl.ds(row, rows), :].astype(BF16)
    row = pl.multiple_of(my_index() * BLK, BLK)
    pre_ref[...] = pre_scratch[pl.ds(row, BLK), :]


def parts(value):
    high = value.astype(BF16)
    return high, (value - high.astype(F32)).astype(BF16)


def dot_parts(left, right, dims=(((1,), (0,)), ((), ()))):
    left_high, left_low = left
    right_high, right_low = right
    total = lax.dot_general(left_high, right_low, dims, preferred_element_type=F32)
    total = total + lax.dot_general(left_low, right_high, dims, preferred_element_type=F32)
    return total + lax.dot_general(left_high, right_high, dims, preferred_element_type=F32)


def split_state_kernel(state_ref, length_ref, high_ref, low_ref, live_ref):
    high_ref[...], low_ref[...] = parts(state_ref[...])
    step_of = lax.broadcasted_iota(jnp.int32, live_ref.shape, 0)
    live_ref[...] = (step_of < length_ref[...]).astype(F32)


def delta_kernel(masks, count, *refs):
    blocks = refs[: len(masks)]
    pre_ref, rate_ref, live_ref, high_ref, low_ref = refs[len(masks) : len(masks) + 5]
    mixed_ref, update_ref, faded_ref, final_ref = refs[len(masks) + 5 :]
    index = my_index()
    first_core = lax.axis_index("tp") == 0
    size = high_ref.shape[-1]
    all_heads = rate_ref.shape[1]
    per_block = all_heads // count
    heads = per_block * len(masks)
    rows = heads * BLK
    width = per_block * size
    taken = []
    for block in blocks:
        both = block[...].astype(F32)
        taken.append(jnp.where(first_core, both[:BLK], both[BLK:]))

    def stack(place):
        found = []
        for block in taken:
            for head in range(per_block):
                column = place * width + head * size
                found.append(block[:, column : column + size])
        return jnp.concatenate(found, axis=0)

    def head_at(head):
        return (index ^ masks[head // per_block]) * per_block + head % per_block

    query, key_in, value, gating = (stack(place) for place in range(4))
    query_unit = query * lax.rsqrt(jnp.sum(query * query, axis=1, keepdims=True) + EPSILON) * (1.0 / math.sqrt(size))
    key_unit = key_in * lax.rsqrt(jnp.sum(key_in * key_in, axis=1, keepdims=True) + EPSILON)
    step_of = lax.broadcasted_iota(jnp.int32, (BLK, all_heads), 0)
    live = live_ref[...]
    pre = pre_ref[...]
    write_gate = jax.nn.sigmoid(pre[:, :all_heads]) * live
    forget_in = pre[:, all_heads:]
    softplus = jnp.maximum(forget_in, 0.0) + jnp.log1p(jnp.exp(-jnp.abs(forget_in)))
    forget = -jnp.exp(rate_ref[...]) * softplus * live
    cumulative = forget
    lower = 1
    while lower < BLK:
        moved = pltpu.roll(cumulative, lower, 0)
        cumulative = cumulative + jnp.where(step_of >= lower, moved, 0.0)
        lower *= 2
    final = jnp.broadcast_to(cumulative[BLK - 1 :, :], (BLK, all_heads))
    head_of = lax.broadcasted_iota(jnp.int32, (BLK, all_heads), 1)
    picked = jnp.concatenate([head_of == head_at(head) for head in range(heads)], axis=0)

    def column_of(array):
        tall = jnp.concatenate([array] * heads, axis=0)
        return jnp.sum(jnp.where(picked, tall, 0.0), axis=1, keepdims=True)

    write_col, live_col = column_of(write_gate), column_of(live)
    cum_col, final_col = column_of(cumulative), column_of(final)
    down_at = lax.broadcasted_iota(jnp.int32, (rows, rows), 0)
    over_at = lax.broadcasted_iota(jnp.int32, (rows, rows), 1)
    same = (down_at // BLK) == (over_at // BLK)
    diagonal = down_at == over_at
    cum_row = jnp.sum(jnp.where(diagonal, cum_col, 0.0), axis=0, keepdims=True)
    causal = same & (down_at >= over_at)
    decay = jnp.where(causal, jnp.exp(jnp.minimum(cum_col - cum_row, 0.0)), 0.0)
    across = (((1,), (1,)), ((), ()))
    key_parts = parts(key_unit)
    strict_part = jnp.where(diagonal, 0.0, write_col * decay * dot_parts(key_parts, key_parts, across))
    scores = decay * dot_parts(parts(query_unit), key_parts, across)
    identity = diagonal.astype(F32)
    strict_split = parts(strict_part)
    squared = dot_parts(strict_split, strict_split)
    squared_split = parts(squared)
    fourth = dot_parts(squared_split, squared_split)
    inverse = identity - strict_part + squared - dot_parts(strict_split, squared_split)
    inverse = inverse + dot_parts(parts(inverse), parts(fourth))
    growth = jnp.exp(cum_col)
    key_grown, query_grown = key_unit * growth, query_unit * growth
    from_key, from_query = [], []
    for head in range(heads):
        at = slice(head * BLK, (head + 1) * BLK)
        both = jnp.concatenate([key_grown[at], query_grown[at]], axis=0)
        found = dot_parts(parts(both), (high_ref[head_at(head)], low_ref[head_at(head)]))
        from_key.append(found[:BLK])
        from_query.append(found[BLK:])
    target = write_col * (value - jnp.concatenate(from_key, axis=0))
    update = dot_parts(parts(inverse), parts(target))
    attend = jnp.concatenate(from_query, axis=0) + dot_parts(parts(scores), parts(update))
    normed = attend * lax.rsqrt(jnp.mean(attend * attend, axis=1, keepdims=True) + EPSILON)
    normed = (normed * (gating * jax.nn.sigmoid(gating)) * live_col).astype(BF16)
    for head in range(heads):
        mixed_ref[:, head * size : (head + 1) * size] = normed[head * BLK : (head + 1) * BLK]
    update_ref[...] = update
    faded_ref[...] = key_unit * jnp.exp(final_col - cum_col)
    final_ref[...] = jnp.broadcast_to(jnp.exp(final_col), final_ref.shape)


def join_kernel(count, first_ref, second_ref, mixed_ref):
    width = mixed_ref.shape[1] // count
    index = my_index()
    for mask in range(count):
        source = second_ref if mask % 2 else first_ref
        place = mask // 2
        column = pl.multiple_of((index ^ mask) * width, width)
        mixed_ref[:, pl.ds(column, width)] = source[:, place * width : (place + 1) * width]


def state_kernel(groups, count, *refs):
    state_ref, new_ref = refs[3 * len(groups) :]
    per_block = state_ref.shape[0] // count
    index = my_index()
    along = (((0,), (0,)), ((), ()))
    for place, masks in enumerate(groups):
        update_ref, faded_ref, final_ref = refs[3 * place : 3 * place + 3]
        for head in range(per_block * len(masks)):
            at = slice(head * BLK, (head + 1) * BLK)
            left_high, left_low = parts(faded_ref[at])
            right_high, right_low = parts(update_ref[at])
            left = jnp.concatenate([left_high, left_high, left_low, left_low], axis=0)
            right = jnp.concatenate([right_high, right_low, right_high, right_low], axis=0)
            grown = lax.dot_general(left, right, along, preferred_element_type=F32)
            scale = final_ref[head * BLK : head * BLK + 1, :]
            owner = (index ^ masks[head // per_block]) * per_block + head % per_block
            new_ref[pl.ds(owner, 1)] = (scale * state_ref[owner] + grown)[None]


def out_kernel(count, *refs):
    blocks = refs[:count]
    weight_ref, base_ref, out_ref, scratch = refs[count:]
    index = my_index()
    lhs = jnp.concatenate([block[...].astype(F32) for block in blocks], axis=0).astype(BF16)
    half = lhs.shape[1] // 2
    first = jnp.dot(lhs[:, :half], weight_ref[:half, :], preferred_element_type=F32).astype(BF16)
    second = jnp.dot(lhs[:, half:], weight_ref[half:, :], preferred_element_type=F32).astype(BF16)
    total = first.astype(F32) + second.astype(F32)
    for mask in range(count):
        row = pl.multiple_of((index ^ mask) * BLK, BLK)
        scratch[pl.ds(row, BLK), :] = total[mask * BLK : (mask + 1) * BLK]
    out_ref[...] = (base_ref[...].astype(F32) + scratch[...]).astype(BF16)


def group_device(
    tokens,
    lengths,
    state,
    gain_first,
    first_gate,
    first_up,
    first_down,
    gain_mix,
    query_weight,
    key_weight,
    value_weight,
    gating_weight,
    write_weight,
    forget_weight,
    forget_rate,
    out_weight,
    gain_second,
    second_gate,
    second_up,
    second_down,
):
    count = lax.axis_size("kv") * lax.axis_size("tp")
    rows, width = tokens.shape
    channels = gain_first.shape[0]
    heads, size = state.shape[1], state.shape[2]
    mark = enter(first_gate, first_up, first_down)
    after_first = half_step(
        tokens, mark, count, gain_first, first_gate, first_up, first_down, first=True
    )
    blocks = gather_blocks(after_first, count)
    columns = 4 * width
    near = count // 2
    early, late = early_masks(count)
    mixers = [
        gain_mix.reshape(1, channels),
        query_weight,
        key_weight,
        value_weight,
        gating_weight,
        write_weight.T,
        forget_weight.T,
    ]
    parts_early = call(
        functools.partial(project_early_kernel, early),
        [
            pltpu.VMEM((rows, columns), F32),
            pltpu.VMEM((rows, 2 * heads), F32),
            pltpu.VMEM((rows, 128), F32),
        ],
        [*(blocks[m] for m in early), *mixers],
    )
    *sends, pre = call(
        functools.partial(project_late_kernel, late),
        [pltpu.VMEM((rows // near, columns), BF16)] * near + [pltpu.VMEM((BLK, 2 * heads), F32)],
        [*(blocks[m] for m in late), *mixers, *parts_early],
        scratch=[pltpu.VMEM((rows, columns), F32), pltpu.VMEM((rows, 2 * heads), F32)],
    )
    owned = pair_up([sends[0]] + far_swaps(sends[1:], count), count)
    matrices = state.reshape(heads, size, size)
    high, low, live = call(
        split_state_kernel,
        [pltpu.VMEM(matrices.shape, BF16)] * 2 + [pltpu.VMEM((BLK, heads), F32)],
        [matrices, lengths.reshape(1, 1)],
        limit=3 << 20,
    )
    groups = [list(range(0, count, 2)), list(range(1, count, 2))]
    mixed_parts, grown = [], []
    for masks in groups:
        tall = heads * BLK // 2
        part, *rest = call(
            functools.partial(delta_kernel, masks, count),
            [pltpu.VMEM((BLK, channels // 2), BF16)] + [pltpu.VMEM((tall, size), F32)] * 3,
            [
                *(owned[m] for m in masks),
                pre,
                forget_rate.reshape(1, heads),
                live,
                high,
                low,
            ],
        )
        mixed_parts.append(part)
        grown += rest
    mixed = call(
        functools.partial(join_kernel, count), pltpu.VMEM((BLK, channels), BF16), mixed_parts
    )
    head_blocks = gather_blocks(mixed, count)
    new_state = call(
        functools.partial(state_kernel, groups, count),
        jax.ShapeDtypeStruct((heads, size, size), F32),
        [*grown, matrices],
    )
    after_mix = call(
        functools.partial(out_kernel, count),
        pltpu.VMEM((rows, width), BF16),
        [*head_blocks, out_weight, after_first],
        scratch=[pltpu.VMEM((rows, width), F32)],
    )
    mixed_out = half_step(
        after_mix, mark, count, gain_second, second_gate, second_up, second_down, last=True
    )
    return (mixed_out, new_state.reshape(state.shape))


def fits_group(mesh):
    near, cores = mesh.shape["kv"], mesh.shape["tp"]
    count = near * cores
    return cores == 2 and near & (near - 1) == 0 and near <= 8 and (HEADS * HEAD) % (count * 128) == 0


def per_device(mesh, *arrays):
    lengths, gate = arrays[1], arrays[4]
    suits = fits_group(mesh) and lengths.shape[0] == 1 and gate.shape[1] % 128 == 0
    if not suits:
        return general_device(*arrays)
    return group_device(*arrays)


def solution(mesh):
    in_specs = (
        P("dp", ("kv", "tp")),
        P(("dp", "kv", "tp")),
        P(("dp", "kv", "tp"), None, None, None),
        P(),
        P(None, "kv"),
        P(None, "kv"),
        P("kv", None),
        P(),
        P(None, ("kv", "tp")),
        P(None, ("kv", "tp")),
        P(None, ("kv", "tp")),
        P(None, ("kv", "tp")),
        P(),
        P(),
        P(),
        P(None, ("kv", "tp")),
        P(),
        P(None, "kv"),
        P(None, "kv"),
        P("kv", None),
    )
    out_specs = (P("dp", ("kv", "tp")), P(("dp", "kv", "tp"), None, None, None))
    return jax.shard_map(
        functools.partial(per_device, mesh),
        mesh=mesh,
        in_specs=in_specs,
        out_specs=out_specs,
        check_vma=False,
    )
```

```python
import functools
import math

import jax
import jax.numpy as jnp
from jax import lax
from jax.experimental import pallas as pl
from jax.experimental.pallas import tpu as pltpu
from jax.sharding import PartitionSpec as P


HEADS = 16
HEAD = 128
BLK = 8


EPSILON = 1e-06


def fold_step(gain, gate_cols, up_cols, portion):
    values = portion.astype(jnp.float32)
    scaled = (values * gain).astype(jnp.bfloat16)
    gate_acc = jnp.dot(scaled, gate_cols, preferred_element_type=jnp.float32)
    up_acc = jnp.dot(scaled, up_cols, preferred_element_type=jnp.float32)
    squares = jnp.sum(values * values, axis=1)
    return (gate_acc, up_acc, squares)


def finish_units(gate_acc, up_acc, squares, channels, down_rows):
    row_scale = lax.rsqrt(squares / channels + EPSILON)[:, None]
    hidden = (jax.nn.silu(gate_acc * row_scale) * (up_acc * row_scale)).astype(jnp.bfloat16)
    return jnp.dot(hidden, down_rows, preferred_element_type=jnp.float32)


def feed_forward(hidden_in, gain, w_gate, w_up, w_down):
    channels = gain.shape[0]
    paired = lax.all_to_all(hidden_in, "tp", split_axis=0, concat_axis=1, tiled=True)
    gate_acc, up_acc, squares = fold_step(
        gain, w_gate, w_up, lax.all_gather(paired, "kv", axis=1, tiled=True)
    )
    ffn_term = finish_units(gate_acc, up_acc, squares, channels, w_down)
    partial_value = lax.psum_scatter(ffn_term, "kv", scatter_dimension=1, tiled=True)
    summed = lax.all_to_all(partial_value, "tp", split_axis=1, concat_axis=0, tiled=True)
    return (hidden_in.astype(jnp.float32) + 0.5 * summed).astype(jnp.bfloat16)


def delta_block(query, key_in, value, gating, write_pre, forget_pre, rates, live, state):
    seq_count, block_len, head_count, head_size = query.shape
    precise = lax.Precision.HIGHEST
    query_unit = (
        query
        * lax.rsqrt(jnp.sum(query * query, axis=-1, keepdims=True) + EPSILON)
        / math.sqrt(head_size)
    )
    key_unit = key_in * lax.rsqrt(jnp.sum(key_in * key_in, axis=-1, keepdims=True) + EPSILON)
    live_rows = live[:, :, None]
    write_gate = jax.nn.sigmoid(write_pre) * live_rows
    forget = -jnp.exp(rates)[None, None, :] * jax.nn.softplus(forget_pre) * live_rows
    cumulative = jnp.cumsum(forget, axis=1)
    cum_heads = jnp.transpose(cumulative, (0, 2, 1))
    positions = jnp.arange(block_len)
    causal = positions[:, None] >= positions[None, :]
    strict = positions[:, None] > positions[None, :]
    differ = jnp.minimum(cum_heads[:, :, :, None] - cum_heads[:, :, None, :], 0.0)
    decay_mat = jnp.where(causal, jnp.exp(differ), 0.0)
    key_dots = jnp.einsum("sthd,suhd->shtu", key_unit, key_unit, precision=precise)
    write_heads = jnp.transpose(write_gate, (0, 2, 1))
    strict_part = jnp.where(strict, write_heads[:, :, :, None] * decay_mat * key_dots, 0.0)
    identity = jnp.eye(block_len, dtype=jnp.float32)
    squared = jnp.einsum("shtu,shuv->shtv", strict_part, strict_part, precision=precise)
    fourth = jnp.einsum("shtu,shuv->shtv", squared, squared, precision=precise)
    inverse = jnp.einsum(
        "shtu,shuv->shtv", identity - strict_part, identity + squared, precision=precise
    )
    inverse = jnp.einsum("shtu,shuv->shtv", inverse, identity + fourth, precision=precise)
    growth = jnp.exp(cumulative)
    target = jnp.einsum(
        "shtu,suhv->sthv", inverse, write_gate[..., None] * value, precision=precise
    )
    key_mix = jnp.einsum(
        "shtu,suhk->sthk", inverse, (write_gate * growth)[..., None] * key_unit, precision=precise
    )
    update = target - jnp.einsum("sthk,shkv->sthv", key_mix, state, precision=precise)
    scores = jnp.einsum("sthd,suhd->shtu", query_unit, key_unit, precision=precise) * decay_mat
    attend = jnp.einsum("sthk,shkv->sthv", query_unit * growth[..., None], state, precision=precise)
    attend = attend + jnp.einsum("shtu,suhv->sthv", scores, update, precision=precise)
    final_cum = cumulative[:, -1:, :]
    fading = jnp.exp(final_cum - cumulative)
    new_state = jnp.exp(final_cum[:, 0, :])[:, :, None, None] * state
    new_state = new_state + jnp.einsum(
        "sthk,sthv->shkv", key_unit * fading[..., None], update, precision=precise
    )
    normed = attend * lax.rsqrt(jnp.mean(attend * attend, axis=-1, keepdims=True) + EPSILON)
    normed = normed * jax.nn.silu(gating) * live[:, :, None, None]
    mixed_heads = normed.reshape(seq_count * block_len, head_count * head_size).astype(jnp.bfloat16)
    return (mixed_heads, new_state)


def general_device(
    tokens,
    lengths,
    state,
    gain_first,
    first_gate,
    first_up,
    first_down,
    gain_mix,
    query_weight,
    key_weight,
    value_weight,
    gating_weight,
    write_weight,
    forget_weight,
    forget_rate,
    out_weight,
    gain_second,
    second_gate,
    second_up,
    second_down,
):
    after_first = feed_forward(tokens, gain_first, first_gate, first_up, first_down)
    seq_count = lengths.shape[0]
    own_count = seq_count * BLK
    whole_rows = lax.all_gather(after_first, ("kv", "tp"), axis=1, tiled=True)
    scaled_all = (whole_rows.astype(jnp.float32) * gain_mix).astype(jnp.bfloat16)
    stacked = jnp.stack(
        [
            jnp.dot(scaled_all, matrix, preferred_element_type=jnp.float32)
            for matrix in (query_weight, key_weight, value_weight, gating_weight)
        ]
    )
    owned = lax.all_to_all(
        stacked.astype(jnp.bfloat16), ("kv", "tp"), split_axis=1, concat_axis=2, tiled=True
    ).astype(stacked.dtype)
    row_start = lax.axis_index(("kv", "tp")) * own_count
    own_values = lax.dynamic_slice_in_dim(whole_rows, row_start, own_count, 0).astype(jnp.float32)
    own_scaled = lax.dynamic_slice_in_dim(scaled_all, row_start, own_count, 0)
    mix_scale = lax.rsqrt(jnp.mean(own_values * own_values, axis=1, keepdims=True) + EPSILON)
    query = (owned[0] * mix_scale).reshape(seq_count, BLK, HEADS, HEAD)
    key_in = (owned[1] * mix_scale).reshape(seq_count, BLK, HEADS, HEAD)
    value = (owned[2] * mix_scale).reshape(seq_count, BLK, HEADS, HEAD)
    gating = (owned[3] * mix_scale).reshape(seq_count, BLK, HEADS, HEAD)
    write_pre = (
        jnp.dot(own_scaled, write_weight, preferred_element_type=jnp.float32) * mix_scale
    ).reshape(seq_count, BLK, HEADS)
    forget_pre = (
        jnp.dot(own_scaled, forget_weight, preferred_element_type=jnp.float32) * mix_scale
    ).reshape(seq_count, BLK, HEADS)
    positions = jnp.arange(BLK, dtype=jnp.int32)
    live = (positions[None, :] < lengths[:, None]).astype(jnp.float32)
    mixed_heads, new_state = delta_block(
        query, key_in, value, gating, write_pre, forget_pre, forget_rate, live, state
    )
    half_cols = mixed_heads.shape[1] // 2
    portion = lax.all_gather(mixed_heads, ("kv", "tp"), axis=0, tiled=True)
    first_half = jnp.dot(
        portion[:, :half_cols], out_weight[:half_cols], preferred_element_type=jnp.float32
    ).astype(jnp.bfloat16)
    second_half = jnp.dot(
        portion[:, half_cols:], out_weight[half_cols:], preferred_element_type=jnp.float32
    ).astype(jnp.bfloat16)
    first_half, second_half = lax.optimization_barrier((first_half, second_half))
    mixed_sum = first_half.astype(jnp.float32) + second_half.astype(jnp.float32)
    after_mix = (after_first.astype(jnp.float32) + mixed_sum).astype(jnp.bfloat16)
    mixed_out = feed_forward(after_mix, gain_second, second_gate, second_up, second_down)
    return (mixed_out, new_state)


VMEM_SPEC = pl.BlockSpec(memory_space=pltpu.VMEM)
HBM_SPEC = pl.BlockSpec(memory_space=pltpu.HBM)
GROUP = ("kv", "tp")
F32, BF16 = jnp.float32, jnp.bfloat16


def call(body, out_shapes, args, in_specs=None, scratch=(), limit=5 << 20, out_specs=None):
    single = not isinstance(out_shapes, (list, tuple))
    shapes = [out_shapes] if single else list(out_shapes)
    outs = pl.pallas_call(
        body,
        out_shape=shapes,
        in_specs=in_specs or [VMEM_SPEC] * len(args),
        out_specs=out_specs or [VMEM_SPEC] * len(shapes),
        scratch_shapes=list(scratch),
        compiler_params=pltpu.CompilerParams(vmem_limit_bytes=limit),
    )(*args)
    return outs[0] if single else outs


def my_index():
    return lax.axis_index("kv") * lax.axis_size("tp") + lax.axis_index("tp")


def swap(value, mask, count):
    return lax.ppermute(value, GROUP, [(i, i ^ mask) for i in range(count)])


def far_swaps(sends, count):
    received = []
    for step, send in enumerate(sends):
        received.append(swap(send, 2 * (step + 1), count))
    return received


def pair_up(near, count):
    blocks = []
    for block in near:
        blocks += [block, swap(block, 1, count)]
    return blocks


def gather_blocks(own, count):
    near = [own] + far_swaps([own] * (count // 2 - 1), count)
    return pair_up(near, count)


def entry_kernel(gate_hbm, up_hbm, down_hbm, mark_ref):
    mark_ref[...] = jnp.zeros_like(mark_ref)


def enter(*weights):
    arrays = [pltpu.with_memory_space_constraint(a, pltpu.HBM) for a in weights]
    return call(
        entry_kernel,
        pltpu.VMEM((8, 128), F32),
        arrays,
        in_specs=[HBM_SPEC] * len(arrays),
        limit=1 << 20,
    )


def stage_kernel(count, *refs):
    sources, targets, sem = refs[:count], refs[count : 2 * count], refs[2 * count]
    copies = [pltpu.make_async_copy(*pair, sem.at[i]) for i, pair in enumerate(zip(sources, targets))]
    for copy in copies:
        copy.start()
    for copy in copies:
        copy.wait()


def stage(*arrays):
    return call(
        functools.partial(stage_kernel, len(arrays)),
        [pltpu.VMEM(a.shape, a.dtype) for a in arrays],
        [pltpu.with_memory_space_constraint(a, pltpu.HBM) for a in arrays],
        in_specs=[HBM_SPEC] * len(arrays),
        scratch=[pltpu.SemaphoreType.DMA((len(arrays),))],
        limit=1 << 20,
    )


def core_span(units):
    tiles = units // 128
    span = -(-tiles // 2) * 128
    return span, units - span


def gained(block, owner, gain_ref):
    width = block.shape[1]
    column = pl.multiple_of(owner * width, width)
    values = block[...].astype(F32)
    squares = values * values
    folded = squares[:, :128]
    for first in range(128, width, 128):
        folded = folded + squares[:, first : first + 128]
    return (values * gain_ref[:, pl.ds(column, width)]).astype(BF16), folded


def scale_of_rows(folded, channels):
    return lax.rsqrt(jnp.sum(folded, axis=1, keepdims=True) / channels + EPSILON)


def plus(total, part):
    return part if total is None else total + part


def early_masks(count):
    late = (3, 5) if count > 4 else (3,)
    return [m for m in range(count) if m not in late], list(late)


def entry_kernel(gate_hbm, up_hbm, down_hbm, mark_ref):
    mark_ref[...] = jnp.zeros_like(mark_ref)


def enter(*weights):
    arrays = [pltpu.with_memory_space_constraint(a, pltpu.HBM) for a in weights]
    return call(
        entry_kernel,
        pltpu.VMEM((8, 128), F32),
        arrays,
        in_specs=[HBM_SPEC] * len(arrays),
        limit=1 << 20,
    )


def core_span(units):
    tiles = units // 128
    span = -(-tiles // 2) * 128
    return span, units - span


def units_of(blocks, masks, gain_ref, gate_ref, up_ref, span, skip):
    index = my_index()
    start = pl.multiple_of(lax.axis_index("tp") * skip, 128)
    gate_acc = up_acc = squares = None
    for mask, block in zip(masks, blocks):
        owner = index ^ mask
        width = block.shape[1]
        rows = pl.ds(pl.multiple_of(owner * width, width), width)
        lhs, folded = gained(block, owner, gain_ref)
        squares = plus(squares, folded)
        columns = pl.ds(start, span)
        gate_acc = plus(gate_acc, jnp.dot(lhs, gate_ref[rows, columns], preferred_element_type=F32))
        up_acc = plus(up_acc, jnp.dot(lhs, up_ref[rows, columns], preferred_element_type=F32))
    return gate_acc, up_acc, squares


def ffn_early_kernel(masks, span, skip, *refs):
    blocks = refs[: len(masks)]
    gain_ref, gate_ref, up_ref, _, _, gate_out, up_out, squares_out = refs[len(masks) :]
    gate_out[...], up_out[...], squares_out[...] = units_of(
        blocks, masks, gain_ref, gate_ref, up_ref, span, skip
    )


def ffn_late_kernel(masks, count, span, skip, *refs):
    blocks = refs[: len(masks)]
    gain_ref, gate_ref, up_ref, down_ref, gate_in, up_in, squares_in = refs[len(masks) : len(masks) + 7]
    hidden_ref, cross_ref = refs[len(masks) + 7 :]
    gate_acc, up_acc, squares = units_of(blocks, masks, gain_ref, gate_ref, up_ref, span, skip)
    channels = gate_ref.shape[0]
    row_scale = scale_of_rows(squares + squares_in[...], channels)
    gate_act = (gate_acc + gate_in[...]) * row_scale
    hidden = gate_act * jax.nn.sigmoid(gate_act) * ((up_acc + up_in[...]) * row_scale)
    repeated = lax.axis_index("tp") * (lax.axis_size("tp") * span - down_ref.shape[0])
    unit = lax.broadcasted_iota(jnp.int32, hidden.shape, 1)
    hidden_ref[...] = jnp.where(unit >= repeated, hidden, 0.0).astype(BF16)
    hidden = hidden_ref[...]
    down_products(hidden, down_ref, range(1, count, 2), cross_ref, skip)


def down_products(hidden, down_ref, masks, out_ref, skip):
    index = my_index()
    start = pl.multiple_of(lax.axis_index("tp") * skip, 128)
    span, width = hidden.shape[1], out_ref.shape[2]
    for place, mask in enumerate(masks):
        column = pl.multiple_of((index ^ mask) * width, width)
        weight = down_ref[pl.ds(start, span), pl.ds(column, width)]
        out_ref[place] = jnp.dot(hidden, weight, preferred_element_type=F32).astype(out_ref.dtype)


def ffn_own_kernel(count, skip, hidden_ref, down_ref, own_ref):
    down_products(hidden_ref[...], down_ref, range(0, count, 2), own_ref, skip)


def pair_sum_kernel(own_ref, cross_ref, mine_ref, *sends):
    mine_ref[...] = own_ref[0] + cross_ref[0].astype(F32)
    for step, send in enumerate(sends):
        send[...] = (own_ref[step + 1] + cross_ref[step + 1].astype(F32)).astype(BF16)


def residual_kernel(base_ref, mine_ref, *refs):
    total = mine_ref[...]
    for received in refs[:-1]:
        total = total + received[...].astype(F32)
    refs[-1][...] = (base_ref[...].astype(F32) + 0.5 * total).astype(BF16)


def half_step(own, mark, count, gain, gate, up, down, first=False, last=False):
    rows, width = own.shape
    near = count // 2
    span, skip = core_span(down.shape[0])
    gain = gain.reshape(1, count * width)
    near_own = own
    if first:
        own, gain = stage(own, gain)
    received = far_swaps([near_own] * (near - 1), count)
    blocks = pair_up([own, *received], count)
    early, late = early_masks(count)
    parts_early = call(
        functools.partial(ffn_early_kernel, early, span, skip),
        [pltpu.VMEM((rows, span), F32)] * 2 + [pltpu.VMEM((rows, 128), F32)],
        [*(blocks[m] for m in early), gain, gate, up, down, mark],
    )
    hidden, cross_part = call(
        functools.partial(ffn_late_kernel, late, count, span, skip),
        [pltpu.VMEM((rows, span), BF16), pltpu.VMEM((near, rows, width), BF16)],
        [*(blocks[m] for m in late), gain, gate, up, down, *parts_early],
    )
    cross_sum = swap(cross_part, 1, count)
    own_part = call(
        functools.partial(ffn_own_kernel, count, skip),
        pltpu.VMEM((near, rows, width), F32),
        [hidden, down],
    )
    mine, *sends = call(
        pair_sum_kernel,
        [pltpu.VMEM((rows, width), F32)] + [pltpu.VMEM((rows, width), BF16)] * (near - 1),
        [own_part, cross_sum],
    )
    received = far_swaps(sends, count)
    shape = jax.ShapeDtypeStruct if last else pltpu.VMEM
    return call(residual_kernel, shape((rows, width), BF16), [own, mine, *received])


def mixes_of(blocks, masks, gain_ref, weights, thin):
    index = my_index()
    wide = [None] * len(weights)
    narrow = [None] * len(thin)
    squares = None
    across = (((1,), (1,)), ((), ()))
    for mask, block in zip(masks, blocks):
        owner = index ^ mask
        width = block.shape[1]
        rows = pl.ds(pl.multiple_of(owner * width, width), width)
        lhs, folded = gained(block, owner, gain_ref)
        squares = plus(squares, folded)
        for place, weight in enumerate(weights):
            wide[place] = plus(wide[place], jnp.dot(lhs, weight[rows, :], preferred_element_type=F32))
        for place, weight in enumerate(thin):
            part = lax.dot_general(lhs, weight[:, rows], across, preferred_element_type=F32)
            narrow[place] = plus(narrow[place], part)
    return wide, narrow, squares


def project_early_kernel(masks, *refs):
    blocks = refs[: len(masks)]
    gain_ref, *weights = refs[len(masks) : len(masks) + 7]
    result, pre, squares_out = refs[len(masks) + 7 :]
    wide, narrow, squares_out[...] = mixes_of(blocks, masks, gain_ref, weights[:4], weights[4:])
    for place, part in enumerate(wide):
        width = part.shape[1]
        result[:, place * width : (place + 1) * width] = part
    for place, part in enumerate(narrow):
        width = part.shape[1]
        pre[:, place * width : (place + 1) * width] = part


def project_late_kernel(masks, *refs):
    blocks = refs[: len(masks)]
    gain_ref, *weights = refs[len(masks) : len(masks) + 7]
    result_in, pre_in, squares_in = refs[len(masks) + 7 : len(masks) + 10]
    *sends, pre_ref, result, pre_scratch = refs[len(masks) + 10 :]
    wide, narrow, squares = mixes_of(blocks, masks, gain_ref, weights[:4], weights[4:])
    row_scale = scale_of_rows(squares + squares_in[...], weights[0].shape[0])
    for place, part in enumerate(wide):
        width = part.shape[1]
        columns = slice(place * width, (place + 1) * width)
        result[:, columns] = (part + result_in[:, columns]) * row_scale
    for place, part in enumerate(narrow):
        width = part.shape[1]
        columns = slice(place * width, (place + 1) * width)
        pre_scratch[:, columns] = (part + pre_in[:, columns]) * row_scale
    for step, send in enumerate(sends):
        rows = send.shape[0]
        row = pl.multiple_of((lax.axis_index("kv") ^ step) * rows, rows)
        send[...] = result[pl.ds(row, rows), :].astype(BF16)
    row = pl.multiple_of(my_index() * BLK, BLK)
    pre_ref[...] = pre_scratch[pl.ds(row, BLK), :]


def parts(value):
    high = value.astype(BF16)
    return high, (value - high.astype(F32)).astype(BF16)


def dot_parts(left, right, dims=(((1,), (0,)), ((), ()))):
    left_high, left_low = left
    right_high, right_low = right
    total = lax.dot_general(left_high, right_low, dims, preferred_element_type=F32)
    total = total + lax.dot_general(left_low, right_high, dims, preferred_element_type=F32)
    return total + lax.dot_general(left_high, right_high, dims, preferred_element_type=F32)


def split_state_kernel(state_ref, length_ref, high_ref, low_ref, live_ref):
    high_ref[...], low_ref[...] = parts(state_ref[...])
    step_of = lax.broadcasted_iota(jnp.int32, live_ref.shape, 0)
    live_ref[...] = (step_of < length_ref[...]).astype(F32)


def delta_kernel(masks, count, *refs):
    blocks = refs[: len(masks)]
    pre_ref, rate_ref, live_ref, high_ref, low_ref = refs[len(masks) : len(masks) + 5]
    mixed_ref, update_ref, faded_ref, final_ref = refs[len(masks) + 5 :]
    index = my_index()
    first_core = lax.axis_index("tp") == 0
    size = high_ref.shape[-1]
    all_heads = rate_ref.shape[1]
    per_block = all_heads // count
    heads = per_block * len(masks)
    rows = heads * BLK
    width = per_block * size
    taken = []
    for block in blocks:
        both = block[...].astype(F32)
        taken.append(jnp.where(first_core, both[:BLK], both[BLK:]))

    def stack(place):
        found = []
        for block in taken:
            for head in range(per_block):
                column = place * width + head * size
                found.append(block[:, column : column + size])
        return jnp.stack(found)

    def head_at(head):
        return (index ^ masks[head // per_block]) * per_block + head % per_block

    def lane_sum(array):
        return jnp.sum(array, axis=-1, keepdims=True)

    query, key_in, value, gating = (stack(place) for place in range(4))
    query_unit = query * lax.rsqrt(lane_sum(query * query) + EPSILON) * (1.0 / math.sqrt(size))
    key_unit = key_in * lax.rsqrt(lane_sum(key_in * key_in) + EPSILON)
    step_of = lax.broadcasted_iota(jnp.int32, (BLK, all_heads), 0)
    head_of = lax.broadcasted_iota(jnp.int32, (BLK, all_heads), 1)
    live = live_ref[...]
    pre = pre_ref[...]
    write_gate = jax.nn.sigmoid(pre[:, :all_heads]) * live
    forget_in = pre[:, all_heads:]
    softplus = jnp.maximum(forget_in, 0.0) + jnp.log1p(jnp.exp(-jnp.abs(forget_in)))
    cumulative = -jnp.exp(rate_ref[...]) * softplus * live
    lower = 1
    while lower < BLK:
        moved = pltpu.roll(cumulative, lower, 0)
        cumulative = cumulative + jnp.where(step_of >= lower, moved, 0.0)
        lower *= 2

    def columns_of(array):
        found = [lane_sum(jnp.where(head_of == head_at(head), array, 0.0)) for head in range(heads)]
        return jnp.broadcast_to(jnp.stack(found), (heads, BLK, size))

    write_col, cum = columns_of(write_gate), columns_of(cumulative)
    live_col = live[:, :1][None]
    growth = jnp.exp(cum)
    key_grown, query_grown = key_unit * growth, query_unit * growth
    from_key, from_query = [], []
    for head in range(heads):
        both = jnp.concatenate([key_grown[head], query_grown[head]], axis=0)
        found = dot_parts(parts(both), (high_ref[head_at(head)], low_ref[head_at(head)]))
        from_key.append(found[:BLK])
        from_query.append(found[BLK:])
    update = write_col * (value - jnp.stack(from_key))
    attend = jnp.stack(from_query)
    row_at = lax.broadcasted_iota(jnp.int32, (heads, BLK, size), 1)
    for step in range(BLK):

        def row_of(array):
            return jnp.broadcast_to(array[:, step : step + 1, :], array.shape)

        key_row = row_of(key_unit)
        decay = jnp.exp(jnp.minimum(cum - row_of(cum), 0.0))
        score = jnp.where(row_at >= step, decay * lane_sum(query_unit * key_row), 0.0)
        update_row = row_of(update)
        attend = attend + score * update_row
        if step < BLK - 1:
            strict = jnp.where(row_at > step, write_col * decay * lane_sum(key_unit * key_row), 0.0)
            update = update - strict * update_row
    normed = attend * lax.rsqrt(lane_sum(attend * attend) / size + EPSILON)
    normed = (normed * (gating * jax.nn.sigmoid(gating)) * live_col).astype(BF16)
    final = jnp.broadcast_to(cum[:, BLK - 1 :, :], cum.shape)
    for head in range(heads):
        mixed_ref[:, head * size : (head + 1) * size] = normed[head]
    update_ref[...] = update.reshape(rows, size)
    faded_ref[...] = (key_unit * jnp.exp(final - cum)).reshape(rows, size)
    final_ref[...] = jnp.exp(final).reshape(rows, size)


def join_kernel(count, first_ref, second_ref, mixed_ref):
    width = mixed_ref.shape[1] // count
    index = my_index()
    for mask in range(count):
        source = second_ref if mask % 2 else first_ref
        place = mask // 2
        column = pl.multiple_of((index ^ mask) * width, width)
        mixed_ref[:, pl.ds(column, width)] = source[:, place * width : (place + 1) * width]


def state_kernel(groups, count, *refs):
    state_ref, new_ref = refs[3 * len(groups) :]
    per_block = state_ref.shape[0] // count
    index = my_index()
    along = (((0,), (0,)), ((), ()))
    for place, masks in enumerate(groups):
        update_ref, faded_ref, final_ref = refs[3 * place : 3 * place + 3]
        for head in range(per_block * len(masks)):
            at = slice(head * BLK, (head + 1) * BLK)
            left_high, left_low = parts(faded_ref[at])
            right_high, right_low = parts(update_ref[at])
            left = jnp.concatenate([left_high, left_high, left_low, left_low], axis=0)
            right = jnp.concatenate([right_high, right_low, right_high, right_low], axis=0)
            grown = lax.dot_general(left, right, along, preferred_element_type=F32)
            scale = final_ref[head * BLK : head * BLK + 1, :]
            owner = (index ^ masks[head // per_block]) * per_block + head % per_block
            new_ref[pl.ds(owner, 1)] = (scale * state_ref[owner] + grown)[None]


def out_kernel(count, *refs):
    blocks = refs[:count]
    weight_ref, base_ref, out_ref, scratch = refs[count:]
    index = my_index()
    lhs = jnp.concatenate([block[...].astype(F32) for block in blocks], axis=0).astype(BF16)
    half = lhs.shape[1] // 2
    first = jnp.dot(lhs[:, :half], weight_ref[:half, :], preferred_element_type=F32).astype(BF16)
    second = jnp.dot(lhs[:, half:], weight_ref[half:, :], preferred_element_type=F32).astype(BF16)
    total = first.astype(F32) + second.astype(F32)
    for mask in range(count):
        row = pl.multiple_of((index ^ mask) * BLK, BLK)
        scratch[pl.ds(row, BLK), :] = total[mask * BLK : (mask + 1) * BLK]
    out_ref[...] = (base_ref[...].astype(F32) + scratch[...]).astype(BF16)


def group_device(
    tokens,
    lengths,
    state,
    gain_first,
    first_gate,
    first_up,
    first_down,
    gain_mix,
    query_weight,
    key_weight,
    value_weight,
    gating_weight,
    write_weight,
    forget_weight,
    forget_rate,
    out_weight,
    gain_second,
    second_gate,
    second_up,
    second_down,
):
    count = lax.axis_size("kv") * lax.axis_size("tp")
    rows, width = tokens.shape
    channels = gain_first.shape[0]
    heads, size = state.shape[1], state.shape[2]
    mark = enter(first_gate, first_up, first_down)
    after_first = half_step(
        tokens, mark, count, gain_first, first_gate, first_up, first_down, first=True
    )
    blocks = gather_blocks(after_first, count)
    columns = 4 * width
    near = count // 2
    early, late = early_masks(count)
    mixers = [
        gain_mix.reshape(1, channels),
        query_weight,
        key_weight,
        value_weight,
        gating_weight,
        write_weight.T,
        forget_weight.T,
    ]
    parts_early = call(
        functools.partial(project_early_kernel, early),
        [
            pltpu.VMEM((rows, columns), F32),
            pltpu.VMEM((rows, 2 * heads), F32),
            pltpu.VMEM((rows, 128), F32),
        ],
        [*(blocks[m] for m in early), *mixers],
    )
    *sends, pre = call(
        functools.partial(project_late_kernel, late),
        [pltpu.VMEM((rows // near, columns), BF16)] * near + [pltpu.VMEM((BLK, 2 * heads), F32)],
        [*(blocks[m] for m in late), *mixers, *parts_early],
        scratch=[pltpu.VMEM((rows, columns), F32), pltpu.VMEM((rows, 2 * heads), F32)],
    )
    owned = pair_up([sends[0]] + far_swaps(sends[1:], count), count)
    matrices = state.reshape(heads, size, size)
    high, low, live = call(
        split_state_kernel,
        [pltpu.VMEM(matrices.shape, BF16)] * 2 + [pltpu.VMEM((BLK, heads), F32)],
        [matrices, lengths.reshape(1, 1)],
        limit=3 << 20,
    )
    groups = [list(range(0, count, 2)), list(range(1, count, 2))]
    mixed_parts, grown = [], []
    for masks in groups:
        tall = heads * BLK // 2
        part, *rest = call(
            functools.partial(delta_kernel, masks, count),
            [pltpu.VMEM((BLK, channels // 2), BF16)] + [pltpu.VMEM((tall, size), F32)] * 3,
            [
                *(owned[m] for m in masks),
                pre,
                forget_rate.reshape(1, heads),
                live,
                high,
                low,
            ],
        )
        mixed_parts.append(part)
        grown += rest
    mixed = call(
        functools.partial(join_kernel, count), pltpu.VMEM((BLK, channels), BF16), mixed_parts
    )
    head_blocks = gather_blocks(mixed, count)
    new_state = call(
        functools.partial(state_kernel, groups, count),
        jax.ShapeDtypeStruct((heads, size, size), F32),
        [*grown, matrices],
    )
    after_mix = call(
        functools.partial(out_kernel, count),
        pltpu.VMEM((rows, width), BF16),
        [*head_blocks, out_weight, after_first],
        scratch=[pltpu.VMEM((rows, width), F32)],
    )
    mixed_out = half_step(
        after_mix, mark, count, gain_second, second_gate, second_up, second_down, last=True
    )
    return (mixed_out, new_state.reshape(state.shape))


def fits_group(mesh):
    near, cores = mesh.shape["kv"], mesh.shape["tp"]
    count = near * cores
    return cores == 2 and near & (near - 1) == 0 and near <= 8 and (HEADS * HEAD) % (count * 128) == 0


def per_device(mesh, *arrays):
    lengths, gate = arrays[1], arrays[4]
    suits = fits_group(mesh) and lengths.shape[0] == 1 and gate.shape[1] % 128 == 0
    if not suits:
        return general_device(*arrays)
    return group_device(*arrays)


def solution(mesh):
    in_specs = (
        P("dp", ("kv", "tp")),
        P(("dp", "kv", "tp")),
        P(("dp", "kv", "tp"), None, None, None),
        P(),
        P(None, "kv"),
        P(None, "kv"),
        P("kv", None),
        P(),
        P(None, ("kv", "tp")),
        P(None, ("kv", "tp")),
        P(None, ("kv", "tp")),
        P(None, ("kv", "tp")),
        P(),
        P(),
        P(),
        P(None, ("kv", "tp")),
        P(),
        P(None, "kv"),
        P(None, "kv"),
        P("kv", None),
    )
    out_specs = (P("dp", ("kv", "tp")), P(("dp", "kv", "tp"), None, None, None))
    return jax.shard_map(
        functools.partial(per_device, mesh),
        mesh=mesh,
        in_specs=in_specs,
        out_specs=out_specs,
        check_vma=False,
    )
```

```python
import functools
import math

import jax
import jax.numpy as jnp
from jax import lax
from jax.experimental import pallas as pl
from jax.experimental.pallas import tpu as pltpu
from jax.sharding import PartitionSpec as P


HEADS = 16
HEAD = 128
BLK = 8


EPSILON = 1e-06


def fold_step(gain, gate_cols, up_cols, portion):
    values = portion.astype(jnp.float32)
    scaled = (values * gain).astype(jnp.bfloat16)
    gate_acc = jnp.dot(scaled, gate_cols, preferred_element_type=jnp.float32)
    up_acc = jnp.dot(scaled, up_cols, preferred_element_type=jnp.float32)
    squares = jnp.sum(values * values, axis=1)
    return (gate_acc, up_acc, squares)


def finish_units(gate_acc, up_acc, squares, channels, down_rows):
    row_scale = lax.rsqrt(squares / channels + EPSILON)[:, None]
    hidden = (jax.nn.silu(gate_acc * row_scale) * (up_acc * row_scale)).astype(jnp.bfloat16)
    return jnp.dot(hidden, down_rows, preferred_element_type=jnp.float32)


def feed_forward(hidden_in, gain, w_gate, w_up, w_down):
    channels = gain.shape[0]
    paired = lax.all_to_all(hidden_in, "tp", split_axis=0, concat_axis=1, tiled=True)
    gate_acc, up_acc, squares = fold_step(
        gain, w_gate, w_up, lax.all_gather(paired, "kv", axis=1, tiled=True)
    )
    ffn_term = finish_units(gate_acc, up_acc, squares, channels, w_down)
    partial_value = lax.psum_scatter(ffn_term, "kv", scatter_dimension=1, tiled=True)
    summed = lax.all_to_all(partial_value, "tp", split_axis=1, concat_axis=0, tiled=True)
    return (hidden_in.astype(jnp.float32) + 0.5 * summed).astype(jnp.bfloat16)


def delta_block(query, key_in, value, gating, write_pre, forget_pre, rates, live, state):
    seq_count, block_len, head_count, head_size = query.shape
    precise = lax.Precision.HIGHEST
    query_unit = (
        query
        * lax.rsqrt(jnp.sum(query * query, axis=-1, keepdims=True) + EPSILON)
        / math.sqrt(head_size)
    )
    key_unit = key_in * lax.rsqrt(jnp.sum(key_in * key_in, axis=-1, keepdims=True) + EPSILON)
    live_rows = live[:, :, None]
    write_gate = jax.nn.sigmoid(write_pre) * live_rows
    forget = -jnp.exp(rates)[None, None, :] * jax.nn.softplus(forget_pre) * live_rows
    cumulative = jnp.cumsum(forget, axis=1)
    cum_heads = jnp.transpose(cumulative, (0, 2, 1))
    positions = jnp.arange(block_len)
    causal = positions[:, None] >= positions[None, :]
    strict = positions[:, None] > positions[None, :]
    differ = jnp.minimum(cum_heads[:, :, :, None] - cum_heads[:, :, None, :], 0.0)
    decay_mat = jnp.where(causal, jnp.exp(differ), 0.0)
    key_dots = jnp.einsum("sthd,suhd->shtu", key_unit, key_unit, precision=precise)
    write_heads = jnp.transpose(write_gate, (0, 2, 1))
    strict_part = jnp.where(strict, write_heads[:, :, :, None] * decay_mat * key_dots, 0.0)
    identity = jnp.eye(block_len, dtype=jnp.float32)
    squared = jnp.einsum("shtu,shuv->shtv", strict_part, strict_part, precision=precise)
    fourth = jnp.einsum("shtu,shuv->shtv", squared, squared, precision=precise)
    inverse = jnp.einsum(
        "shtu,shuv->shtv", identity - strict_part, identity + squared, precision=precise
    )
    inverse = jnp.einsum("shtu,shuv->shtv", inverse, identity + fourth, precision=precise)
    growth = jnp.exp(cumulative)
    target = jnp.einsum(
        "shtu,suhv->sthv", inverse, write_gate[..., None] * value, precision=precise
    )
    key_mix = jnp.einsum(
        "shtu,suhk->sthk", inverse, (write_gate * growth)[..., None] * key_unit, precision=precise
    )
    update = target - jnp.einsum("sthk,shkv->sthv", key_mix, state, precision=precise)
    scores = jnp.einsum("sthd,suhd->shtu", query_unit, key_unit, precision=precise) * decay_mat
    attend = jnp.einsum("sthk,shkv->sthv", query_unit * growth[..., None], state, precision=precise)
    attend = attend + jnp.einsum("shtu,suhv->sthv", scores, update, precision=precise)
    final_cum = cumulative[:, -1:, :]
    fading = jnp.exp(final_cum - cumulative)
    new_state = jnp.exp(final_cum[:, 0, :])[:, :, None, None] * state
    new_state = new_state + jnp.einsum(
        "sthk,sthv->shkv", key_unit * fading[..., None], update, precision=precise
    )
    normed = attend * lax.rsqrt(jnp.mean(attend * attend, axis=-1, keepdims=True) + EPSILON)
    normed = normed * jax.nn.silu(gating) * live[:, :, None, None]
    mixed_heads = normed.reshape(seq_count * block_len, head_count * head_size).astype(jnp.bfloat16)
    return (mixed_heads, new_state)


def general_device(
    tokens,
    lengths,
    state,
    gain_first,
    first_gate,
    first_up,
    first_down,
    gain_mix,
    query_weight,
    key_weight,
    value_weight,
    gating_weight,
    write_weight,
    forget_weight,
    forget_rate,
    out_weight,
    gain_second,
    second_gate,
    second_up,
    second_down,
):
    after_first = feed_forward(tokens, gain_first, first_gate, first_up, first_down)
    seq_count = lengths.shape[0]
    own_count = seq_count * BLK
    whole_rows = lax.all_gather(after_first, ("kv", "tp"), axis=1, tiled=True)
    scaled_all = (whole_rows.astype(jnp.float32) * gain_mix).astype(jnp.bfloat16)
    stacked = jnp.stack(
        [
            jnp.dot(scaled_all, matrix, preferred_element_type=jnp.float32)
            for matrix in (query_weight, key_weight, value_weight, gating_weight)
        ]
    )
    owned = lax.all_to_all(
        stacked.astype(jnp.bfloat16), ("kv", "tp"), split_axis=1, concat_axis=2, tiled=True
    ).astype(stacked.dtype)
    row_start = lax.axis_index(("kv", "tp")) * own_count
    own_values = lax.dynamic_slice_in_dim(whole_rows, row_start, own_count, 0).astype(jnp.float32)
    own_scaled = lax.dynamic_slice_in_dim(scaled_all, row_start, own_count, 0)
    mix_scale = lax.rsqrt(jnp.mean(own_values * own_values, axis=1, keepdims=True) + EPSILON)
    query = (owned[0] * mix_scale).reshape(seq_count, BLK, HEADS, HEAD)
    key_in = (owned[1] * mix_scale).reshape(seq_count, BLK, HEADS, HEAD)
    value = (owned[2] * mix_scale).reshape(seq_count, BLK, HEADS, HEAD)
    gating = (owned[3] * mix_scale).reshape(seq_count, BLK, HEADS, HEAD)
    write_pre = (
        jnp.dot(own_scaled, write_weight, preferred_element_type=jnp.float32) * mix_scale
    ).reshape(seq_count, BLK, HEADS)
    forget_pre = (
        jnp.dot(own_scaled, forget_weight, preferred_element_type=jnp.float32) * mix_scale
    ).reshape(seq_count, BLK, HEADS)
    positions = jnp.arange(BLK, dtype=jnp.int32)
    live = (positions[None, :] < lengths[:, None]).astype(jnp.float32)
    mixed_heads, new_state = delta_block(
        query, key_in, value, gating, write_pre, forget_pre, forget_rate, live, state
    )
    half_cols = mixed_heads.shape[1] // 2
    portion = lax.all_gather(mixed_heads, ("kv", "tp"), axis=0, tiled=True)
    first_half = jnp.dot(
        portion[:, :half_cols], out_weight[:half_cols], preferred_element_type=jnp.float32
    ).astype(jnp.bfloat16)
    second_half = jnp.dot(
        portion[:, half_cols:], out_weight[half_cols:], preferred_element_type=jnp.float32
    ).astype(jnp.bfloat16)
    first_half, second_half = lax.optimization_barrier((first_half, second_half))
    mixed_sum = first_half.astype(jnp.float32) + second_half.astype(jnp.float32)
    after_mix = (after_first.astype(jnp.float32) + mixed_sum).astype(jnp.bfloat16)
    mixed_out = feed_forward(after_mix, gain_second, second_gate, second_up, second_down)
    return (mixed_out, new_state)


VMEM_SPEC = pl.BlockSpec(memory_space=pltpu.VMEM)
HBM_SPEC = pl.BlockSpec(memory_space=pltpu.HBM)
GROUP = ("kv", "tp")
LIVE_HALVES = 7
F32, BF16 = jnp.float32, jnp.bfloat16


def call(body, out_shapes, args, in_specs=None, scratch=(), limit=5 << 20, out_specs=None):
    single = not isinstance(out_shapes, (list, tuple))
    shapes = [out_shapes] if single else list(out_shapes)
    outs = pl.pallas_call(
        body,
        out_shape=shapes,
        in_specs=in_specs or [VMEM_SPEC] * len(args),
        out_specs=out_specs or [VMEM_SPEC] * len(shapes),
        scratch_shapes=list(scratch),
        compiler_params=pltpu.CompilerParams(vmem_limit_bytes=limit),
    )(*args)
    return outs[0] if single else outs


def my_index():
    return lax.axis_index("kv") * lax.axis_size("tp") + lax.axis_index("tp")


def swap(value, mask, count):
    return lax.ppermute(value, GROUP, [(i, i ^ mask) for i in range(count)])


def far_swaps(sends, count):
    received = []
    for step, send in enumerate(sends):
        received.append(swap(send, 2 * (step + 1), count))
    return received


def pair_up(near, count):
    blocks = []
    for block in near:
        blocks += [block, swap(block, 1, count)]
    return blocks


def gather_blocks(own, count):
    near = [own] + far_swaps([own] * (count // 2 - 1), count)
    return pair_up(near, count)


def entry_kernel(length_ref, tokens_hbm, gain_hbm, gate_hbm, up_hbm, down_hbm, *refs):
    tokens_ref, gain_ref, sem = refs
    rows = tokens_hbm.shape[0]
    copies = [
        pltpu.make_async_copy(tokens_hbm, tokens_ref.at[pl.ds(0, rows)], sem.at[0]),
        pltpu.make_async_copy(gain_hbm, gain_ref, sem.at[1]),
    ]
    for copy in copies:
        copy.start()
    tail = (BLK, tokens_ref.shape[1])
    tokens_ref[pl.ds(rows, BLK), :] = jnp.full(tail, length_ref[0].astype(F32)).astype(BF16)
    for copy in copies:
        copy.wait()


def enter(tokens, gain, lengths, *weights):
    arrays = [tokens, gain, *weights]
    arrays = [pltpu.with_memory_space_constraint(a, pltpu.HBM) for a in arrays]
    rows, width = tokens.shape
    return call(
        entry_kernel,
        [pltpu.VMEM((rows + BLK, width), BF16), pltpu.VMEM(gain.shape, F32)],
        [lengths, *arrays],
        in_specs=[pl.BlockSpec(memory_space=pltpu.SMEM)] + [HBM_SPEC] * len(arrays),
        scratch=[pltpu.SemaphoreType.DMA((2,))],
        limit=1 << 20,
    )


def core_span(units):
    tiles = units // 128
    span = -(-tiles // 2) * 128
    return span, units - span


def gained(block, owner, gain_ref):
    width = block.shape[1]
    column = pl.multiple_of(owner * width, width)
    values = block[...].astype(F32)
    squares = values * values
    folded = squares[:, :128]
    for first in range(128, width, 128):
        folded = folded + squares[:, first : first + 128]
    return (values * gain_ref[:, pl.ds(column, width)]).astype(BF16), folded


def scale_of_rows(folded, channels):
    return lax.rsqrt(jnp.sum(folded, axis=1, keepdims=True) / channels + EPSILON)


def plus(total, part):
    return part if total is None else total + part


def early_masks(count):
    late = (3, 5) if count > 4 else (3,)
    return [m for m in range(count) if m not in late], list(late)


def units_of(blocks, masks, gain_ref, gate_ref, up_ref, span, skip, row_count):
    index = my_index()
    blocks = [block.at[pl.ds(0, row_count)] for block in blocks]
    start = pl.multiple_of(lax.axis_index("tp") * skip, 128)
    gate_acc = up_acc = squares = None
    for mask, block in zip(masks, blocks):
        owner = index ^ mask
        width = block.shape[1]
        rows = pl.ds(pl.multiple_of(owner * width, width), width)
        lhs, folded = gained(block, owner, gain_ref)
        squares = plus(squares, folded)
        columns = pl.ds(start, span)
        gate_acc = plus(gate_acc, jnp.dot(lhs, gate_ref[rows, columns], preferred_element_type=F32))
        up_acc = plus(up_acc, jnp.dot(lhs, up_ref[rows, columns], preferred_element_type=F32))
    return gate_acc, up_acc, squares


def ffn_early_kernel(masks, span, skip, *refs):
    blocks = refs[: len(masks)]
    gain_ref, gate_ref, up_ref, _, gate_out, up_out, squares_out = refs[len(masks) :]
    gate_out[...], up_out[...], squares_out[...] = units_of(
        blocks, masks, gain_ref, gate_ref, up_ref, span, skip, gate_out.shape[0]
    )


def ffn_late_kernel(masks, count, span, skip, *refs):
    blocks = refs[: len(masks)]
    gain_ref, gate_ref, up_ref, down_ref, gate_in, up_in, squares_in = refs[len(masks) : len(masks) + 7]
    hidden_ref, cross_ref = refs[len(masks) + 7 :]
    gate_acc, up_acc, squares = units_of(
        blocks, masks, gain_ref, gate_ref, up_ref, span, skip, gate_in.shape[0]
    )
    channels = gate_ref.shape[0]
    row_scale = scale_of_rows(squares + squares_in[...], channels)
    gate_act = (gate_acc + gate_in[...]) * row_scale
    hidden = gate_act * jax.nn.sigmoid(gate_act) * ((up_acc + up_in[...]) * row_scale)
    repeated = lax.axis_index("tp") * (lax.axis_size("tp") * span - down_ref.shape[0])
    unit = lax.broadcasted_iota(jnp.int32, hidden.shape, 1)
    hidden_ref[...] = jnp.where(unit >= repeated, hidden, 0.0).astype(BF16)
    hidden = hidden_ref[...]
    down_products(hidden, down_ref, range(1, count, 2), cross_ref, skip)


def down_products(hidden, down_ref, masks, out_ref, skip):
    index = my_index()
    start = pl.multiple_of(lax.axis_index("tp") * skip, 128)
    span, width = hidden.shape[1], out_ref.shape[2]
    for place, mask in enumerate(masks):
        column = pl.multiple_of((index ^ mask) * width, width)
        weight = down_ref[pl.ds(start, span), pl.ds(column, width)]
        out_ref[place] = jnp.dot(hidden, weight, preferred_element_type=F32).astype(out_ref.dtype)


def ffn_own_kernel(count, skip, hidden_ref, down_ref, own_ref):
    down_products(hidden_ref[...], down_ref, range(0, count, 2), own_ref, skip)


def pair_sum_kernel(own_ref, cross_ref, mine_ref, *sends):
    mine_ref[...] = own_ref[0] + cross_ref[0].astype(F32)
    for step, send in enumerate(sends):
        send[...] = (own_ref[step + 1] + cross_ref[step + 1].astype(F32)).astype(BF16)


def residual_kernel(base_ref, mine_ref, *refs):
    total = mine_ref[...]
    for received in refs[:-1]:
        total = total + received[...].astype(F32)
    refs[-1][...] = (base_ref[...].astype(F32) + 0.5 * total).astype(BF16)


def live_kernel(count, rows, *refs):
    blocks, pick_ref = refs[:count], refs[count]
    index = my_index()
    lane = lax.broadcasted_iota(jnp.int32, (BLK, rows), 1)
    lengths = jnp.zeros((BLK, rows), F32)
    for mask, block in enumerate(blocks):
        length = block[pl.ds(rows, BLK), :rows].astype(F32)
        lengths = jnp.where(lane // BLK == (index ^ mask), length, lengths)
    live = (lane % BLK).astype(F32) < lengths
    before = lax.broadcasted_iota(jnp.int32, (rows, rows), 0) < lax.broadcasted_iota(
        jnp.int32, (rows, rows), 1
    )
    rank = jnp.dot(live.astype(BF16), before.astype(BF16), preferred_element_type=F32)
    rank = jnp.where(live, rank, -1.0)[:1]
    wanted = lax.broadcasted_iota(jnp.int32, pick_ref.shape, 0).astype(F32)
    pick_ref[...] = (rank == wanted).astype(F32).astype(BF16)


def spread_kernel(near, pick_ref, own_ref, cross_ref, mine_ref, kept_ref, *sends):
    pick = pick_ref[...]
    packed = pick.shape[0]
    rows = own_ref.shape[1]
    whole, chosen = [], []
    for step in range(near):
        total = own_ref[step] + cross_ref[step].astype(F32)
        if step == 0:
            mine_ref[...] = total
        high, low = parts(total)
        upper = jnp.dot(pick, high, preferred_element_type=F32)
        whole.append(high)
        chosen.append(upper.astype(BF16))
        if step:
            kept_ref[step - 1] = upper + jnp.dot(pick, low, preferred_element_type=F32)
    for step, send in enumerate(sends, 1):
        send[pl.ds(0, rows), :] = whole[step]
        others = [other for other in range(near) if other != step]
        for place, other in enumerate(others):
            send[pl.ds(rows + place * packed, packed), :] = chosen[other]


def collect_kernel(near, *refs):
    pick_ref, mine_ref, kept_ref = refs[:3]
    tokens, received = refs[3 : 3 + near], refs[3 + near : 2 + 2 * near]
    after_ref, near_ref = refs[2 + 2 * near :]
    pick = pick_ref[...]
    packed = pick.shape[0]
    rows = mine_ref.shape[0]
    total = mine_ref[...]
    for part in received:
        total = total + part[pl.ds(0, rows), :].astype(F32)
    base = tokens[0][pl.ds(0, rows), :].astype(F32)
    after = (base + 0.5 * total).astype(BF16)
    after_ref[...] = after
    near_ref[0] = jnp.dot(pick, after, preferred_element_type=F32).astype(BF16)
    for step in range(1, near):
        total = kept_ref[step - 1]
        for sender, part in enumerate(received, 1):
            place = [other for other in range(near) if other != sender].index(sender ^ step)
            total = total + part[pl.ds(rows + place * packed, packed), :].astype(F32)
        base = jnp.dot(pick, tokens[step][pl.ds(0, rows), :], preferred_element_type=F32)
        near_ref[step] = (base + 0.5 * total).astype(BF16)


def hidden_sums(blocks, rows, count, gain, gate, up, down):
    near = count // 2
    width = blocks[0].shape[1]
    span, skip = core_span(down.shape[0])
    early, late = early_masks(count)
    parts_early = call(
        functools.partial(ffn_early_kernel, early, span, skip),
        [pltpu.VMEM((rows, span), F32)] * 2 + [pltpu.VMEM((rows, 128), F32)],
        [*(blocks[m] for m in early), gain, gate, up, down],
    )
    hidden, cross_part = call(
        functools.partial(ffn_late_kernel, late, count, span, skip),
        [pltpu.VMEM((rows, span), BF16), pltpu.VMEM((near, rows, width), BF16)],
        [*(blocks[m] for m in late), gain, gate, up, down, *parts_early],
    )
    cross_sum = swap(cross_part, 1, count)
    own_part = call(
        functools.partial(ffn_own_kernel, count, skip),
        pltpu.VMEM((near, rows, width), F32),
        [hidden, down],
    )
    return own_part, cross_sum


def first_half_step(tokens, rows, count, gain, gate, up, down):
    near = count // 2
    width = tokens.shape[1]
    blocks = gather_blocks(tokens, count)
    own_part, cross_sum = hidden_sums(blocks, rows, count, gain, gate, up, down)
    live_rows = count * LIVE_HALVES // 2
    packed = -(-live_rows // 16) * 16
    pick = call(
        functools.partial(live_kernel, count, rows), pltpu.VMEM((packed, rows), BF16), blocks
    )
    sent = rows + (near - 1) * packed
    mine, kept, *sends = call(
        functools.partial(spread_kernel, near),
        [pltpu.VMEM((rows, width), F32), pltpu.VMEM((near - 1, packed, width), F32)]
        + [pltpu.VMEM((sent, width), BF16)] * (near - 1),
        [pick, own_part, cross_sum],
    )
    received = far_swaps(sends, count)
    after, near_live = call(
        functools.partial(collect_kernel, near),
        [pltpu.VMEM((rows, width), BF16), pltpu.VMEM((near, packed, width), BF16)],
        [pick, mine, kept, *blocks[::2], *received],
    )
    return after, near_live, pick


def second_half_step(own, count, gain, gate, up, down):
    rows, width = own.shape
    near = count // 2
    gain = gain.reshape(1, count * width)
    blocks = gather_blocks(own, count)
    own_part, cross_sum = hidden_sums(blocks, rows, count, gain, gate, up, down)
    mine, *sends = call(
        pair_sum_kernel,
        [pltpu.VMEM((rows, width), F32)] + [pltpu.VMEM((rows, width), BF16)] * (near - 1),
        [own_part, cross_sum],
    )
    received = far_swaps(sends, count)
    return call(residual_kernel, jax.ShapeDtypeStruct((rows, width), BF16), [own, mine, *received])


def mixes_of(blocks, masks, gain_ref, weights, thin):
    index = my_index()
    wide = [None] * len(weights)
    narrow = [None] * len(thin)
    squares = None
    across = (((1,), (1,)), ((), ()))
    for mask, block in zip(masks, blocks):
        owner = index ^ mask
        width = block.shape[1]
        rows = pl.ds(pl.multiple_of(owner * width, width), width)
        lhs, folded = gained(block, owner, gain_ref)
        squares = plus(squares, folded)
        for place, weight in enumerate(weights):
            wide[place] = plus(wide[place], jnp.dot(lhs, weight[rows, :], preferred_element_type=F32))
        for place, weight in enumerate(thin):
            part = lax.dot_general(lhs, weight[:, rows], across, preferred_element_type=F32)
            narrow[place] = plus(narrow[place], part)
    return wide, narrow, squares


def project_early_kernel(masks, near_ref, gain_ref, *refs):
    weights, (result, pre, squares_out) = refs[:6], refs[6:]
    blocks = [near_ref.at[place] for place in range(len(masks))]
    wide, narrow, squares_out[...] = mixes_of(blocks, masks, gain_ref, weights[:4], weights[4:])
    for place, part in enumerate(wide):
        width = part.shape[1]
        result[:, place * width : (place + 1) * width] = part
    for place, part in enumerate(narrow):
        width = part.shape[1]
        pre[:, place * width : (place + 1) * width] = part


def project_late_kernel(masks, near_ref, gain_ref, *refs):
    weights, (result_in, pre_in, squares_in, pick_ref) = refs[:6], refs[6:10]
    *sends, pre_ref, result, pre_scratch = refs[10:]
    blocks = [near_ref.at[place] for place in range(len(masks))]
    wide, narrow, squares = mixes_of(blocks, masks, gain_ref, weights[:4], weights[4:])
    row_scale = scale_of_rows(squares + squares_in[...], weights[0].shape[0])
    pick = pick_ref[...]
    back = (((0,), (0,)), ((), ()))
    for place, part in enumerate(wide):
        width = part.shape[1]
        columns = slice(place * width, (place + 1) * width)
        rounded = ((part + result_in[:, columns]) * row_scale).astype(BF16)
        result[:, columns] = lax.dot_general(pick, rounded, back, preferred_element_type=F32)
    for place, part in enumerate(narrow):
        width = part.shape[1]
        columns = slice(place * width, (place + 1) * width)
        high, low = parts((part + pre_in[:, columns]) * row_scale)
        total = lax.dot_general(pick, high, back, preferred_element_type=F32)
        pre_scratch[:, columns] = total + lax.dot_general(
            pick, low, back, preferred_element_type=F32
        )
    for step, send in enumerate(sends):
        rows = send.shape[0]
        row = pl.multiple_of((lax.axis_index("kv") ^ step) * rows, rows)
        send[...] = result[pl.ds(row, rows), :].astype(BF16)
    row = pl.multiple_of(my_index() * BLK, BLK)
    pre_ref[...] = pre_scratch[pl.ds(row, BLK), :]


def parts(value):
    high = value.astype(BF16)
    return high, (value - high.astype(F32)).astype(BF16)


def dot_parts(left, right, dims=(((1,), (0,)), ((), ()))):
    left_high, left_low = left
    right_high, right_low = right
    total = lax.dot_general(left_high, right_low, dims, preferred_element_type=F32)
    total = total + lax.dot_general(left_low, right_high, dims, preferred_element_type=F32)
    return total + lax.dot_general(left_high, right_high, dims, preferred_element_type=F32)


def split_state_kernel(state_ref, length_ref, high_ref, low_ref, live_ref):
    high_ref[...], low_ref[...] = parts(state_ref[...])
    step_of = lax.broadcasted_iota(jnp.int32, live_ref.shape, 0)
    live_ref[...] = (step_of < length_ref[...]).astype(F32)


def delta_kernel(masks, count, *refs):
    blocks = refs[: len(masks)]
    pre_ref, rate_ref, live_ref, high_ref, low_ref = refs[len(masks) : len(masks) + 5]
    mixed_ref, update_ref, faded_ref, final_ref = refs[len(masks) + 5 :]
    index = my_index()
    first_core = lax.axis_index("tp") == 0
    size = high_ref.shape[-1]
    all_heads = rate_ref.shape[1]
    per_block = all_heads // count
    heads = per_block * len(masks)
    rows = heads * BLK
    width = per_block * size
    taken = []
    for block in blocks:
        both = block[...].astype(F32)
        taken.append(jnp.where(first_core, both[:BLK], both[BLK:]))

    def stack(place):
        found = []
        for block in taken:
            for head in range(per_block):
                column = place * width + head * size
                found.append(block[:, column : column + size])
        return jnp.stack(found)

    def head_at(head):
        return (index ^ masks[head // per_block]) * per_block + head % per_block

    def lane_sum(array):
        return jnp.sum(array, axis=-1, keepdims=True)

    query, key_in, value, gating = (stack(place) for place in range(4))
    query_unit = query * lax.rsqrt(lane_sum(query * query) + EPSILON) * (1.0 / math.sqrt(size))
    key_unit = key_in * lax.rsqrt(lane_sum(key_in * key_in) + EPSILON)
    step_of = lax.broadcasted_iota(jnp.int32, (BLK, all_heads), 0)
    head_of = lax.broadcasted_iota(jnp.int32, (BLK, all_heads), 1)
    live = live_ref[...]
    pre = pre_ref[...]
    write_gate = jax.nn.sigmoid(pre[:, :all_heads]) * live
    forget_in = pre[:, all_heads:]
    softplus = jnp.maximum(forget_in, 0.0) + jnp.log1p(jnp.exp(-jnp.abs(forget_in)))
    cumulative = -jnp.exp(rate_ref[...]) * softplus * live
    lower = 1
    while lower < BLK:
        moved = pltpu.roll(cumulative, lower, 0)
        cumulative = cumulative + jnp.where(step_of >= lower, moved, 0.0)
        lower *= 2

    def columns_of(array):
        found = [lane_sum(jnp.where(head_of == head_at(head), array, 0.0)) for head in range(heads)]
        return jnp.broadcast_to(jnp.stack(found), (heads, BLK, size))

    write_col, cum = columns_of(write_gate), columns_of(cumulative)
    live_col = live[:, :1][None]
    growth = jnp.exp(cum)
    key_grown, query_grown = key_unit * growth, query_unit * growth
    from_key, from_query = [], []
    for head in range(heads):
        both = jnp.concatenate([key_grown[head], query_grown[head]], axis=0)
        found = dot_parts(parts(both), (high_ref[head_at(head)], low_ref[head_at(head)]))
        from_key.append(found[:BLK])
        from_query.append(found[BLK:])
    update = write_col * (value - jnp.stack(from_key))
    attend = jnp.stack(from_query)
    row_at = lax.broadcasted_iota(jnp.int32, (heads, BLK, size), 1)
    for step in range(BLK):

        def row_of(array):
            return jnp.broadcast_to(array[:, step : step + 1, :], array.shape)

        key_row = row_of(key_unit)
        decay = jnp.exp(jnp.minimum(cum - row_of(cum), 0.0))
        score = jnp.where(row_at >= step, decay * lane_sum(query_unit * key_row), 0.0)
        update_row = row_of(update)
        attend = attend + score * update_row
        if step < BLK - 1:
            strict = jnp.where(row_at > step, write_col * decay * lane_sum(key_unit * key_row), 0.0)
            update = update - strict * update_row
    normed = attend * lax.rsqrt(lane_sum(attend * attend) / size + EPSILON)
    normed = (normed * (gating * jax.nn.sigmoid(gating)) * live_col).astype(BF16)
    final = jnp.broadcast_to(cum[:, BLK - 1 :, :], cum.shape)
    for head in range(heads):
        mixed_ref[:, head * size : (head + 1) * size] = normed[head]
    update_ref[...] = update.reshape(rows, size)
    faded_ref[...] = (key_unit * jnp.exp(final - cum)).reshape(rows, size)
    final_ref[...] = jnp.exp(final).reshape(rows, size)


def join_kernel(count, first_ref, second_ref, mixed_ref):
    width = mixed_ref.shape[1] // count
    index = my_index()
    for mask in range(count):
        source = second_ref if mask % 2 else first_ref
        place = mask // 2
        column = pl.multiple_of((index ^ mask) * width, width)
        mixed_ref[:, pl.ds(column, width)] = source[:, place * width : (place + 1) * width]


def state_kernel(groups, count, *refs):
    state_ref, new_ref = refs[3 * len(groups) :]
    per_block = state_ref.shape[0] // count
    index = my_index()
    along = (((0,), (0,)), ((), ()))
    for place, masks in enumerate(groups):
        update_ref, faded_ref, final_ref = refs[3 * place : 3 * place + 3]
        for head in range(per_block * len(masks)):
            at = slice(head * BLK, (head + 1) * BLK)
            left_high, left_low = parts(faded_ref[at])
            right_high, right_low = parts(update_ref[at])
            left = jnp.concatenate([left_high, left_high, left_low, left_low], axis=0)
            right = jnp.concatenate([right_high, right_low, right_high, right_low], axis=0)
            grown = lax.dot_general(left, right, along, preferred_element_type=F32)
            scale = final_ref[head * BLK : head * BLK + 1, :]
            owner = (index ^ masks[head // per_block]) * per_block + head % per_block
            new_ref[pl.ds(owner, 1)] = (scale * state_ref[owner] + grown)[None]


def out_kernel(count, *refs):
    blocks = refs[:count]
    weight_ref, base_ref, out_ref, scratch = refs[count:]
    index = my_index()
    lhs = jnp.concatenate([block[...].astype(F32) for block in blocks], axis=0).astype(BF16)
    half = lhs.shape[1] // 2
    first = jnp.dot(lhs[:, :half], weight_ref[:half, :], preferred_element_type=F32).astype(BF16)
    second = jnp.dot(lhs[:, half:], weight_ref[half:, :], preferred_element_type=F32).astype(BF16)
    total = first.astype(F32) + second.astype(F32)
    for mask in range(count):
        row = pl.multiple_of((index ^ mask) * BLK, BLK)
        scratch[pl.ds(row, BLK), :] = total[mask * BLK : (mask + 1) * BLK]
    out_ref[...] = (base_ref[...].astype(F32) + scratch[...]).astype(BF16)


def group_device(
    tokens,
    lengths,
    state,
    gain_first,
    first_gate,
    first_up,
    first_down,
    gain_mix,
    query_weight,
    key_weight,
    value_weight,
    gating_weight,
    write_weight,
    forget_weight,
    forget_rate,
    out_weight,
    gain_second,
    second_gate,
    second_up,
    second_down,
):
    count = lax.axis_size("kv") * lax.axis_size("tp")
    rows, width = tokens.shape
    channels = gain_first.shape[0]
    heads, size = state.shape[1], state.shape[2]
    entered, gain_ready = enter(
        tokens, gain_first.reshape(1, channels), lengths, first_gate, first_up, first_down
    )
    after_first, near_live, pick = first_half_step(
        entered, rows, count, gain_ready, first_gate, first_up, first_down
    )
    cross_live = swap(near_live, 1, count)
    packed = pick.shape[0]
    columns = 4 * width
    near = count // 2
    near_masks, cross_masks = list(range(0, count, 2)), list(range(1, count, 2))
    mixers = [
        gain_mix.reshape(1, channels),
        query_weight,
        key_weight,
        value_weight,
        gating_weight,
        write_weight.T,
        forget_weight.T,
    ]
    parts_early = call(
        functools.partial(project_early_kernel, near_masks),
        [
            pltpu.VMEM((packed, columns), F32),
            pltpu.VMEM((packed, 2 * heads), F32),
            pltpu.VMEM((packed, 128), F32),
        ],
        [near_live, *mixers],
    )
    *sends, pre = call(
        functools.partial(project_late_kernel, cross_masks),
        [pltpu.VMEM((rows // near, columns), BF16)] * near + [pltpu.VMEM((BLK, 2 * heads), F32)],
        [cross_live, *mixers, *parts_early, pick],
        scratch=[pltpu.VMEM((rows, columns), F32), pltpu.VMEM((rows, 2 * heads), F32)],
    )
    owned = pair_up([sends[0]] + far_swaps(sends[1:], count), count)
    matrices = state.reshape(heads, size, size)
    high, low, live = call(
        split_state_kernel,
        [pltpu.VMEM(matrices.shape, BF16)] * 2 + [pltpu.VMEM((BLK, heads), F32)],
        [matrices, lengths.reshape(1, 1)],
        limit=3 << 20,
    )
    groups = [list(range(0, count, 2)), list(range(1, count, 2))]
    mixed_parts, grown = [], []
    for masks in groups:
        tall = heads * BLK // 2
        part, *rest = call(
            functools.partial(delta_kernel, masks, count),
            [pltpu.VMEM((BLK, channels // 2), BF16)] + [pltpu.VMEM((tall, size), F32)] * 3,
            [
                *(owned[m] for m in masks),
                pre,
                forget_rate.reshape(1, heads),
                live,
                high,
                low,
            ],
        )
        mixed_parts.append(part)
        grown += rest
    mixed = call(
        functools.partial(join_kernel, count), pltpu.VMEM((BLK, channels), BF16), mixed_parts
    )
    head_blocks = gather_blocks(mixed, count)
    new_state = call(
        functools.partial(state_kernel, groups, count),
        jax.ShapeDtypeStruct((heads, size, size), F32),
        [*grown, matrices],
    )
    after_mix = call(
        functools.partial(out_kernel, count),
        pltpu.VMEM((rows, width), BF16),
        [*head_blocks, out_weight, after_first],
        scratch=[pltpu.VMEM((rows, width), F32)],
    )
    mixed_out = second_half_step(
        after_mix, count, gain_second, second_gate, second_up, second_down
    )
    return (mixed_out, new_state.reshape(state.shape))


def fits_group(mesh):
    near, cores = mesh.shape["kv"], mesh.shape["tp"]
    count = near * cores
    return cores == 2 and near & (near - 1) == 0 and near <= 8 and (HEADS * HEAD) % (count * 128) == 0


def per_device(mesh, *arrays):
    lengths, gate = arrays[1], arrays[4]
    suits = fits_group(mesh) and lengths.shape[0] == 1 and gate.shape[1] % 128 == 0
    if not suits:
        return general_device(*arrays)
    return group_device(*arrays)


def solution(mesh):
    in_specs = (
        P("dp", ("kv", "tp")),
        P(("dp", "kv", "tp")),
        P(("dp", "kv", "tp"), None, None, None),
        P(),
        P(None, "kv"),
        P(None, "kv"),
        P("kv", None),
        P(),
        P(None, ("kv", "tp")),
        P(None, ("kv", "tp")),
        P(None, ("kv", "tp")),
        P(None, ("kv", "tp")),
        P(),
        P(),
        P(),
        P(None, ("kv", "tp")),
        P(),
        P(None, "kv"),
        P(None, "kv"),
        P("kv", None),
    )
    out_specs = (P("dp", ("kv", "tp")), P(("dp", "kv", "tp"), None, None, None))
    return jax.shard_map(
        functools.partial(per_device, mesh),
        mesh=mesh,
        in_specs=in_specs,
        out_specs=out_specs,
        check_vma=False,
    )
```

```python
import functools
import math

import jax
import jax.numpy as jnp
from jax import lax
from jax.experimental import pallas as pl
from jax.experimental.pallas import tpu as pltpu
from jax.sharding import PartitionSpec as P


HEADS = 16
HEAD = 128
BLK = 8


EPSILON = 1e-06


def fold_step(gain, gate_cols, up_cols, portion):
    values = portion.astype(jnp.float32)
    scaled = (values * gain).astype(jnp.bfloat16)
    gate_acc = jnp.dot(scaled, gate_cols, preferred_element_type=jnp.float32)
    up_acc = jnp.dot(scaled, up_cols, preferred_element_type=jnp.float32)
    squares = jnp.sum(values * values, axis=1)
    return (gate_acc, up_acc, squares)


def finish_units(gate_acc, up_acc, squares, channels, down_rows):
    row_scale = lax.rsqrt(squares / channels + EPSILON)[:, None]
    hidden = (jax.nn.silu(gate_acc * row_scale) * (up_acc * row_scale)).astype(jnp.bfloat16)
    return jnp.dot(hidden, down_rows, preferred_element_type=jnp.float32)


def feed_forward(hidden_in, gain, w_gate, w_up, w_down):
    channels = gain.shape[0]
    paired = lax.all_to_all(hidden_in, "tp", split_axis=0, concat_axis=1, tiled=True)
    gate_acc, up_acc, squares = fold_step(
        gain, w_gate, w_up, lax.all_gather(paired, "kv", axis=1, tiled=True)
    )
    ffn_term = finish_units(gate_acc, up_acc, squares, channels, w_down)
    partial_value = lax.psum_scatter(ffn_term, "kv", scatter_dimension=1, tiled=True)
    summed = lax.all_to_all(partial_value, "tp", split_axis=1, concat_axis=0, tiled=True)
    return (hidden_in.astype(jnp.float32) + 0.5 * summed).astype(jnp.bfloat16)


def delta_block(query, key_in, value, gating, write_pre, forget_pre, rates, live, state):
    seq_count, block_len, head_count, head_size = query.shape
    precise = lax.Precision.HIGHEST
    query_unit = (
        query
        * lax.rsqrt(jnp.sum(query * query, axis=-1, keepdims=True) + EPSILON)
        / math.sqrt(head_size)
    )
    key_unit = key_in * lax.rsqrt(jnp.sum(key_in * key_in, axis=-1, keepdims=True) + EPSILON)
    live_rows = live[:, :, None]
    write_gate = jax.nn.sigmoid(write_pre) * live_rows
    forget = -jnp.exp(rates)[None, None, :] * jax.nn.softplus(forget_pre) * live_rows
    cumulative = jnp.cumsum(forget, axis=1)
    cum_heads = jnp.transpose(cumulative, (0, 2, 1))
    positions = jnp.arange(block_len)
    causal = positions[:, None] >= positions[None, :]
    strict = positions[:, None] > positions[None, :]
    differ = jnp.minimum(cum_heads[:, :, :, None] - cum_heads[:, :, None, :], 0.0)
    decay_mat = jnp.where(causal, jnp.exp(differ), 0.0)
    key_dots = jnp.einsum("sthd,suhd->shtu", key_unit, key_unit, precision=precise)
    write_heads = jnp.transpose(write_gate, (0, 2, 1))
    strict_part = jnp.where(strict, write_heads[:, :, :, None] * decay_mat * key_dots, 0.0)
    identity = jnp.eye(block_len, dtype=jnp.float32)
    squared = jnp.einsum("shtu,shuv->shtv", strict_part, strict_part, precision=precise)
    fourth = jnp.einsum("shtu,shuv->shtv", squared, squared, precision=precise)
    inverse = jnp.einsum(
        "shtu,shuv->shtv", identity - strict_part, identity + squared, precision=precise
    )
    inverse = jnp.einsum("shtu,shuv->shtv", inverse, identity + fourth, precision=precise)
    growth = jnp.exp(cumulative)
    target = jnp.einsum(
        "shtu,suhv->sthv", inverse, write_gate[..., None] * value, precision=precise
    )
    key_mix = jnp.einsum(
        "shtu,suhk->sthk", inverse, (write_gate * growth)[..., None] * key_unit, precision=precise
    )
    update = target - jnp.einsum("sthk,shkv->sthv", key_mix, state, precision=precise)
    scores = jnp.einsum("sthd,suhd->shtu", query_unit, key_unit, precision=precise) * decay_mat
    attend = jnp.einsum("sthk,shkv->sthv", query_unit * growth[..., None], state, precision=precise)
    attend = attend + jnp.einsum("shtu,suhv->sthv", scores, update, precision=precise)
    final_cum = cumulative[:, -1:, :]
    fading = jnp.exp(final_cum - cumulative)
    new_state = jnp.exp(final_cum[:, 0, :])[:, :, None, None] * state
    new_state = new_state + jnp.einsum(
        "sthk,sthv->shkv", key_unit * fading[..., None], update, precision=precise
    )
    normed = attend * lax.rsqrt(jnp.mean(attend * attend, axis=-1, keepdims=True) + EPSILON)
    normed = normed * jax.nn.silu(gating) * live[:, :, None, None]
    mixed_heads = normed.reshape(seq_count * block_len, head_count * head_size).astype(jnp.bfloat16)
    return (mixed_heads, new_state)


def general_device(
    tokens,
    lengths,
    state,
    gain_first,
    first_gate,
    first_up,
    first_down,
    gain_mix,
    query_weight,
    key_weight,
    value_weight,
    gating_weight,
    write_weight,
    forget_weight,
    forget_rate,
    out_weight,
    gain_second,
    second_gate,
    second_up,
    second_down,
):
    after_first = feed_forward(tokens, gain_first, first_gate, first_up, first_down)
    seq_count = lengths.shape[0]
    own_count = seq_count * BLK
    whole_rows = lax.all_gather(after_first, ("kv", "tp"), axis=1, tiled=True)
    scaled_all = (whole_rows.astype(jnp.float32) * gain_mix).astype(jnp.bfloat16)
    stacked = jnp.stack(
        [
            jnp.dot(scaled_all, matrix, preferred_element_type=jnp.float32)
            for matrix in (query_weight, key_weight, value_weight, gating_weight)
        ]
    )
    owned = lax.all_to_all(
        stacked.astype(jnp.bfloat16), ("kv", "tp"), split_axis=1, concat_axis=2, tiled=True
    ).astype(stacked.dtype)
    row_start = lax.axis_index(("kv", "tp")) * own_count
    own_values = lax.dynamic_slice_in_dim(whole_rows, row_start, own_count, 0).astype(jnp.float32)
    own_scaled = lax.dynamic_slice_in_dim(scaled_all, row_start, own_count, 0)
    mix_scale = lax.rsqrt(jnp.mean(own_values * own_values, axis=1, keepdims=True) + EPSILON)
    query = (owned[0] * mix_scale).reshape(seq_count, BLK, HEADS, HEAD)
    key_in = (owned[1] * mix_scale).reshape(seq_count, BLK, HEADS, HEAD)
    value = (owned[2] * mix_scale).reshape(seq_count, BLK, HEADS, HEAD)
    gating = (owned[3] * mix_scale).reshape(seq_count, BLK, HEADS, HEAD)
    write_pre = (
        jnp.dot(own_scaled, write_weight, preferred_element_type=jnp.float32) * mix_scale
    ).reshape(seq_count, BLK, HEADS)
    forget_pre = (
        jnp.dot(own_scaled, forget_weight, preferred_element_type=jnp.float32) * mix_scale
    ).reshape(seq_count, BLK, HEADS)
    positions = jnp.arange(BLK, dtype=jnp.int32)
    live = (positions[None, :] < lengths[:, None]).astype(jnp.float32)
    mixed_heads, new_state = delta_block(
        query, key_in, value, gating, write_pre, forget_pre, forget_rate, live, state
    )
    half_cols = mixed_heads.shape[1] // 2
    portion = lax.all_gather(mixed_heads, ("kv", "tp"), axis=0, tiled=True)
    first_half = jnp.dot(
        portion[:, :half_cols], out_weight[:half_cols], preferred_element_type=jnp.float32
    ).astype(jnp.bfloat16)
    second_half = jnp.dot(
        portion[:, half_cols:], out_weight[half_cols:], preferred_element_type=jnp.float32
    ).astype(jnp.bfloat16)
    first_half, second_half = lax.optimization_barrier((first_half, second_half))
    mixed_sum = first_half.astype(jnp.float32) + second_half.astype(jnp.float32)
    after_mix = (after_first.astype(jnp.float32) + mixed_sum).astype(jnp.bfloat16)
    mixed_out = feed_forward(after_mix, gain_second, second_gate, second_up, second_down)
    return (mixed_out, new_state)


VMEM_SPEC = pl.BlockSpec(memory_space=pltpu.VMEM)
HBM_SPEC = pl.BlockSpec(memory_space=pltpu.HBM)
GROUP = ("kv", "tp")
CROSSED = ("ex_e",)
LIVE_HALVES = 7
F32, BF16 = jnp.float32, jnp.bfloat16


def call(body, out_shapes, args, in_specs=None, scratch=(), limit=5 << 20, out_specs=None):
    single = not isinstance(out_shapes, (list, tuple))
    shapes = [out_shapes] if single else list(out_shapes)
    outs = pl.pallas_call(
        body,
        out_shape=shapes,
        in_specs=in_specs or [VMEM_SPEC] * len(args),
        out_specs=out_specs or [VMEM_SPEC] * len(shapes),
        scratch_shapes=list(scratch),
        compiler_params=pltpu.CompilerParams(vmem_limit_bytes=limit),
    )(*args)
    return outs[0] if single else outs


def my_index():
    return lax.axis_index("kv") * lax.axis_size("tp") + lax.axis_index("tp")


def swap(value, mask, count):
    return lax.ppermute(value, GROUP, [(i, i ^ mask) for i in range(count)])


def far_swaps(sends, count):
    received = []
    for step, send in enumerate(sends):
        received.append(swap(send, 2 * (step + 1), count))
    return received


def pair_up(near, count, known=()):
    blocks = []
    for step, block in enumerate(near):
        if step in known:
            blocks += [block, known[step]]
            continue
        blocks += [block, swap(block, 1, count)]
    return blocks


def exchange_blocks(sends, count, label):
    near = [sends[0]] + far_swaps(sends[1:], count)
    if label not in CROSSED:
        return pair_up(near, count)
    nearest = swap(sends[1], 3, count)
    return pair_up(near, count, {1: nearest})


def gather_blocks(own, count, label):
    return exchange_blocks([own] * (count // 2), count, label)


def entry_kernel(length_ref, tokens_hbm, gain_hbm, gate_hbm, up_hbm, down_hbm, *refs):
    tokens_ref, gain_ref, sem = refs
    rows = tokens_hbm.shape[0]
    copies = [
        pltpu.make_async_copy(tokens_hbm, tokens_ref.at[pl.ds(0, rows)], sem.at[0]),
        pltpu.make_async_copy(gain_hbm, gain_ref, sem.at[1]),
    ]
    for copy in copies:
        copy.start()
    tail = (BLK, tokens_ref.shape[1])
    tokens_ref[pl.ds(rows, BLK), :] = jnp.full(tail, length_ref[0].astype(F32)).astype(BF16)
    for copy in copies:
        copy.wait()


def enter(tokens, gain, lengths, *weights):
    arrays = [tokens, gain, *weights]
    arrays = [pltpu.with_memory_space_constraint(a, pltpu.HBM) for a in arrays]
    rows, width = tokens.shape
    return call(
        entry_kernel,
        [pltpu.VMEM((rows + BLK, width), BF16), pltpu.VMEM(gain.shape, F32)],
        [lengths, *arrays],
        in_specs=[pl.BlockSpec(memory_space=pltpu.SMEM)] + [HBM_SPEC] * len(arrays),
        scratch=[pltpu.SemaphoreType.DMA((2,))],
        limit=1 << 20,
    )


def core_span(units):
    tiles = units // 128
    span = -(-tiles // 2) * 128
    return span, units - span


def gained(block, owner, gain_ref):
    width = block.shape[1]
    column = pl.multiple_of(owner * width, width)
    values = block[...].astype(F32)
    squares = values * values
    folded = squares[:, :128]
    for first in range(128, width, 128):
        folded = folded + squares[:, first : first + 128]
    return (values * gain_ref[:, pl.ds(column, width)]).astype(BF16), folded


def scale_of_rows(folded, channels):
    return lax.rsqrt(jnp.sum(folded, axis=1, keepdims=True) / channels + EPSILON)


def plus(total, part):
    return part if total is None else total + part


def mask_groups(count):
    return [], [m for m in range(count) if m not in (3, 5)], [3, 5]


def units_of(blocks, masks, gain_ref, gate_ref, up_ref, span, skip, row_count):
    index = my_index()
    blocks = [block.at[pl.ds(0, row_count)] for block in blocks]
    start = pl.multiple_of(lax.axis_index("tp") * skip, 128)
    gate_acc = up_acc = squares = None
    for mask, block in zip(masks, blocks):
        owner = index ^ mask
        width = block.shape[1]
        rows = pl.ds(pl.multiple_of(owner * width, width), width)
        lhs, folded = gained(block, owner, gain_ref)
        squares = plus(squares, folded)
        columns = pl.ds(start, span)
        gate_acc = plus(gate_acc, jnp.dot(lhs, gate_ref[rows, columns], preferred_element_type=F32))
        up_acc = plus(up_acc, jnp.dot(lhs, up_ref[rows, columns], preferred_element_type=F32))
    return gate_acc, up_acc, squares


def ffn_early_kernel(masks, span, skip, *refs):
    blocks = refs[: len(masks)]
    gain_ref, gate_ref, up_ref, _, *carried = refs[len(masks) :]
    outs, before = carried[-3:], carried[:-3]
    found = units_of(
        blocks, masks, gain_ref, gate_ref, up_ref, span, skip, outs[0].shape[0]
    )
    for place, (out, part) in enumerate(zip(outs, found)):
        out[...] = part + before[place][...] if before else part


def ffn_late_kernel(masks, count, span, skip, *refs):
    blocks = refs[: len(masks)]
    gain_ref, gate_ref, up_ref, down_ref, gate_in, up_in, squares_in = refs[len(masks) : len(masks) + 7]
    hidden_ref, cross_ref = refs[len(masks) + 7 :]
    gate_acc, up_acc, squares = units_of(
        blocks, masks, gain_ref, gate_ref, up_ref, span, skip, gate_in.shape[0]
    )
    channels = gate_ref.shape[0]
    row_scale = scale_of_rows(squares + squares_in[...], channels)
    gate_act = (gate_acc + gate_in[...]) * row_scale
    hidden = gate_act * jax.nn.sigmoid(gate_act) * ((up_acc + up_in[...]) * row_scale)
    repeated = lax.axis_index("tp") * (lax.axis_size("tp") * span - down_ref.shape[0])
    unit = lax.broadcasted_iota(jnp.int32, hidden.shape, 1)
    hidden_ref[...] = jnp.where(unit >= repeated, hidden, 0.0).astype(BF16)
    hidden = hidden_ref[...]
    down_products(hidden, down_ref, range(1, count, 2), cross_ref, skip)


def down_products(hidden, down_ref, masks, out_ref, skip):
    index = my_index()
    start = pl.multiple_of(lax.axis_index("tp") * skip, 128)
    span, width = hidden.shape[1], out_ref.shape[2]
    for place, mask in enumerate(masks):
        column = pl.multiple_of((index ^ mask) * width, width)
        weight = down_ref[pl.ds(start, span), pl.ds(column, width)]
        out_ref[place] = jnp.dot(hidden, weight, preferred_element_type=F32).astype(out_ref.dtype)


def ffn_own_kernel(count, skip, hidden_ref, down_ref, own_ref):
    down_products(hidden_ref[...], down_ref, range(0, count, 2), own_ref, skip)


def pair_sum_kernel(own_ref, cross_ref, mine_ref, *sends):
    mine_ref[...] = own_ref[0] + cross_ref[0].astype(F32)
    for step, send in enumerate(sends):
        send[...] = (own_ref[step + 1] + cross_ref[step + 1].astype(F32)).astype(BF16)


def residual_kernel(base_ref, mine_ref, *refs):
    total = mine_ref[...]
    for received in refs[:-1]:
        total = total + received[...].astype(F32)
    refs[-1][...] = (base_ref[...].astype(F32) + 0.5 * total).astype(BF16)


def live_kernel(count, rows, *refs):
    blocks, pick_ref = refs[:count], refs[count]
    index = my_index()
    lane = lax.broadcasted_iota(jnp.int32, (BLK, rows), 1)
    lengths = jnp.zeros((BLK, rows), F32)
    for mask, block in enumerate(blocks):
        length = block[pl.ds(rows, BLK), :rows].astype(F32)
        lengths = jnp.where(lane // BLK == (index ^ mask), length, lengths)
    live = (lane % BLK).astype(F32) < lengths
    before = lax.broadcasted_iota(jnp.int32, (rows, rows), 0) < lax.broadcasted_iota(
        jnp.int32, (rows, rows), 1
    )
    rank = jnp.dot(live.astype(BF16), before.astype(BF16), preferred_element_type=F32)
    rank = jnp.where(live, rank, -1.0)[:1]
    wanted = lax.broadcasted_iota(jnp.int32, pick_ref.shape, 0).astype(F32)
    pick_ref[...] = (rank == wanted).astype(F32).astype(BF16)


def spread_kernel(near, live_rows, pick_ref, own_ref, cross_ref, mine_ref, kept_ref, *sends):
    *sends, packed_ref = sends
    pick = pick_ref[...]
    packed = pick.shape[0]
    rows = own_ref.shape[1]
    whole, chosen = [], []
    for step in range(near):
        total = own_ref[step] + cross_ref[step].astype(F32)
        if step == 0:
            mine_ref[...] = total
        high, low = parts(total)
        upper = jnp.dot(pick, high, preferred_element_type=F32)
        whole.append(high)
        chosen.append(upper)
        if step:
            kept_ref[step - 1] = upper + jnp.dot(pick, low, preferred_element_type=F32)
    for step, send in enumerate(sends, 1):
        send[pl.ds(0, rows), :] = whole[step]
        others = [other for other in range(near) if other != step]
        for place, other in enumerate(others):
            packed_ref[pl.ds(place * live_rows, packed), :] = chosen[other]
        send[pl.ds(rows, packed_ref.shape[0]), :] = packed_ref[...].astype(BF16)


def collect_kernel(near, live_rows, *refs):
    pick_ref, mine_ref, kept_ref = refs[:3]
    tokens, received = refs[3 : 3 + near], refs[3 + near : 2 + 2 * near]
    after_ref, near_ref = refs[2 + 2 * near :]
    pick = pick_ref[...]
    packed = pick.shape[0]
    rows = mine_ref.shape[0]
    total = mine_ref[...]
    for part in received:
        total = total + part[pl.ds(0, rows), :].astype(F32)
    base = tokens[0][pl.ds(0, rows), :].astype(F32)
    after = (base + 0.5 * total).astype(BF16)
    after_ref[...] = after
    near_ref[0] = jnp.dot(pick, after, preferred_element_type=F32).astype(BF16)
    tails = [part[pl.ds(rows, part.shape[0] - rows), :].astype(F32) for part in received]
    for step in range(1, near):
        total = kept_ref[step - 1]
        for sender, tail in enumerate(tails, 1):
            place = [other for other in range(near) if other != sender].index(sender ^ step)
            total = total + tail[place * live_rows : place * live_rows + packed]
        base = jnp.dot(pick, tokens[step][pl.ds(0, rows), :], preferred_element_type=F32)
        near_ref[step] = (base + 0.5 * total).astype(BF16)


def hidden_sums(blocks, rows, count, gain, gate, up, down):
    near = count // 2
    width = blocks[0].shape[1]
    span, skip = core_span(down.shape[0])
    _, early, late = mask_groups(count)
    parts_early = []
    for masks in (early,):
        parts_early = call(
            functools.partial(ffn_early_kernel, masks, span, skip),
            [pltpu.VMEM((rows, span), F32)] * 2 + [pltpu.VMEM((rows, 128), F32)],
            [*(blocks[m] for m in masks), gain, gate, up, down, *parts_early],
        )
    hidden, cross_part = call(
        functools.partial(ffn_late_kernel, late, count, span, skip),
        [pltpu.VMEM((rows, span), BF16), pltpu.VMEM((near, rows, width), BF16)],
        [*(blocks[m] for m in late), gain, gate, up, down, *parts_early],
    )
    cross_sum = swap(cross_part, 1, count)
    own_part = call(
        functools.partial(ffn_own_kernel, count, skip),
        pltpu.VMEM((near, rows, width), F32),
        [hidden, down],
    )
    return own_part, cross_sum


def first_half_step(tokens, rows, count, gain, gate, up, down):
    near = count // 2
    width = tokens.shape[1]
    blocks = gather_blocks(tokens, count, "ex_a")
    own_part, cross_sum = hidden_sums(blocks, rows, count, gain, gate, up, down)
    live_rows = count * LIVE_HALVES // 2
    packed = -(-live_rows // 16) * 16
    pick = call(
        functools.partial(live_kernel, count, rows),
        pltpu.VMEM((packed, rows), BF16),
        blocks,
    )
    tail = -(-((near - 2) * live_rows + packed) // BLK) * BLK
    sent = rows + tail
    mine, kept, *sends = call(
        functools.partial(spread_kernel, near, live_rows),
        [pltpu.VMEM((rows, width), F32), pltpu.VMEM((near - 1, packed, width), F32)]
        + [pltpu.VMEM((sent, width), BF16)] * (near - 1),
        [pick, own_part, cross_sum],
        scratch=[pltpu.VMEM((tail, width), F32)],
    )
    received = far_swaps(sends, count)
    after, near_live = call(
        functools.partial(collect_kernel, near, live_rows),
        [pltpu.VMEM((rows, width), BF16), pltpu.VMEM((near, packed, width), BF16)],
        [pick, mine, kept, *blocks[::2], *received],
    )
    return after, near_live, pick


def second_half_step(own, count, gain, gate, up, down):
    rows, width = own.shape
    near = count // 2
    gain = gain.reshape(1, count * width)
    blocks = gather_blocks(own, count, "ex_f")
    own_part, cross_sum = hidden_sums(blocks, rows, count, gain, gate, up, down)
    mine, *sends = call(
        pair_sum_kernel,
        [pltpu.VMEM((rows, width), F32)] + [pltpu.VMEM((rows, width), BF16)] * (near - 1),
        [own_part, cross_sum],
    )
    received = far_swaps(sends, count)
    return call(
        residual_kernel,
        jax.ShapeDtypeStruct((rows, width), BF16),
        [own, mine, *received],
    )


def mixes_of(blocks, masks, gain_ref, weights, thin):
    index = my_index()
    wide = [None] * len(weights)
    narrow = [None] * len(thin)
    squares = None
    across = (((1,), (1,)), ((), ()))
    for mask, block in zip(masks, blocks):
        owner = index ^ mask
        width = block.shape[1]
        rows = pl.ds(pl.multiple_of(owner * width, width), width)
        lhs, folded = gained(block, owner, gain_ref)
        squares = plus(squares, folded)
        for place, weight in enumerate(weights):
            wide[place] = plus(wide[place], jnp.dot(lhs, weight[rows, :], preferred_element_type=F32))
        for place, weight in enumerate(thin):
            part = lax.dot_general(lhs, weight[:, rows], across, preferred_element_type=F32)
            narrow[place] = plus(narrow[place], part)
    return wide, narrow, squares


def project_early_kernel(masks, near_ref, gain_ref, *refs):
    weights, (result, pre, squares_out) = refs[:6], refs[6:]
    blocks = [near_ref.at[place] for place in range(len(masks))]
    wide, narrow, squares_out[...] = mixes_of(blocks, masks, gain_ref, weights[:4], weights[4:])
    for place, part in enumerate(wide):
        width = part.shape[1]
        result[:, place * width : (place + 1) * width] = part
    for place, part in enumerate(narrow):
        width = part.shape[1]
        pre[:, place * width : (place + 1) * width] = part


def project_late_kernel(masks, near_ref, gain_ref, *refs):
    weights, (result_in, pre_in, squares_in, pick_ref) = refs[:6], refs[6:10]
    *sends, pre_ref, result, pre_scratch = refs[10:]
    blocks = [near_ref.at[place] for place in range(len(masks))]
    wide, narrow, squares = mixes_of(blocks, masks, gain_ref, weights[:4], weights[4:])
    row_scale = scale_of_rows(squares + squares_in[...], weights[0].shape[0])
    pick = pick_ref[...]
    back = (((0,), (0,)), ((), ()))
    for place, part in enumerate(wide):
        width = part.shape[1]
        columns = slice(place * width, (place + 1) * width)
        rounded = ((part + result_in[:, columns]) * row_scale).astype(BF16)
        result[:, columns] = lax.dot_general(pick, rounded, back, preferred_element_type=F32)
    for place, part in enumerate(narrow):
        width = part.shape[1]
        columns = slice(place * width, (place + 1) * width)
        high, low = parts((part + pre_in[:, columns]) * row_scale)
        total = lax.dot_general(pick, high, back, preferred_element_type=F32)
        pre_scratch[:, columns] = total + lax.dot_general(
            pick, low, back, preferred_element_type=F32
        )
    for step, send in enumerate(sends):
        rows = send.shape[0]
        row = pl.multiple_of((lax.axis_index("kv") ^ step) * rows, rows)
        send[...] = result[pl.ds(row, rows), :].astype(BF16)
    row = pl.multiple_of(my_index() * BLK, BLK)
    pre_ref[...] = pre_scratch[pl.ds(row, BLK), :]


def parts(value):
    high = value.astype(BF16)
    return high, (value - high.astype(F32)).astype(BF16)


def dot_parts(left, right, dims=(((1,), (0,)), ((), ()))):
    left_high, left_low = left
    right_high, right_low = right
    total = lax.dot_general(left_high, right_low, dims, preferred_element_type=F32)
    total = total + lax.dot_general(left_low, right_high, dims, preferred_element_type=F32)
    return total + lax.dot_general(left_high, right_high, dims, preferred_element_type=F32)


def split_state_kernel(state_ref, length_ref, high_ref, low_ref, live_ref):
    high_ref[...], low_ref[...] = parts(state_ref[...])
    step_of = lax.broadcasted_iota(jnp.int32, live_ref.shape, 0)
    live_ref[...] = (step_of < length_ref[...]).astype(F32)


def delta_kernel(masks, count, joined, *refs):
    blocks = refs[: len(masks)]
    pre_ref, rate_ref, live_ref, high_ref, low_ref = refs[len(masks) : len(masks) + 5]
    *before, mixed_ref, update_ref, faded_ref, final_ref = refs[len(masks) + 5 :]
    index = my_index()
    first_core = lax.axis_index("tp") == 0
    size = high_ref.shape[-1]
    all_heads = rate_ref.shape[1]
    per_block = all_heads // count
    heads = per_block * len(masks)
    rows = heads * BLK
    width = per_block * size
    taken = []
    for block in blocks:
        both = block[...].astype(F32)
        taken.append(jnp.where(first_core, both[:BLK], both[BLK:]))

    def stack(place):
        found = []
        for block in taken:
            for head in range(per_block):
                column = place * width + head * size
                found.append(block[:, column : column + size])
        return jnp.stack(found)

    def head_at(head):
        return (index ^ masks[head // per_block]) * per_block + head % per_block

    def lane_sum(array):
        return jnp.sum(array, axis=-1, keepdims=True)

    query, key_in, value, gating = (stack(place) for place in range(4))
    query_unit = query * lax.rsqrt(lane_sum(query * query) + EPSILON) * (1.0 / math.sqrt(size))
    key_unit = key_in * lax.rsqrt(lane_sum(key_in * key_in) + EPSILON)
    step_of = lax.broadcasted_iota(jnp.int32, (BLK, all_heads), 0)
    head_of = lax.broadcasted_iota(jnp.int32, (BLK, all_heads), 1)
    live = live_ref[...]
    pre = pre_ref[...]
    write_gate = jax.nn.sigmoid(pre[:, :all_heads]) * live
    forget_in = pre[:, all_heads:]
    softplus = jnp.maximum(forget_in, 0.0) + jnp.log1p(jnp.exp(-jnp.abs(forget_in)))
    cumulative = -jnp.exp(rate_ref[...]) * softplus * live
    lower = 1
    while lower < BLK:
        moved = pltpu.roll(cumulative, lower, 0)
        cumulative = cumulative + jnp.where(step_of >= lower, moved, 0.0)
        lower *= 2

    def columns_of(array):
        found = [lane_sum(jnp.where(head_of == head_at(head), array, 0.0)) for head in range(heads)]
        return jnp.broadcast_to(jnp.stack(found), (heads, BLK, size))

    write_col, cum = columns_of(write_gate), columns_of(cumulative)
    live_col = live[:, :1][None]
    growth = jnp.exp(cum)
    key_grown, query_grown = key_unit * growth, query_unit * growth
    from_key, from_query = [], []
    for head in range(heads):
        both = jnp.concatenate([key_grown[head], query_grown[head]], axis=0)
        found = dot_parts(parts(both), (high_ref[head_at(head)], low_ref[head_at(head)]))
        from_key.append(found[:BLK])
        from_query.append(found[BLK:])
    update = write_col * (value - jnp.stack(from_key))
    attend = jnp.stack(from_query)
    row_at = lax.broadcasted_iota(jnp.int32, (heads, BLK, size), 1)
    for step in range(BLK):

        def row_of(array):
            return jnp.broadcast_to(array[:, step : step + 1, :], array.shape)

        key_row = row_of(key_unit)
        decay = jnp.exp(jnp.minimum(cum - row_of(cum), 0.0))
        score = jnp.where(row_at >= step, decay * lane_sum(query_unit * key_row), 0.0)
        update_row = row_of(update)
        attend = attend + score * update_row
        if step < BLK - 1:
            strict = jnp.where(row_at > step, write_col * decay * lane_sum(key_unit * key_row), 0.0)
            update = update - strict * update_row
    normed = attend * lax.rsqrt(lane_sum(attend * attend) / size + EPSILON)
    normed = (normed * (gating * jax.nn.sigmoid(gating)) * live_col).astype(BF16)
    final = jnp.broadcast_to(cum[:, BLK - 1 :, :], cum.shape)
    for place, mask in enumerate(masks):
        block = jnp.concatenate([normed[place * per_block + e] for e in range(per_block)], axis=1)
        if not joined:
            mixed_ref[:, place * width : (place + 1) * width] = block
            continue
        mixed_ref[:, pl.ds(pl.multiple_of((index ^ mask) * width, width), width)] = block
        column = pl.multiple_of((index ^ mask ^ 1) * width, width)
        mixed_ref[:, pl.ds(column, width)] = before[0][:, place * width : (place + 1) * width]
    update_ref[...] = update.reshape(rows, size)
    faded_ref[...] = (key_unit * jnp.exp(final - cum)).reshape(rows, size)
    final_ref[...] = jnp.exp(final).reshape(rows, size)


def state_kernel(groups, count, *refs):
    state_ref, new_ref = refs[3 * len(groups) :]
    per_block = state_ref.shape[0] // count
    index = my_index()
    along = (((0,), (0,)), ((), ()))
    for place, masks in enumerate(groups):
        update_ref, faded_ref, final_ref = refs[3 * place : 3 * place + 3]
        for head in range(per_block * len(masks)):
            at = slice(head * BLK, (head + 1) * BLK)
            left_high, left_low = parts(faded_ref[at])
            right_high, right_low = parts(update_ref[at])
            left = jnp.concatenate([left_high, left_high, left_low, left_low], axis=0)
            right = jnp.concatenate([right_high, right_low, right_high, right_low], axis=0)
            grown = lax.dot_general(left, right, along, preferred_element_type=F32)
            scale = final_ref[head * BLK : head * BLK + 1, :]
            owner = (index ^ masks[head // per_block]) * per_block + head % per_block
            new_ref[pl.ds(owner, 1)] = (scale * state_ref[owner] + grown)[None]


def out_kernel(count, *refs):
    blocks = refs[:count]
    weight_ref, base_ref, out_ref, scratch = refs[count:]
    index = my_index()
    lhs = jnp.concatenate([block[...].astype(F32) for block in blocks], axis=0).astype(BF16)
    half = lhs.shape[1] // 2
    first = jnp.dot(lhs[:, :half], weight_ref[:half, :], preferred_element_type=F32).astype(BF16)
    second = jnp.dot(lhs[:, half:], weight_ref[half:, :], preferred_element_type=F32).astype(BF16)
    total = first.astype(F32) + second.astype(F32)
    for mask in range(count):
        row = pl.multiple_of((index ^ mask) * BLK, BLK)
        scratch[pl.ds(row, BLK), :] = total[mask * BLK : (mask + 1) * BLK]
    out_ref[...] = (base_ref[...].astype(F32) + scratch[...]).astype(BF16)


def group_device(
    tokens,
    lengths,
    state,
    gain_first,
    first_gate,
    first_up,
    first_down,
    gain_mix,
    query_weight,
    key_weight,
    value_weight,
    gating_weight,
    write_weight,
    forget_weight,
    forget_rate,
    out_weight,
    gain_second,
    second_gate,
    second_up,
    second_down,
):
    count = lax.axis_size("kv") * lax.axis_size("tp")
    rows, width = tokens.shape
    channels = gain_first.shape[0]
    heads, size = state.shape[1], state.shape[2]
    entered, gain_ready = enter(
        tokens, gain_first.reshape(1, channels), lengths, first_gate, first_up, first_down
    )
    after_first, near_live, pick = first_half_step(
        entered, rows, count, gain_ready, first_gate, first_up, first_down
    )
    cross_live = swap(near_live, 1, count)
    packed = pick.shape[0]
    columns = 4 * width
    near = count // 2
    near_masks, cross_masks = list(range(0, count, 2)), list(range(1, count, 2))
    mixers = [
        gain_mix.reshape(1, channels),
        query_weight,
        key_weight,
        value_weight,
        gating_weight,
        write_weight.T,
        forget_weight.T,
    ]
    parts_early = call(
        functools.partial(project_early_kernel, near_masks),
        [
            pltpu.VMEM((packed, columns), F32),
            pltpu.VMEM((packed, 2 * heads), F32),
            pltpu.VMEM((packed, 128), F32),
        ],
        [near_live, *mixers],
    )
    *sends, pre = call(
        functools.partial(project_late_kernel, cross_masks),
        [pltpu.VMEM((rows // near, columns), BF16)] * near + [pltpu.VMEM((BLK, 2 * heads), F32)],
        [cross_live, *mixers, *parts_early, pick],
        scratch=[pltpu.VMEM((rows, columns), F32), pltpu.VMEM((rows, 2 * heads), F32)],
    )
    owned = exchange_blocks(sends, count, "ex_d")
    matrices = state.reshape(heads, size, size)
    high, low, live = call(
        split_state_kernel,
        [pltpu.VMEM(matrices.shape, BF16)] * 2 + [pltpu.VMEM((BLK, heads), F32)],
        [matrices, lengths.reshape(1, 1)],
        limit=3 << 20,
    )
    groups = [list(range(0, count, 2)), list(range(1, count, 2))]
    mixed_parts, grown = [], []
    for place, masks in enumerate(groups):
        tall = heads * BLK // 2
        part, *rest = call(
            functools.partial(delta_kernel, masks, count, bool(place)),
            [pltpu.VMEM((BLK, channels // (2 - place)), BF16)] + [pltpu.VMEM((tall, size), F32)] * 3,
            [
                *(owned[m] for m in masks),
                pre,
                forget_rate.reshape(1, heads),
                live,
                high,
                low,
                *mixed_parts,
            ],
        )
        mixed_parts.append(part)
        grown += rest
    mixed = mixed_parts[1]
    head_blocks = gather_blocks(mixed, count, "ex_e")
    new_state = call(
        functools.partial(state_kernel, groups, count),
        jax.ShapeDtypeStruct((heads, size, size), F32),
        [*grown, matrices],
    )
    after_mix = call(
        functools.partial(out_kernel, count),
        pltpu.VMEM((rows, width), BF16),
        [*head_blocks, out_weight, after_first],
        scratch=[pltpu.VMEM((rows, width), F32)],
    )
    mixed_out = second_half_step(
        after_mix, count, gain_second, second_gate, second_up, second_down
    )
    return (mixed_out, new_state.reshape(state.shape))


def fits_group(mesh):
    near, cores = mesh.shape["kv"], mesh.shape["tp"]
    count = near * cores
    return cores == 2 and near & (near - 1) == 0 and near <= 8 and (HEADS * HEAD) % (count * 128) == 0


def per_device(mesh, *arrays):
    lengths, gate = arrays[1], arrays[4]
    suits = fits_group(mesh) and lengths.shape[0] == 1 and gate.shape[1] % 128 == 0
    if not suits:
        return general_device(*arrays)
    return group_device(*arrays)


def solution(mesh):
    in_specs = (
        P("dp", ("kv", "tp")),
        P(("dp", "kv", "tp")),
        P(("dp", "kv", "tp"), None, None, None),
        P(),
        P(None, "kv"),
        P(None, "kv"),
        P("kv", None),
        P(),
        P(None, ("kv", "tp")),
        P(None, ("kv", "tp")),
        P(None, ("kv", "tp")),
        P(None, ("kv", "tp")),
        P(),
        P(),
        P(),
        P(None, ("kv", "tp")),
        P(),
        P(None, "kv"),
        P(None, "kv"),
        P("kv", None),
    )
    out_specs = (P("dp", ("kv", "tp")), P(("dp", "kv", "tp"), None, None, None))
    return jax.shard_map(
        functools.partial(per_device, mesh),
        mesh=mesh,
        in_specs=in_specs,
        out_specs=out_specs,
        check_vma=False,
    )
```
